512 devices in a mesh: sp: 64 (over z, y), tp: 8 (over x, core).
Axes of the slice: x: 4, y: 4, z: 16, core: 2. Of those that a mesh axis runs over, the one named last changes fastest.
Arguments:
- latent: bfloat16 [16384, 2048], P(('sp', 'tp')), may hold values from -36 to 36
- condition: float32 [2048], replicated, may hold values from -16 to 16
- context: bfloat16 [256, 2048], P('sp'), may hold values from -6 to 6
- context_condition_vector: float32 [2048], replicated, may hold values from -6 to 6
- modulation_matrix: bfloat16 [3, 2048, 2048], P(None, 'sp', 'tp'), may hold values from -0.125 to 0.125
- query_matrix: bfloat16 [2048, 2048], P(None, 'tp'), may hold values from -0.125 to 0.125
- key_matrix: bfloat16 [2048, 2048], P(None, 'tp'), may hold values from -0.125 to 0.125
- value_matrix: bfloat16 [2048, 2048], P(None, 'tp'), may hold values from -0.125 to 0.125
- decay_input_weight: bfloat16 [2048, 32], replicated, may hold values from -0.125 to 0.125
- write_strength_weight: bfloat16 [2048, 32], replicated, may hold values from -0.125 to 0.125
- head_decay_rate: float32 [32], replicated, may hold values from 0 to 1, as said below
- write_strength_bias: float32 [32], replicated, may hold values from -20 to 0
- context_write_offset_bias: float32 [32], replicated, may hold values from 1.5 to 4.5
- log_spike_added: float32 [16384, 32], P('sp'), may hold values from -2 to 0, as said below
- head_norm_gain: float32 [128], replicated, may hold values from 0.1 to 1.9
- output_matrix: bfloat16 [2048, 2048], P('tp'), may hold values from -0.125 to 0.125
Outputs:
- mixed: bfloat16 [16384, 2048], P(('sp', 'tp'))
The draws below stay inside these ranges and needn't reach their ends.
Inputs may be any that keep to these rules, and one draw needn't show every extreme that they name: `head_decay_rate`: positive. `log_spike_added`: no entry is positive.
All inputs are finite; a program needn't handle non-finite values.
Results may differ from the reference program's by a relative error of at most 0.018.
Values may be sent and summed in bfloat16 or wider, within the bound.
No kernel may reach another device: no remote copies, remote signals or barrier semaphores. Data moves between devices by JAX's collectives and lax.ppermute only.
A program may use at most 128 MiB of HBM per device.

```python
import math
import jax
import jax.numpy as jnp
from jax import lax

D = 2048
RECURRENT_HEADS = 16
DK = 128
BLOCK = 64
TOK_DEV = 256
CTX = 256
LATENT_TOKENS = 16384


def draw_latent(key, part):
    base_key = jax.random.fold_in(key, 11)
    noise_key, row_key, col_key = jax.random.split(base_key, 3)
    noise_part = jnp.clip(jax.random.normal(noise_key, (LATENT_TOKENS, D), jnp.float32), -4.0, 4.0)
    row_scale = jnp.exp(jax.random.uniform(row_key, (LATENT_TOKENS, 1), jnp.float32, math.log(0.3), math.log(3.0)))
    col_scale = jnp.exp(jax.random.uniform(col_key, (1, D), jnp.float32, math.log(0.3), math.log(3.0)))
    return (noise_part * row_scale * col_scale).astype(jnp.bfloat16)


def draw_condition(key, part):
    base_key = jax.random.fold_in(key, 12)
    noise_part = jnp.clip(jax.random.normal(base_key, (D,), jnp.float32), -4.0, 4.0)
    rising = jnp.exp(jnp.linspace(0.0, math.log(3.0), D))
    return noise_part * rising


def draw_head_decay_rate(key, part):
    base_key = jax.random.fold_in(key, 13)
    pick_key, fast_key, slow_key = jax.random.split(base_key, 3)
    fast_heads = jax.random.randint(pick_key, (2 * RECURRENT_HEADS,), 0, 2) == 0
    fast_rate = jnp.exp(jax.random.uniform(fast_key, (2 * RECURRENT_HEADS,), jnp.float32, math.log(0.025), math.log(0.06)))
    slow_rate = jnp.exp(jax.random.uniform(slow_key, (2 * RECURRENT_HEADS,), jnp.float32, math.log(0.05), math.log(0.5))) / LATENT_TOKENS
    return jnp.where(fast_heads, fast_rate, slow_rate)


def draw_write_strength_bias(key, part):
    base_key = jax.random.fold_in(key, 14)
    centre = math.log(DK / (4.0 * LATENT_TOKENS))
    return jax.random.uniform(base_key, (2 * RECURRENT_HEADS,), jnp.float32, centre - 1.0, centre + 1.0)


def draw_log_spike_added(key, part):
    base_key = jax.random.fold_in(key, 15)
    rate_key, location_random_key, magnitude_random_key = jax.random.split(base_key, 3)
    span_length = max(TOK_DEV // 2, 1)
    span_count = LATENT_TOKENS // span_length
    base_rate = jnp.exp(jax.random.uniform(rate_key, (span_count, 2 * RECURRENT_HEADS), jnp.float32, math.log(0.1), math.log(1.0))) / LATENT_TOKENS
    spike_magnitude = jnp.log(jax.random.uniform(magnitude_random_key, (2, 2 * RECURRENT_HEADS), jnp.float32, 0.5, 0.8))
    base_complete = jnp.repeat(base_rate, span_length, axis=0)
    spike_location = jax.random.randint(location_random_key, (2, 2 * RECURRENT_HEADS), 0, LATENT_TOKENS)
    token_position = jnp.arange(LATENT_TOKENS)[:, None, None]
    spike_total = jnp.sum(jnp.where(token_position == spike_location[None], spike_magnitude[None], 0.0), axis=1)
    return spike_total - base_complete


def block_levels(stream_key, dims, shards, low, high):
    def one(dim, shards_of):
        steps = jax.random.uniform(jax.random.fold_in(jax.random.fold_in(stream_key, 6), dim), (shards_of,), jnp.float32, low / len(shards), high / len(shards))
        return jnp.repeat(jnp.exp(steps), dims[dim] // shards_of).reshape((-1,) + (1,) * (len(dims) - dim - 1))

    loudness = one(*shards[0])
    for cut in shards[1:]:
        loudness = loudness * one(*cut)
    return loudness


def scatter_about(rng, shape, scale, limit, cuts=(), kind=jnp.bfloat16):
    gain = block_levels(rng, shape, cuts, -0.22, 0.18) if cuts else 1.0
    entries = jax.random.normal(rng, shape, jnp.float32) * scale * gain
    return jnp.minimum(jnp.maximum(entries, -limit), limit).astype(kind)


def setup_inputs(seed: int = 0) -> dict:
    splits = jax.random.split(jax.random.key(seed), 17)
    latent = draw_latent(jax.random.fold_in(splits[16], 71), 0)
    condition = draw_condition(jax.random.fold_in(splits[16], 71), 0)
    context = scatter_about(splits[2], (CTX, D), 1.0, 6.0, ((0, 64),))
    context_condition_vector = scatter_about(splits[3], (D,), 1.0, 6.0, (), jnp.float32)
    modulation_matrix = scatter_about(splits[4], (3, D, D), D ** -0.5, 0.125, ((1, 64), (2, 8)))
    query_matrix = scatter_about(splits[5], (D, RECURRENT_HEADS * DK), D ** -0.5, 0.125, ((1, 8),))
    key_matrix = scatter_about(splits[6], (D, RECURRENT_HEADS * DK), D ** -0.5, 0.125, ((1, 8),))
    value_matrix = scatter_about(splits[7], (D, RECURRENT_HEADS * DK), D ** -0.5, 0.125, ((1, 8),))
    decay_input_weight = scatter_about(splits[8], (D, 2 * RECURRENT_HEADS), D ** -0.5, 0.125)
    write_strength_weight = scatter_about(splits[9], (D, 2 * RECURRENT_HEADS), D ** -0.5, 0.125)
    head_decay_rate = draw_head_decay_rate(jax.random.fold_in(splits[16], 71), 0)
    write_strength_bias = draw_write_strength_bias(jax.random.fold_in(splits[16], 71), 0)
    context_write_offset_bias = jnp.clip(jax.random.uniform(splits[12], (2 * RECURRENT_HEADS,), jnp.float32, 1.5, 4.5), 1.5, 4.5)
    log_spike_added = draw_log_spike_added(jax.random.fold_in(splits[16], 71), 0)
    head_norm_gain = jnp.clip(1.0 + 0.18 * jax.random.normal(splits[14], (DK,), jnp.float32), 0.1, 1.9)
    output_matrix = scatter_about(splits[15], (RECURRENT_HEADS * DK, D), (RECURRENT_HEADS * DK) ** -0.5, 0.125, ((0, 8),))
    return dict(latent=latent, condition=condition, context=context, context_condition_vector=context_condition_vector, modulation_matrix=modulation_matrix, query_matrix=query_matrix, key_matrix=key_matrix, value_matrix=value_matrix, decay_input_weight=decay_input_weight, write_strength_weight=write_strength_weight, head_decay_rate=head_decay_rate, write_strength_bias=write_strength_bias, context_write_offset_bias=context_write_offset_bias, log_spike_added=log_spike_added, head_norm_gain=head_norm_gain, output_matrix=output_matrix)


EPSILON = 1e-06
TOP_PRECISION = lax.Precision.HIGHEST

def layer_norm(matrix):
    widened = matrix.astype(jnp.float32)
    centred = widened - lax.optimization_barrier(jnp.mean(widened, axis=-1, keepdims=True))
    spread = lax.optimization_barrier(jnp.mean(centred * centred, axis=-1, keepdims=True))
    return centred * lax.rsqrt(spread + EPSILON)

def modulate(matrix, shift_vec, scale_vec):
    return (layer_norm(matrix) * (1.0 + scale_vec) + shift_vec).astype(jnp.bfloat16)

def rounded(matrix):
    return lax.optimization_barrier(matrix.astype(jnp.bfloat16)).astype(jnp.float32)

def project(row_block, weight):
    return rounded(jnp.dot(row_block.astype(jnp.float32), weight.astype(jnp.float32), preferred_element_type=jnp.float32))

def unit_length(vectors):
    return vectors * lax.rsqrt(lax.optimization_barrier(jnp.sum(vectors * vectors, axis=-1, keepdims=True)) + EPSILON)

def orient(matrix, direction):
    return matrix if direction == 0 else jnp.flip(matrix, axis=0)

def to_blocks(matrix):
    block_count = matrix.shape[0] // BLOCK
    shaped = matrix.reshape((block_count, BLOCK) + matrix.shape[1:])
    return jnp.swapaxes(shaped, 1, 2)

def from_blocks(matrix):
    shaped = jnp.swapaxes(matrix, 1, 2)
    return shaped.reshape((shaped.shape[0] * shaped.shape[1],) + shaped.shape[2:])

def block_terms(key_rows, value_rows, logarithm_decay, strength):
    key_blocks = to_blocks(key_rows)
    value_blocks = to_blocks(value_rows)
    strength_blocks = to_blocks(strength)
    cumulative = jnp.cumsum(to_blocks(logarithm_decay), axis=-1)
    token_position = jnp.arange(BLOCK)
    inclusive = token_position[:, None] >= token_position[None, :]
    strictly = token_position[:, None] > token_position[None, :]
    spread_log = cumulative[..., :, None] - cumulative[..., None, :]
    decay_mat = jnp.where(inclusive, jnp.exp(jnp.where(inclusive, spread_log, 0.0)), 0.0)
    weighted = key_blocks * strength_blocks[..., None]
    lower_part = jnp.where(strictly, jnp.einsum('nhid,nhjd->nhij', weighted, key_blocks, precision=TOP_PRECISION) * decay_mat, 0.0)
    system = lower_part + jnp.eye(BLOCK, dtype=jnp.float32)
    right_side = jnp.concatenate([value_blocks * strength_blocks[..., None], weighted * jnp.exp(cumulative)[..., None]], axis=-1)
    solved = jax.scipy.linalg.solve_triangular(system, right_side, lower=True, unit_diagonal=True)
    value_width = value_blocks.shape[-1]
    final_log_value = cumulative[..., -1]
    decayed_keys = key_blocks * jnp.exp(final_log_value[..., None] - cumulative)[..., None]
    return (key_blocks, solved[..., :value_width], solved[..., value_width:], decayed_keys, final_log_value, cumulative, decay_mat)

def advance(carried_state, state_update, correction_term, decayed_keys, final_log_value):
    fresh_values = state_update - jnp.einsum('xui,xij->xuj', correction_term, carried_state, precision=TOP_PRECISION)
    following_rows = carried_state * jnp.exp(final_log_value)[:, None, None] + jnp.einsum('fga,fgo->fao', decayed_keys, fresh_values, precision=TOP_PRECISION)
    return (fresh_values, following_rows)

def final_state(key_rows, value_rows, logarithm_decay, strength, start_state):
    block_parts = block_terms(key_rows, value_rows, logarithm_decay, strength)

    def block_step(carried_state, inputs):
        fresh_values, following_rows = advance(carried_state, *inputs)
        return (following_rows, None)
    carried_state, _ = lax.scan(block_step, start_state, block_parts[1:5])
    return carried_state

def read_out(query_rows, block_parts, start_state):
    key_blocks, state_update, correction_term, decayed_keys, final_log_value, cumulative, decay_mat = block_parts
    query_blocks = to_blocks(query_rows)
    query_decayed = query_blocks * jnp.exp(cumulative)[..., None]
    token_position = jnp.arange(BLOCK)
    inclusive = token_position[:, None] >= token_position[None, :]
    scores = jnp.where(inclusive, jnp.einsum('nhid,nhjd->nhij', query_blocks, key_blocks, precision=TOP_PRECISION) * decay_mat, 0.0)

    def block_step(carried_state, inputs):
        piece_update, piece_fix, piece_keys, piece_log, segment_query, piece_score = inputs
        fresh_values, following_rows = advance(carried_state, piece_update, piece_fix, piece_keys, piece_log)
        result_output = jnp.einsum('xui,xij->xuj', segment_query, carried_state, precision=TOP_PRECISION)
        result_output = result_output + jnp.einsum('hij,hjv->hiv', piece_score, fresh_values, precision=TOP_PRECISION)
        return (following_rows, result_output)
    _, result_output = lax.scan(block_step, start_state, (state_update, correction_term, decayed_keys, final_log_value, query_decayed, scores))
    return from_blocks(result_output)

def reference(latent, condition, context, context_condition_vector, modulation_matrix, query_matrix, key_matrix, value_matrix, decay_input_weight, write_strength_weight, head_decay_rate, write_strength_bias, context_write_offset_bias, log_spike_added, head_norm_gain, output_matrix):
    mod_float = modulation_matrix.astype(jnp.float32)
    latent_factors = jnp.einsum('i,rij->rj', jax.nn.silu(condition), mod_float, precision=TOP_PRECISION)
    context_factors = jnp.einsum('i,rij->rj', jax.nn.silu(context_condition_vector), mod_float[:2], precision=TOP_PRECISION)
    hidden = modulate(latent, latent_factors[0], latent_factors[1])
    context_hidden = modulate(context, context_factors[0], context_factors[1])
    length_total = hidden.shape[0]
    context_length = context_hidden.shape[0]
    queries = project(hidden, query_matrix).reshape(length_total, RECURRENT_HEADS, DK)
    latent_keys = unit_length(project(hidden, key_matrix).reshape(length_total, RECURRENT_HEADS, DK))
    latent_values = project(hidden, value_matrix).reshape(length_total, RECURRENT_HEADS, DK)
    decay_rates = head_decay_rate.reshape(RECURRENT_HEADS, 2)
    logarithm_decay = -decay_rates * jax.nn.softplus(project(hidden, decay_input_weight).reshape(length_total, RECURRENT_HEADS, 2))
    logarithm_decay = logarithm_decay + log_spike_added.reshape(length_total, RECURRENT_HEADS, 2)
    strength = jax.nn.sigmoid(project(hidden, write_strength_weight).reshape(length_total, RECURRENT_HEADS, 2) + write_strength_bias.reshape(RECURRENT_HEADS, 2))
    context_keys = unit_length(project(context_hidden, key_matrix).reshape(context_length, RECURRENT_HEADS, DK))
    context_values = project(context_hidden, value_matrix).reshape(context_length, RECURRENT_HEADS, DK)
    context_decay = -decay_rates * jax.nn.softplus(project(context_hidden, decay_input_weight).reshape(context_length, RECURRENT_HEADS, 2))
    context_strength = jax.nn.sigmoid(project(context_hidden, write_strength_weight).reshape(context_length, RECURRENT_HEADS, 2) + write_strength_bias.reshape(RECURRENT_HEADS, 2) + context_write_offset_bias.reshape(RECURRENT_HEADS, 2))
    zero_state = jnp.zeros((RECURRENT_HEADS, DK, DK), jnp.float32)
    summed = jnp.zeros((length_total, RECURRENT_HEADS, DK), jnp.float32)
    for direction in range(2):
        carried_state = final_state(orient(context_keys, direction), orient(context_values, direction), orient(context_decay[..., direction], direction), orient(context_strength[..., direction], direction), zero_state)
        block_parts = block_terms(orient(latent_keys, direction), orient(latent_values, direction), orient(logarithm_decay[..., direction], direction), orient(strength[..., direction], direction))
        summed = summed + orient(read_out(orient(queries, direction), block_parts, carried_state), direction)
    normed = summed * lax.rsqrt(lax.optimization_barrier(jnp.mean(summed * summed, axis=-1, keepdims=True)) + EPSILON) * head_norm_gain
    normed = normed.astype(jnp.bfloat16).reshape(length_total, RECURRENT_HEADS * DK)
    branch = jnp.dot(normed.astype(jnp.float32), output_matrix.astype(jnp.float32), preferred_element_type=jnp.float32)
    return (latent.astype(jnp.float32) + latent_factors[2] * branch).astype(jnp.bfloat16)
```

```python
import jax
import jax.numpy as jnp
from jax import lax
from jax.experimental import pallas as pl
from jax.experimental.pallas import tpu as pltpu
from jax.sharding import Mesh
from jax.sharding import PartitionSpec as P

D = 2048
DK = 128
EPS = 1e-06
HI = lax.Precision.HIGHEST
F32 = jnp.float32
BF = jnp.bfloat16
Z = ("zh", "zl")
TP = ("x", "c")
SP = ("zh", "zl", "y")
ALL = ("zh", "zl", "y", "x", "c")
VM = pl.BlockSpec(memory_space=pltpu.VMEM)
SM = pl.BlockSpec(memory_space=pltpu.SMEM)


def mm(a, b, dims=((1,), (0,))):
    return lax.dot_general(
        a.astype(BF), b.astype(BF), (dims, ((), ())), preferred_element_type=F32
    )


def norm_rows(rows, scale, shift):
    wide = rows.astype(F32)
    centred = wide - jnp.mean(wide, axis=-1, keepdims=True)
    spread = jnp.mean(centred * centred, axis=-1, keepdims=True)
    return (centred * lax.rsqrt(spread + EPS) * (1.0 + scale) + shift).astype(BF)


def column(matrix, lane):
    lanes = lax.broadcasted_iota(jnp.int32, matrix.shape, 1)
    return jnp.sum(jnp.where(lanes == lane, matrix, 0.0), axis=1, keepdims=True)


def softplus(t):
    return jnp.maximum(t, 0.0) + jnp.log1p(jnp.exp(-jnp.abs(t)))


def sigmoid(t):
    return 1.0 / (1.0 + jnp.exp(-t))


def inverse_of(lower, row, col):
    eye = (row == col).astype(F32)
    own = (row // 16) == (col // 16)
    base = [jnp.where(own, m, 0.0) for m in lower]
    inv = [eye - m for m in base]
    power = [mm(m, m) for m in base]
    for step in range(3):
        inv = [p + mm(p, x) for p, x in zip(inv, power)]
        if step < 2:
            power = [mm(x, x) for x in power]
    size = 16
    while size < 256:
        here = ((row // (2 * size)) == (col // (2 * size))) & ((row // size) != (col // size))
        side = [mm(jnp.where(here, m, 0.0), p) for m, p in zip(lower, inv)]
        inv = [p - mm(p, s) for p, s in zip(inv, side)]
        size *= 2
    out = []
    for m, p in zip(lower, inv):
        first = p.astype(BF)
        high = m.astype(BF)
        low = (m - high.astype(F32)).astype(BF)
        wide = first.astype(F32)
        left = (eye - wide) - (mm(high, first) + mm(low, first))
        out.append(wide + mm(first, left))
    return out


def project_kernel(pos, lat, ctx, fac, wq, wk, wv, wd, ww, q_o, k_o, v_o, r_o, w_o, c_o, hid):
    factors = [[], [], [], []]
    for t in range(8):
        f = (fac[t] + fac[8 + t]) + (fac[16 + t] + fac[24 + t])
        for slot, r in enumerate((0, 1, 3, 4)):
            factors[slot].append(f[r : r + 1])
    shift, scale, c_shift, c_scale = (jnp.concatenate(f, axis=1) for f in factors)
    for t in range(8):
        hid[32 * t : 32 * t + 32] = norm_rows(lat[t], scale, shift)
    hid[256:272] = norm_rows(ctx[...], c_scale, c_shift)
    rows = hid[...]
    q_o[...] = mm(hid[0:256], wq[...]).astype(BF)
    keys = mm(rows, wk[...]).astype(BF)
    values = mm(rows, wv[...]).astype(BF)
    rate = mm(rows, wd[...]).astype(BF).astype(F32)
    write = mm(rows, ww[...]).astype(BF).astype(F32)
    k_o[...] = keys[:256]
    v_o[...] = values[:256]
    r_o[...] = rate[:256]
    w_o[...] = write[:256]
    combo = pos[0]
    first = combo < 2
    ck, cv = (keys[256:272].astype(F32), values[256:272].astype(F32))
    c_o[:, 0:128] = jnp.where(first, ck[:, :128], ck[:, 128:]).astype(BF)
    c_o[:, 128:256] = jnp.where(first, cv[:, :128], cv[:, 128:]).astype(BF)
    lane = pos[1] * 4 + combo
    lanes = lax.broadcasted_iota(jnp.int32, (16, 128), 1)
    gates = jnp.where(lanes == 0, column(rate[256:272], lane), 0.0)
    gates = jnp.where(lanes == 1, column(write[256:272], lane), gates)
    c_o[:, 256:384] = gates.astype(BF)


def chunk_kernel(pos, q, k, v, rate, write, spike, decay, bias, m_o, r_o, o_o):
    row = lax.broadcasted_iota(jnp.int32, (256, 256), 0)
    col = lax.broadcasted_iota(jnp.int32, (256, 256), 1)
    eye = row == col
    logs = -decay[...] * softplus(rate[...]) + spike[...]
    strength = sigmoid(write[...] + bias[...])
    below = (row >= col).astype(F32)
    above = (row <= col).astype(F32)
    sums = (
        jnp.dot(below, logs, precision=HI, preferred_element_type=F32),
        jnp.dot(above, logs, precision=HI, preferred_element_type=F32),
    )
    lowers, parts = ([], [])
    for h in range(2):
        kh = k[:, 128 * h : 128 * h + 128]
        qh = q[:, 128 * h : 128 * h + 128]
        kf = kh.astype(F32)
        unit = lax.rsqrt(jnp.sum(kf * kf, axis=1, keepdims=True) + EPS)
        unit_row = jnp.sum(jnp.where(eye, unit, 0.0), axis=0, keepdims=True)
        gram = mm(kh, kh, ((1,), (1,))) * unit_row
        cross = mm(qh, kh, ((1,), (1,))) * unit_row
        for e in range(2):
            lane = pos[1] * 4 + 2 * h + e
            total = column(sums[e], lane)
            b = column(strength, lane)
            total_row = jnp.sum(jnp.where(eye, total, 0.0), axis=0, keepdims=True)
            last = total[255:256] if e == 0 else total[0:1]
            inside = row >= col if e == 0 else row <= col
            fade = jnp.where(inside, jnp.exp(jnp.where(inside, total - total_row, 0.0)), 0.0)
            lowers.append(jnp.where(eye, 0.0, (b * unit) * gram * fade))
            grown = jnp.exp(total)
            right = jnp.concatenate(
                [
                    b * v[:, 128 * h : 128 * h + 128].astype(F32),
                    (b * unit * grown) * kf,
                ],
                axis=1,
            ).astype(BF)
            faded = (kf * (unit * jnp.exp(last - total))).astype(BF)
            scores = (cross * fade).astype(BF)
            parts.append((right, faded, scores, grown * qh.astype(F32), jnp.exp(last) - 1.0))
    solved = inverse_of(lowers, row, col)
    small = lax.broadcasted_iota(jnp.int32, (128, 128), 0) == lax.broadcasted_iota(
        jnp.int32, (128, 128), 1
    )
    outs = [None, None]
    for j in range(4):
        right, faded, scores, grown_q, short = parts[j]
        both = mm(solved[j], right).astype(BF)
        maps = mm(faded, both, ((0,), (0,)))
        read = mm(scores, both)
        m_o[j, :, 0:128] = (jnp.where(small, short, 0.0) - maps[:, 128:]).astype(BF)
        m_o[j, :, 128:256] = maps[:, :128].astype(BF)
        h, e = divmod(j, 2)
        r_o[h, :, 128 * e : 128 * e + 128] = (grown_q - read[:, 128:]).astype(BF)
        outs[h] = read[:, :128] if e == 0 else outs[h] + read[:, :128]
    o_o[:, 0:128] = outs[0]
    o_o[:, 128:256] = outs[1]


def context_kernel(pos, rows, decay, bias, extra, s_o):
    row = lax.broadcasted_iota(jnp.int32, (256, 256), 0)
    col = lax.broadcasted_iota(jnp.int32, (256, 256), 1)
    eye = row == col
    lane = pos[1] * 4 + pos[0]
    ahead = (row - col) * (1 - 2 * (pos[0] % 2))
    inside = ahead >= 0
    kh = rows[:, 0:128]
    kf = kh.astype(F32)
    gates = rows[:, 256:384].astype(F32)
    logs = -column(decay[...], lane) * softplus(gates)
    b = column(sigmoid(gates + column(bias[...], lane) + column(extra[...], lane)), 1)
    sums = jnp.dot(inside.astype(F32), logs, precision=HI, preferred_element_type=F32)
    total = column(sums, 0)
    total_row = jnp.sum(jnp.where(eye, total, 0.0), axis=0, keepdims=True)
    last = jnp.min(total, axis=0, keepdims=True)
    unit = lax.rsqrt(jnp.sum(kf * kf, axis=1, keepdims=True) + EPS)
    unit_row = jnp.sum(jnp.where(eye, unit, 0.0), axis=0, keepdims=True)
    fade = jnp.where(inside, jnp.exp(jnp.where(inside, total - total_row, 0.0)), 0.0)
    lower = jnp.where(
        eye, 0.0, (b * unit) * (mm(kh, kh, ((1,), (1,))) * unit_row) * fade
    )
    solved = inverse_of([lower], row, col)[0]
    fresh = mm(solved, b * rows[:, 128:256].astype(F32))
    faded = kf * (unit * jnp.exp(last - total))
    s_o[...] = mm(faded, fresh, ((0,), (0,)))


def apply_to(linear, state):
    high = state.astype(BF)
    low = (state - high.astype(F32)).astype(BF)
    both = mm(linear, jnp.concatenate([high, low], axis=1))
    n = state.shape[1]
    return both[:, :n] + both[:, n:]


def compose_kernel(pos, maps, o):
    back = pos[0] % 2
    at = back * 3
    step = 1 - 2 * back
    total = maps[at].astype(F32)
    for _ in range(3):
        at = at + step
        total = total + maps[at].astype(F32) + apply_to(maps[at][:, 0:128], total)
    out = total.astype(BF)
    for i in range(4):
        o[i] = out


def scan_kernel(pos, start, high, low, own, o):
    back = pos[0] % 2
    step = 1 - 2 * back
    state = start[...]
    for maps, mine in ((high, pos[2]), (low, pos[3])):
        at = back * 3
        for _ in range(3):
            moved = state + maps[at][:, 128:256].astype(F32) + apply_to(maps[at][:, 0:128], state)
            state = jnp.where((mine - at) * step > 0, moved, state)
            at = at + step
    at = back * 3
    for i in range(4):
        o[at] = state.astype(BF)
        if i < 3:
            state = state + own[at][:, 128:256].astype(F32) + apply_to(own[at][:, 0:128], state)
        at = at + step


def read_kernel(states, reads, base, gain, o):
    for h in range(2):
        total = base[:, 128 * h : 128 * h + 128] + mm(reads[h], states[h])
        mean = jnp.mean(total * total, axis=1, keepdims=True)
        o[:, 128 * h : 128 * h + 128] = (total * lax.rsqrt(mean + EPS) * gain[...]).astype(BF)


def output_kernel(at, rows, fac, lat, *rest):
    weights, o = (rest[:8], rest[8])
    branch = mm(rows[at[0]], weights[0][...])
    for i in range(1, 8):
        branch = branch + mm(rows[at[i]], weights[i][...])
    gates = []
    for t in range(8):
        f = (fac[t] + fac[8 + t]) + (fac[16 + t] + fac[24 + t])
        gates.append(f[2:3])
    gate = jnp.concatenate(gates, axis=1)
    o[...] = (lat[...].astype(F32) + gate * branch).astype(BF)


def call(kernel, outs, specs, scratch=(), flops=1):
    def shape(s):
        return jax.ShapeDtypeStruct(*s)

    many = isinstance(outs, list)
    return pl.pallas_call(
        kernel,
        out_shape=[shape(s) for s in outs] if many else shape(outs),
        in_specs=specs,
        out_specs=[VM] * len(outs) if many else VM,
        scratch_shapes=scratch,
        cost_estimate=pl.CostEstimate(flops=flops, bytes_accessed=1, transcendentals=0),
    )


def to_all(value, axes, count):
    return lax.all_to_all(
        jnp.broadcast_to(value[None], (count, *value.shape)), axes, 0, 0, tiled=True
    )


def per_device(
    latent,
    condition,
    context,
    context_condition_vector,
    modulation_matrix,
    query_matrix,
    key_matrix,
    value_matrix,
    decay_input_weight,
    write_strength_weight,
    head_decay_rate,
    write_strength_bias,
    context_write_offset_bias,
    log_spike_added,
    head_norm_gain,
    output_matrix,
):
    zh, zl, y = (lax.axis_index("zh"), lax.axis_index("zl"), lax.axis_index("y"))
    x, c = (lax.axis_index("x"), lax.axis_index("c"))
    pos = jnp.stack([y, x * 2 + c, zh, zl]).astype(jnp.int32)
    sp_index = lax.axis_index(SP)
    signals = jnp.stack([condition, context_condition_vector])
    signals = lax.dynamic_slice_in_dim(jax.nn.silu(signals), sp_index * 32, 32, 1)
    mod = modulation_matrix.astype(F32)
    part = jnp.concatenate(
        [
            jnp.sum(mod * signals[0][None, :, None], axis=1),
            jnp.sum(mod[:2] * signals[1][None, :, None], axis=1),
        ]
    )
    part = jnp.sum(to_all(part, Z, 16), axis=0)
    fac = to_all(part, ("y", "x", "c"), 32)
    lat = to_all(latent, TP, 8)
    ctx = to_all(context, "y", 4).reshape(16, D)

    weights = [output_matrix]
    own = lax.optimization_barrier((output_matrix, lat))[0]
    for d in range(1, 4):
        weights.append(lax.ppermute(own, "x", [(i, (i + d) % 4) for i in range(4)]))
    for d in range(4):
        weights.append(lax.ppermute(weights[d], "c", [(0, 1), (1, 0)]))
    shifted = (x - jnp.arange(4, dtype=jnp.int32)) % 4
    where = jnp.concatenate([shifted * 2 + c, shifted * 2 + 1 - c]).astype(jnp.int32)

    queries, keys, values, rate, write, rows = call(
        project_kernel,
        [
            ((256, 256), BF),
            ((256, 256), BF),
            ((256, 256), BF),
            ((256, 32), F32),
            ((256, 32), F32),
            ((16, 384), BF),
        ],
        [SM] + [VM] * 8,
        [pltpu.VMEM((272, D), BF)],
        flops=10**9,
    )(
        pos,
        lat,
        ctx,
        fac,
        query_matrix,
        key_matrix,
        value_matrix,
        decay_input_weight,
        write_strength_weight,
    )
    all_rows = to_all(rows, Z, 16).reshape(256, 384)
    decay = head_decay_rate.reshape(1, 32)
    bias = write_strength_bias.reshape(1, 32)
    extra = context_write_offset_bias.reshape(1, 32)
    maps, reads, base = call(
        chunk_kernel,
        [((4, 128, 256), BF), ((2, 256, 256), BF), ((256, 256), F32)],
        [SM] + [VM] * 8,
        flops=4 * 10**9,
    )(pos, queries, keys, values, rate, write, log_spike_added, decay, bias)
    of_y = lax.all_to_all(maps, "y", 0, 0, tiled=True)
    start = call(context_kernel, ((128, 128), F32), [SM] + [VM] * 4, flops=10**9)(
        pos, all_rows, decay, bias, extra
    )
    group = call(compose_kernel, ((4, 128, 256), BF), [SM, VM], flops=10**8)
    of_low = lax.all_to_all(group(pos, of_y), "zl", 0, 0, tiled=True)
    of_high = lax.all_to_all(group(pos, of_low), "zh", 0, 0, tiled=True)
    states = call(scan_kernel, ((4, 128, 128), BF), [SM] + [VM] * 4, flops=10**8)(
        pos, start, of_high, of_low, of_y
    )
    states = lax.all_to_all(states, "y", 0, 0, tiled=True).reshape(2, 256, 128)
    normed = call(read_kernel, ((256, 256), BF), [VM] * 4, flops=10**8)(
        states, reads, base, head_norm_gain.reshape(1, 128)
    )
    heads = lax.all_to_all(normed.reshape(8, 32, 256), TP, 0, 0, tiled=True)
    return call(output_kernel, ((32, D), BF), [SM] + [VM] * 11, flops=10**9)(
        where, heads, fac, latent, *weights
    )


def solution(mesh):
    split = Mesh(mesh.devices.reshape(4, 4, 4, 4, 2), ALL)
    return jax.shard_map(
        per_device,
        mesh=split,
        in_specs=(
            P(ALL, None),
            P(),
            P(SP, None),
            P(),
            P(None, SP, TP),
            P(None, TP),
            P(None, TP),
            P(None, TP),
            P(),
            P(),
            P(),
            P(),
            P(),
            P(SP, None),
            P(),
            P(TP, None),
        ),
        out_specs=P(ALL, None),
        check_vma=False,
    )
```

```python
from functools import partial

import jax
import jax.numpy as jnp
from jax import lax
from jax.experimental import pallas as pl
from jax.experimental.pallas import tpu as pltpu
from jax.sharding import Mesh
from jax.sharding import PartitionSpec as P


D = 2048
EPS = 1e-06
HI = lax.Precision.HIGHEST
F32 = jnp.float32
BF = jnp.bfloat16
Z = ("zh", "zl")
TP = ("x", "c")
SP = ("zh", "zl", "y")
ALL = ("zh", "zl", "y", "x", "c")
VM = pl.BlockSpec(memory_space=pltpu.VMEM)
SM = pl.BlockSpec(memory_space=pltpu.SMEM)


def mm(a, b, dims=((1,), (0,))):
    return lax.dot_general(
        a.astype(BF), b.astype(BF), (dims, ((), ())), preferred_element_type=F32
    )


def norm_rows(rows, scale, shift):
    wide = rows.astype(F32)
    centred = wide - jnp.mean(wide, axis=-1, keepdims=True)
    spread = jnp.mean(centred * centred, axis=-1, keepdims=True)
    return (centred * lax.rsqrt(spread + EPS) * (1.0 + scale) + shift).astype(BF)


def column(matrix, lane):
    lanes = lax.broadcasted_iota(jnp.int32, matrix.shape, 1)
    return jnp.sum(jnp.where(lanes == lane, matrix, 0.0), axis=1, keepdims=True)


def softplus(t):
    return jnp.maximum(t, 0.0) + jnp.log1p(jnp.exp(-jnp.abs(t)))


def sigmoid(t):
    return 1.0 / (1.0 + jnp.exp(-t))


def inverse_of(lower, row, col):
    eye = (row == col).astype(F32)
    own = (row // 16) == (col // 16)
    base = [jnp.where(own, m, 0.0) for m in lower]
    inv = [eye - m for m in base]
    power = [mm(m, m) for m in base]
    for step in range(3):
        inv = [p + mm(p, x) for p, x in zip(inv, power)]
        if step < 2:
            power = [mm(x, x) for x in power]
    size = 16
    while size < 256:
        here = ((row // (2 * size)) == (col // (2 * size))) & ((row // size) != (col // size))
        side = [mm(jnp.where(here, m, 0.0), p) for m, p in zip(lower, inv)]
        inv = [p - mm(p, s) for p, s in zip(inv, side)]
        size *= 2
    out = []
    for m, p in zip(lower, inv):
        first = p.astype(BF)
        high = m.astype(BF)
        low = (m - high.astype(F32)).astype(BF)
        wide = first.astype(F32)
        left = (eye - wide) - (mm(high, first) + mm(low, first))
        out.append(wide + mm(first, left))
    return out


def project_kernel(pos, one, two, ctx, fac, wq, wk, wv, wd, ww, q_o, k_o, v_o, r_o, w_o, c_o, hid):
    factors = [[], [], [], []]
    for t in range(8):
        f = (fac[t] + fac[8 + t]) + (fac[16 + t] + fac[24 + t])
        for slot, r in enumerate((0, 1, 3, 4)):
            factors[slot].append(f[r : r + 1])
    shift, scale, c_shift, c_scale = (jnp.concatenate(f, axis=1) for f in factors)
    for d in range(4):
        for lat, core in ((one, pos[6]), (two, 1 - pos[6])):
            spot = (2 * ((pos[7] + 4 - d) % 4) + core) * 32
            hid[pl.ds(pl.multiple_of(spot, 32), 32)] = norm_rows(lat[d], scale, shift)
    hid[256:260] = norm_rows(ctx[...], c_scale, c_shift)
    hid[260:272] = jnp.zeros((12, D), BF)
    rows = hid[...]
    q_o[...] = mm(hid[0:256], wq[...]).astype(BF)
    keys = mm(rows, wk[...]).astype(BF)
    values = mm(rows, wv[...]).astype(BF)
    k_o[...] = keys[:256]
    v_o[...] = values[:256]
    last_two = ((1,), (1,))
    r_o[...] = mm(wd[...], hid[0:256], last_two).astype(BF).astype(F32)
    w_o[...] = mm(ww[...], hid[0:256], last_two).astype(BF).astype(F32)
    rate = mm(hid[256:264], wd[...], last_two).astype(BF).astype(F32)
    write = mm(hid[256:264], ww[...], last_two).astype(BF).astype(F32)
    lanes = lax.broadcasted_iota(jnp.int32, (8, 256), 1)
    spots = lanes == lax.broadcasted_iota(jnp.int32, (8, 256), 0) + pos[5]
    wide = [rows_of[256:264].astype(F32) for rows_of in (keys, values)]
    for j in range(4):
        h = j // 2
        to = (j + pos[4]) % 4
        lane = pos[1] * 4 + j
        pieces = [
            jnp.concatenate([w[0:4, 128 * h : 128 * h + 128] for w in wide], axis=1),
            jnp.sum(jnp.where(spots, column(rate, lane), 0.0), axis=0, keepdims=True),
            jnp.sum(jnp.where(spots, column(write, lane), 0.0), axis=0, keepdims=True),
            jnp.zeros((10, 256), F32),
        ]
        c_o[to] = jnp.concatenate(pieces, axis=0).astype(BF)


def chunk_kernel(pos, q, k, v, rate, write, rows, spike, decay, bias, m_o, r_o, o_o):
    row = lax.broadcasted_iota(jnp.int32, (256, 256), 0)
    col = lax.broadcasted_iota(jnp.int32, (256, 256), 1)
    eye = row == col
    logs = -decay[...] * softplus(rate[...]) + spike[...]
    strength = sigmoid(write[...] + bias[...])
    entry = lax.broadcasted_iota(jnp.int32, (32, 256), 0) - pos[1] * 4
    below = (row >= col).astype(F32)
    above = (row <= col).astype(F32)
    sums = (
        jnp.dot(logs, above, precision=HI, preferred_element_type=F32),
        jnp.dot(logs, below, precision=HI, preferred_element_type=F32),
    )

    def upright(line):
        return jnp.sum(jnp.where(eye, line, 0.0), axis=1, keepdims=True)

    lowers, parts = ([], [])
    for h in range(2):
        kh = k[:, 128 * h : 128 * h + 128]
        qh = q[:, 128 * h : 128 * h + 128]
        kf = kh.astype(F32)
        unit = lax.rsqrt(jnp.sum(kf * kf, axis=1, keepdims=True) + EPS)
        unit_row = jnp.sum(jnp.where(eye, unit, 0.0), axis=0, keepdims=True)
        gram = mm(kh, kh, ((1,), (1,))) * unit_row
        cross = mm(qh, kh, ((1,), (1,))) * unit_row
        for e in range(2):
            j = 2 * h + e
            total_row = jnp.sum(jnp.where(entry == j, sums[e], 0.0), axis=0, keepdims=True)
            total = upright(total_row)
            b = upright(jnp.sum(jnp.where(entry == j, strength, 0.0), axis=0, keepdims=True))
            last = total[255:256] if e == 0 else total[0:1]
            inside = row >= col if e == 0 else row <= col
            fade = jnp.where(inside, jnp.exp(jnp.where(inside, total - total_row, 0.0)), 0.0)
            lowers.append(jnp.where(eye, 0.0, (b * unit) * gram * fade))
            grown = jnp.exp(total)
            right = jnp.concatenate(
                [
                    b * v[:, 128 * h : 128 * h + 128].astype(F32),
                    (b * unit * grown) * kf,
                ],
                axis=1,
            ).astype(BF)
            faded = (kf * (unit * jnp.exp(last - total))).astype(BF)
            scores = (cross * fade).astype(BF)
            parts.append((right, faded, scores, grown * qh.astype(F32), jnp.exp(last) - 1.0))
    solved = inverse_of(lowers, row, col)
    small = lax.broadcasted_iota(jnp.int32, (128, 128), 0) == lax.broadcasted_iota(
        jnp.int32, (128, 128), 1
    )
    outs = [None, None]
    for j in range(4):
        right, faded, scores, grown_q, short = parts[j]
        both = mm(solved[j], right).astype(BF)
        maps = mm(faded, both, ((0,), (0,)))
        read = mm(scores, both)
        to = (j + pos[4]) % 4
        m_o[to, 0:128, 0:128] = (jnp.where(small, short, 0.0) - maps[:, 128:]).astype(BF)
        m_o[to, 0:128, 128:256] = maps[:, :128].astype(BF)
        h, e = divmod(j, 2)
        r_o[h, :, 128 * e : 128 * e + 128] = (grown_q - read[:, 128:]).astype(BF)
        outs[h] = read[:, :128] if e == 0 else outs[h] + read[:, :128]
    m_o[:, 128:144] = rows[...]
    o_o[:, 0:128] = outs[0]
    o_o[:, 128:256] = outs[1]


def context_state(pos, rows, rate, write, decay, bias, extra):
    row = lax.broadcasted_iota(jnp.int32, (256, 256), 0)
    col = lax.broadcasted_iota(jnp.int32, (256, 256), 1)
    eye = row == col
    lane = pos[1] * 4 + pos[0]
    inside = (row - col) * (1 - 2 * (pos[0] % 2)) >= 0
    kh = rows[:, 0:128].astype(BF)
    kf = rows[:, 0:128]
    logs = -column(decay, lane) * softplus(rate)
    strength = sigmoid(write + column(bias, lane) + column(extra, lane))
    b = jnp.sum(jnp.where(eye, strength, 0.0), axis=1, keepdims=True)
    total = jnp.sum(jnp.where(inside, logs, 0.0), axis=1, keepdims=True)
    total_row = jnp.sum(jnp.where(eye, total, 0.0), axis=0, keepdims=True)
    last = jnp.sum(logs, axis=1, keepdims=True)
    unit = lax.rsqrt(jnp.sum(kf * kf, axis=1, keepdims=True) + EPS)
    unit_row = jnp.sum(jnp.where(eye, unit, 0.0), axis=0, keepdims=True)
    fade = jnp.where(inside, jnp.exp(jnp.where(inside, total - total_row, 0.0)), 0.0)
    lower = jnp.where(
        eye, 0.0, (b * unit) * (mm(kh, kh, ((1,), (1,))) * unit_row) * fade
    )
    solved = inverse_of([lower], row, col)[0]
    fresh = mm(solved, b * rows[:, 128:256])
    faded = kf * (unit * jnp.exp(last - total))
    return mm(faded, fresh, ((0,), (0,)))


def apply_to(linear, state):
    high = state.astype(BF)
    low = (state - high.astype(F32)).astype(BF)
    both = mm(linear, jnp.concatenate([high, low], axis=1))
    n = state.shape[1]
    return both[:, :n] + both[:, n:]


def compose_kernel(pos, maps, o, *, count):
    back = pos[0] % 2
    at = back * 3
    step = 1 - 2 * back
    total = maps[at][0:128].astype(F32)
    for _ in range(3):
        at = at + step
        total = total + maps[at][0:128].astype(F32) + apply_to(maps[at][0:128, 0:128], total)
    wide = [maps[i][128:].astype(F32) for i in range(4)]
    rows = [w[0:count] for w in wide]
    gates = sum(w[count : count + 2] for w in wide)
    out = jnp.concatenate([total, *rows, gates, jnp.zeros((14, 256), F32)], axis=0).astype(BF)
    for i in range(4):
        o[i] = out


def scan_kernel(pos, high, low, own, decay, bias, extra, o):
    back = pos[0] % 2
    step = 1 - 2 * back
    wide = [high[i][128:].astype(F32) for i in range(4)]
    rows = jnp.concatenate([w[0:64] for w in wide], axis=0)
    gates = sum(w[64:66] for w in wide)
    state = context_state(
        pos, rows, gates[0:1], gates[1:2], decay[...], bias[...], extra[...]
    )
    for maps, mine in ((high, pos[2]), (low, pos[3])):
        at = back * 3
        for _ in range(3):
            m = maps[at][0:128]
            moved = state + m[:, 128:256].astype(F32) + apply_to(m[:, 0:128], state)
            state = jnp.where((mine - at) * step > 0, moved, state)
            at = at + step
    at = back * 3
    for i in range(4):
        o[at] = state.astype(BF)
        if i < 3:
            m = own[at][0:128]
            state = state + m[:, 128:256].astype(F32) + apply_to(m[:, 0:128], state)
        at = at + step


def read_kernel(pos, states, reads, base, gain, weight, o):
    heads = []
    for h in range(2):
        first = states[(2 * h + pos[4]) % 4]
        second = states[(2 * h + 1 + pos[4]) % 4]
        total = base[:, 128 * h : 128 * h + 128] + (
            mm(reads[h][:, 0:128], first) + mm(reads[h][:, 128:256], second)
        )
        mean = jnp.mean(total * total, axis=1, keepdims=True)
        heads.append((total * lax.rsqrt(mean + EPS) * gain[...]).astype(BF))
    branch = mm(jnp.concatenate(heads, axis=1), weight[...]).astype(BF)
    for t in range(8):
        o[t] = branch[32 * t : 32 * t + 32]


def output_kernel(rows, fac, lat, o):
    branch = rows[0].astype(F32)
    for i in range(1, 8):
        branch = branch + rows[i].astype(F32)
    gates = []
    for t in range(8):
        f = (fac[t] + fac[8 + t]) + (fac[16 + t] + fac[24 + t])
        gates.append(f[2:3])
    gate = jnp.concatenate(gates, axis=1)
    o[...] = (lat[...].astype(F32) + gate * branch).astype(BF)


def call(kernel, outs, specs, scratch=(), flops=1):
    def shape(s):
        return jax.ShapeDtypeStruct(*s)

    many = isinstance(outs, list)
    return pl.pallas_call(
        kernel,
        out_shape=[shape(s) for s in outs] if many else shape(outs),
        in_specs=specs,
        out_specs=[VM] * len(outs) if many else VM,
        scratch_shapes=scratch,
        compiler_params=pltpu.CompilerParams(vmem_limit_bytes=24 * 2**20),
        cost_estimate=pl.CostEstimate(flops=flops, bytes_accessed=1, transcendentals=0),
    )


def to_all(value, axes, count):
    return lax.all_to_all(
        jnp.broadcast_to(value[None], (count, *value.shape)), axes, 0, 0, tiled=True
    )


def per_device(
    latent,
    condition,
    context,
    context_condition_vector,
    modulation_matrix,
    query_matrix,
    key_matrix,
    value_matrix,
    decay_input_weight,
    write_strength_weight,
    head_decay_rate,
    write_strength_bias,
    context_write_offset_bias,
    log_spike_added,
    head_norm_gain,
    output_matrix,
):
    zh, zl, y = (lax.axis_index("zh"), lax.axis_index("zl"), lax.axis_index("y"))
    x, c = (lax.axis_index("x"), lax.axis_index("c"))
    sp_index = lax.axis_index(SP)
    pos = jnp.stack([(y + c) % 4, x * 2 + c, zh, zl, (4 - c) % 4, sp_index * 4, c, x])
    pos = pos.astype(jnp.int32)
    parts = [latent]
    for d in range(1, 4):
        parts.append(lax.ppermute(latent, "x", [(i, (i + d) % 4) for i in range(4)]))
    mine = jnp.stack(parts)
    other = lax.ppermute(mine, "c", [(0, 1), (1, 0)])
    signals = jnp.stack([condition, context_condition_vector])
    signals = lax.dynamic_slice_in_dim(jax.nn.silu(signals), sp_index * 32, 32, 1)
    mod = modulation_matrix.astype(F32)
    part = jnp.concatenate(
        [
            jnp.sum(mod * signals[0][None, :, None], axis=1),
            jnp.sum(mod[:2] * signals[1][None, :, None], axis=1),
        ]
    )
    part = to_all(part, Z, 16)
    part = jnp.sum(part, axis=0)
    fac = to_all(part, ("y", "x", "c"), 32)

    queries, keys, values, rate, write, rows = call(
        project_kernel,
        [
            ((256, 256), BF),
            ((256, 256), BF),
            ((256, 256), BF),
            ((32, 256), F32),
            ((32, 256), F32),
            ((4, 16, 256), BF),
        ],
        [SM] + [VM] * 9,
        [pltpu.VMEM((272, D), BF)],
        flops=10**9,
    )(
        pos,
        mine,
        other,
        context,
        fac,
        query_matrix,
        key_matrix,
        value_matrix,
        decay_input_weight.T,
        write_strength_weight.T,
    )
    maps, reads, base = call(
        chunk_kernel,
        [((4, 144, 256), BF), ((2, 256, 256), BF), ((256, 256), F32)],
        [SM] + [VM] * 9,
        flops=4 * 10**9,
    )(
        pos,
        queries,
        keys,
        values,
        rate,
        write,
        rows,
        log_spike_added.T,
        head_decay_rate.reshape(32, 1),
        write_strength_bias.reshape(32, 1),
    )
    of_y = lax.all_to_all(maps, "y", 0, 0, tiled=True)
    low = call(partial(compose_kernel, count=4), ((4, 160, 256), BF), [SM, VM])(pos, of_y)
    of_low = lax.all_to_all(low, "zl", 0, 0, tiled=True)
    high = call(partial(compose_kernel, count=16), ((4, 208, 256), BF), [SM, VM])(pos, of_low)
    of_high = lax.all_to_all(high, "zh", 0, 0, tiled=True)
    states = call(scan_kernel, ((4, 128, 128), BF), [SM] + [VM] * 6, flops=10**8)(
        pos,
        of_high,
        of_low,
        of_y,
        head_decay_rate.reshape(1, 32),
        write_strength_bias.reshape(1, 32),
        context_write_offset_bias.reshape(1, 32),
    )
    states = lax.all_to_all(states, "y", 0, 0, tiled=True)
    branch = call(read_kernel, ((8, 32, D), BF), [SM] + [VM] * 5, flops=10**8)(
        pos, states, reads, base, head_norm_gain.reshape(1, 128), output_matrix
    )
    branch = lax.all_to_all(branch, TP, 0, 0, tiled=True)
    return call(output_kernel, ((32, D), BF), [VM] * 3, flops=10**8)(branch, fac, latent)


def solution(mesh):
    split = Mesh(mesh.devices.reshape(4, 4, 4, 4, 2), ALL)
    return jax.shard_map(
        per_device,
        mesh=split,
        in_specs=(
            P(ALL, None),
            P(),
            P(SP, None),
            P(),
            P(None, SP, TP),
            P(None, TP),
            P(None, TP),
            P(None, TP),
            P(),
            P(),
            P(),
            P(),
            P(),
            P(SP, None),
            P(),
            P(TP, None),
        ),
        out_specs=P(ALL, None),
        check_vma=False,
    )
```

```python
import jax
import jax.numpy as jnp
from jax import lax
from jax.experimental import pallas as pl
from jax.experimental.pallas import tpu as pltpu
from jax.sharding import Mesh
from jax.sharding import PartitionSpec as P


D = 2048
EPS = 1e-06
HI = lax.Precision.HIGHEST
F32 = jnp.float32
BF = jnp.bfloat16
Z = ("zh", "zl")
TP = ("x", "c")
SP = ("zh", "zl", "y")
ALL = ("zh", "zl", "y", "x", "c")
VM = pl.BlockSpec(memory_space=pltpu.VMEM)
SM = pl.BlockSpec(memory_space=pltpu.SMEM)
HB = pl.BlockSpec(memory_space=pltpu.HBM)


def mm(a, b, dims=((1,), (0,))):
    return lax.dot_general(
        a.astype(BF), b.astype(BF), (dims, ((), ())), preferred_element_type=F32
    )


def norm_rows(rows, scale, shift):
    wide = rows.astype(F32)
    centred = wide - jnp.mean(wide, axis=-1, keepdims=True)
    spread = jnp.mean(centred * centred, axis=-1, keepdims=True)
    return (centred * lax.rsqrt(spread + EPS) * (1.0 + scale) + shift).astype(BF)


def column(matrix, lane):
    lanes = lax.broadcasted_iota(jnp.int32, matrix.shape, 1)
    return jnp.sum(jnp.where(lanes == lane, matrix, 0.0), axis=1, keepdims=True)


def softplus(t):
    return jnp.maximum(t, 0.0) + jnp.log1p(jnp.exp(-jnp.abs(t)))


def sigmoid(t):
    return 1.0 / (1.0 + jnp.exp(-t))


def inverse_of(lower, row, col):
    eye = (row == col).astype(F32)
    own = (row // 16) == (col // 16)
    base = [jnp.where(own, m, 0.0) for m in lower]
    inv = [eye - m for m in base]
    power = [mm(m, m) for m in base]
    for step in range(3):
        inv = [p + mm(p, x) for p, x in zip(inv, power)]
        if step < 2:
            power = [mm(x, x) for x in power]
    size = 16
    while size < 256:
        here = ((row // (2 * size)) == (col // (2 * size))) & ((row // size) != (col // size))
        side = [mm(jnp.where(here, m, 0.0), p) for m, p in zip(lower, inv)]
        inv = [p - mm(p, s) for p, s in zip(inv, side)]
        size *= 2
    out = []
    for m, p in zip(lower, inv):
        first = p.astype(BF)
        high = m.astype(BF)
        low = (m - high.astype(F32)).astype(BF)
        wide = first.astype(F32)
        left = (eye - wide) - (mm(high, first) + mm(low, first))
        out.append(wide + mm(first, left))
    return out


def project_kernel(
    pos, p0, p1, p2, p3, fac, wq, wk, wv_h, wd_h, ww_h, ctx_h,
    q_o, k_o, v_o, r_o, w_o, c_o,
    hid, wv, wd, ww, ctx, sems,
):
    copies = [
        pltpu.make_async_copy(source, target, sems.at[i])
        for i, (source, target) in enumerate(((ctx_h, ctx), (wv_h, wv), (wd_h, wd), (ww_h, ww)))
    ]
    for copy in copies:
        copy.start()
    factors = [[], [], [], []]
    for t in range(8):
        f = (fac[t] + fac[8 + t]) + (fac[16 + t] + fac[24 + t])
        for slot, r in enumerate((0, 1, 3, 4)):
            factors[slot].append(f[r : r + 1])
    shift, scale, c_shift, c_scale = (jnp.concatenate(f, axis=1) for f in factors)
    for d, pair in enumerate((p0, p1, p2, p3)):
        for i in range(2):
            core = pos[6] if i == 0 else 1 - pos[6]
            spot = (2 * ((pos[7] + 4 - d) % 4) + core) * 32
            hid[pl.ds(pl.multiple_of(spot, 32), 32)] = norm_rows(pair[i], scale, shift)
    copies[0].wait()
    hid[256:260] = norm_rows(ctx[...], c_scale, c_shift)
    hid[260:272] = jnp.zeros((12, D), BF)
    rows = hid[...]
    q_o[...] = mm(hid[0:256], wq[...]).astype(BF)
    keys = mm(rows, wk[...]).astype(BF)
    k_o[...] = keys[:256]
    for copy in copies[1:]:
        copy.wait()
    values = mm(rows, wv[...]).astype(BF)
    v_o[...] = values[:256]
    last_two = ((1,), (1,))
    r_o[...] = mm(wd[...], hid[0:256], last_two).astype(BF).astype(F32)
    w_o[...] = mm(ww[...], hid[0:256], last_two).astype(BF).astype(F32)
    rate = mm(hid[256:264], wd[...], last_two).astype(BF).astype(F32)
    write = mm(hid[256:264], ww[...], last_two).astype(BF).astype(F32)
    lanes = lax.broadcasted_iota(jnp.int32, (8, 256), 1)
    rank = lax.broadcasted_iota(jnp.int32, (8, 256), 0)
    spots = (lanes == rank + pos[5]) & (rank < 4)
    wide = [rows_of[256:264].astype(F32)[0:4] for rows_of in (keys, values)]
    pieces = [jnp.concatenate(wide, axis=1)]
    for j in range(4):
        lane = pos[1] * 4 + j
        gates = [
            jnp.sum(jnp.where(spots, column(g, lane), 0.0), axis=0, keepdims=True)
            for g in (rate, write)
        ]
        pieces.append(jnp.concatenate(gates, axis=1))
    out = jnp.concatenate(pieces, axis=0).astype(BF)
    for i in range(4):
        c_o[i] = out


def chunk_kernel(pos, q, k, v, rate, write, spike, decay, bias, m_o, r_o, o_o):
    row = lax.broadcasted_iota(jnp.int32, (256, 256), 0)
    col = lax.broadcasted_iota(jnp.int32, (256, 256), 1)
    eye = row == col
    logs = -decay[...] * softplus(rate[...]) + spike[...]
    strength = sigmoid(write[...] + bias[...])
    entry = lax.broadcasted_iota(jnp.int32, (32, 256), 0) - pos[1] * 4
    below = (row >= col).astype(F32)
    above = (row <= col).astype(F32)
    sums = (
        jnp.dot(logs, above, precision=HI, preferred_element_type=F32),
        jnp.dot(logs, below, precision=HI, preferred_element_type=F32),
    )

    def upright(line):
        return jnp.sum(jnp.where(eye, line, 0.0), axis=1, keepdims=True)

    lowers, parts = ([], [])
    for h in range(2):
        kh = k[:, 128 * h : 128 * h + 128]
        qh = q[:, 128 * h : 128 * h + 128]
        kf = kh.astype(F32)
        unit = lax.rsqrt(jnp.sum(kf * kf, axis=1, keepdims=True) + EPS)
        unit_row = jnp.sum(jnp.where(eye, unit, 0.0), axis=0, keepdims=True)
        gram = mm(kh, kh, ((1,), (1,))) * unit_row
        cross = mm(qh, kh, ((1,), (1,))) * unit_row
        for e in range(2):
            j = 2 * h + e
            total_row = jnp.sum(jnp.where(entry == j, sums[e], 0.0), axis=0, keepdims=True)
            total = upright(total_row)
            b = upright(jnp.sum(jnp.where(entry == j, strength, 0.0), axis=0, keepdims=True))
            last = total[255:256] if e == 0 else total[0:1]
            inside = row >= col if e == 0 else row <= col
            fade = jnp.where(inside, jnp.exp(jnp.where(inside, total - total_row, 0.0)), 0.0)
            lowers.append(jnp.where(eye, 0.0, (b * unit) * gram * fade))
            grown = jnp.exp(total)
            right = jnp.concatenate(
                [
                    b * v[:, 128 * h : 128 * h + 128].astype(F32),
                    (b * unit * grown) * kf,
                ],
                axis=1,
            ).astype(BF)
            faded = (kf * (unit * jnp.exp(last - total))).astype(BF)
            scores = (cross * fade).astype(BF)
            parts.append((right, faded, scores, grown * qh.astype(F32), jnp.exp(last) - 1.0))
    solved = inverse_of(lowers, row, col)
    small = lax.broadcasted_iota(jnp.int32, (128, 128), 0) == lax.broadcasted_iota(
        jnp.int32, (128, 128), 1
    )
    outs = [None, None]
    for j in range(4):
        right, faded, scores, grown_q, short = parts[j]
        both = mm(solved[j], right).astype(BF)
        maps = mm(faded, both, ((0,), (0,)))
        read = mm(scores, both)
        to = (j + pos[4]) % 4
        m_o[to, 0:128, 0:128] = (jnp.where(small, short, 0.0) - maps[:, 128:]).astype(BF)
        m_o[to, 0:128, 128:256] = maps[:, :128].astype(BF)
        h, e = divmod(j, 2)
        r_o[h, :, 128 * e : 128 * e + 128] = (grown_q - read[:, 128:]).astype(BF)
        outs[h] = read[:, :128] if e == 0 else outs[h] + read[:, :128]
    m_o[:, 128:160] = jnp.zeros((4, 32, 256), BF)
    o_o[:, 0:128] = outs[0]
    o_o[:, 128:256] = outs[1]


def context_state(pos, rows, rate, write, decay, bias, extra):
    row = lax.broadcasted_iota(jnp.int32, (256, 256), 0)
    col = lax.broadcasted_iota(jnp.int32, (256, 256), 1)
    eye = row == col
    lane = pos[1] * 4 + pos[0]
    inside = (row - col) * (1 - 2 * (pos[0] % 2)) >= 0
    kh = rows[:, 0:128].astype(BF)
    kf = rows[:, 0:128]
    logs = -column(decay, lane) * softplus(rate)
    strength = sigmoid(write + column(bias, lane) + column(extra, lane))
    b = jnp.sum(jnp.where(eye, strength, 0.0), axis=1, keepdims=True)
    total = jnp.sum(jnp.where(inside, logs, 0.0), axis=1, keepdims=True)
    total_row = jnp.sum(jnp.where(eye, total, 0.0), axis=0, keepdims=True)
    last = jnp.sum(logs, axis=1, keepdims=True)
    unit = lax.rsqrt(jnp.sum(kf * kf, axis=1, keepdims=True) + EPS)
    unit_row = jnp.sum(jnp.where(eye, unit, 0.0), axis=0, keepdims=True)
    fade = jnp.where(inside, jnp.exp(jnp.where(inside, total - total_row, 0.0)), 0.0)
    lower = jnp.where(
        eye, 0.0, (b * unit) * (mm(kh, kh, ((1,), (1,))) * unit_row) * fade
    )
    solved = inverse_of([lower], row, col)[0]
    fresh = mm(solved, b * rows[:, 128:256])
    faded = kf * (unit * jnp.exp(last - total))
    return mm(faded, fresh, ((0,), (0,)))


def apply_to(linear, state):
    high = state.astype(BF)
    low = (state - high.astype(F32)).astype(BF)
    both = mm(linear, jnp.concatenate([high, low], axis=1))
    n = state.shape[1]
    return both[:, :n] + both[:, n:]


def pack_kernel(pos, maps, rows, o):
    wide = [rows[i].astype(F32) for i in range(4)]
    for j in range(4):
        h = j // 2
        to = (j + pos[4]) % 4
        parts = []
        for w in wide:
            sides = [w[0:4, at + 128 * h : at + 128 * h + 128] for at in (0, 256)]
            parts.append(jnp.concatenate(sides, axis=1))
        gates = sum(w[4 + j : 5 + j] for w in wide)
        parts += [gates[:, 0:256], gates[:, 256:512], jnp.zeros((14, 256), F32)]
        o[to, 128:160] = jnp.concatenate(parts, axis=0).astype(BF)


def composed(pos, maps):
    back = pos[0] % 2
    at = back * 3
    step = 1 - 2 * back
    total = maps[at][0:128].astype(F32)
    for _ in range(3):
        at = at + step
        total = total + maps[at][0:128].astype(F32) + apply_to(maps[at][0:128, 0:128], total)
    return total


def low_kernel(pos, maps, o):
    total = composed(pos, maps)
    wide = [maps[i][128:].astype(F32) for i in range(4)]
    parts = [w[4 * i : 4 * i + 4] for i in range(4) for w in wide]
    parts += [sum(w[16:18] for w in wide), jnp.zeros((14, 256), F32)]
    out = jnp.concatenate([total, *parts], axis=0).astype(BF)
    for i in range(4):
        o[i] = out


def high_kernel(pos, maps, o):
    o[...] = composed(pos, maps).astype(BF)


def context_kernel(pos, low, decay, bias, extra, o):
    wide = [low[i][128:].astype(F32) for i in range(4)]
    rows = jnp.concatenate([w[16 * i : 16 * i + 16] for i in range(4) for w in wide], axis=0)
    gates = sum(w[64:66] for w in wide)
    o[...] = context_state(
        pos, rows, gates[0:1], gates[1:2], decay[...], bias[...], extra[...]
    )


def moved(maps, state):
    return state + maps[:, 128:256].astype(F32) + apply_to(maps[:, 0:128], state)


def scan_kernel(pos, start, far, middle, near, low, own, o):
    back = pos[0] % 2
    step = 1 - 2 * back
    state = start[...]
    for maps in (far, middle, near):
        state = moved(maps[...], state)
    at = back * 3
    for _ in range(3):
        state = jnp.where((pos[3] - at) * step > 0, moved(low[at][0:128], state), state)
        at = at + step
    at = back * 3
    for i in range(4):
        o[at] = state.astype(BF)
        if i < 3:
            state = moved(own[at][0:128], state)
        at = at + step


def read_kernel(pos, states, reads, base, gain, weight, o):
    heads = []
    for h in range(2):
        first = states[(2 * h + pos[4]) % 4]
        second = states[(2 * h + 1 + pos[4]) % 4]
        total = base[:, 128 * h : 128 * h + 128] + (
            mm(reads[h][:, 0:128], first) + mm(reads[h][:, 128:256], second)
        )
        mean = jnp.mean(total * total, axis=1, keepdims=True)
        heads.append((total * lax.rsqrt(mean + EPS) * gain[...]).astype(BF))
    branch = mm(jnp.concatenate(heads, axis=1), weight[...]).astype(BF)
    for t in range(8):
        o[t] = branch[32 * t : 32 * t + 32]


def output_kernel(rows, fac, lat, o):
    branch = rows[0].astype(F32)
    for i in range(1, 8):
        branch = branch + rows[i].astype(F32)
    gates = []
    for t in range(8):
        f = (fac[t] + fac[8 + t]) + (fac[16 + t] + fac[24 + t])
        gates.append(f[2:3])
    gate = jnp.concatenate(gates, axis=1)
    o[...] = (lat[...].astype(F32) + gate * branch).astype(BF)


def call(kernel, outs, specs, scratch=(), flops=1, aliases=None):
    def shape(s):
        return jax.ShapeDtypeStruct(*s)

    many = isinstance(outs, list)
    return pl.pallas_call(
        kernel,
        out_shape=[shape(s) for s in outs] if many else shape(outs),
        in_specs=specs,
        out_specs=[VM] * len(outs) if many else VM,
        scratch_shapes=scratch,
        input_output_aliases=aliases or {},
        compiler_params=pltpu.CompilerParams(vmem_limit_bytes=24 * 2**20),
        cost_estimate=pl.CostEstimate(flops=flops, bytes_accessed=1, transcendentals=0),
    )


def to_all(value, axes, count):
    return lax.all_to_all(
        jnp.broadcast_to(value[None], (count, *value.shape)), axes, 0, 0, tiled=True
    )


def onward(d):
    pairs = []
    for zh in range(4):
        for y in range(4):
            for c in range(2):
                to = zh + d if (y + c) % 2 == 0 else zh - d
                if 0 <= to < 4:
                    pairs.append((zh * 8 + y * 2 + c, to * 8 + y * 2 + c))
    return pairs


def per_device(
    latent,
    condition,
    context,
    context_condition_vector,
    modulation_matrix,
    query_matrix,
    key_matrix,
    value_matrix,
    decay_input_weight,
    write_strength_weight,
    head_decay_rate,
    write_strength_bias,
    context_write_offset_bias,
    log_spike_added,
    head_norm_gain,
    output_matrix,
):
    zh, zl, y = (lax.axis_index("zh"), lax.axis_index("zl"), lax.axis_index("y"))
    x, c = (lax.axis_index("x"), lax.axis_index("c"))
    sp_index = lax.axis_index(SP)
    pos = jnp.stack([(y + c) % 4, x * 2 + c, zh, zl, (4 - c) % 4, sp_index * 4, c, x])
    pos = pos.astype(jnp.int32)
    other = lax.ppermute(latent, "c", [(0, 1), (1, 0)])
    pairs = [jnp.stack([latent, other])]
    for d in range(1, 4):
        pairs.append(lax.ppermute(pairs[0], "x", [(i, (i + d) % 4) for i in range(4)]))
    signals = jnp.stack([condition, context_condition_vector])
    signals = lax.dynamic_slice_in_dim(jax.nn.silu(signals), sp_index * 32, 32, 1)
    mod = modulation_matrix.astype(F32)
    part = jnp.concatenate(
        [
            jnp.sum(mod * signals[0][None, :, None], axis=1),
            jnp.sum(mod[:2] * signals[1][None, :, None], axis=1),
        ]
    )
    part = to_all(part, Z, 16)
    part = jnp.sum(part, axis=0)
    fac = to_all(part, ("y", "x", "c"), 32)

    queries, keys, values, rate, write, rows = call(
        project_kernel,
        [
            ((256, 256), BF),
            ((256, 256), BF),
            ((256, 256), BF),
            ((32, 256), F32),
            ((32, 256), F32),
            ((4, 8, 512), BF),
        ],
        [SM] + [VM] * 7 + [HB] * 4,
        [
            pltpu.VMEM((272, D), BF),
            pltpu.VMEM((D, 256), BF),
            pltpu.VMEM((32, D), BF),
            pltpu.VMEM((32, D), BF),
            pltpu.VMEM((4, D), BF),
            pltpu.SemaphoreType.DMA((4,)),
        ],
        flops=10**9,
    )(
        pos,
        *pairs,
        fac,
        query_matrix,
        key_matrix,
        value_matrix,
        decay_input_weight.T,
        write_strength_weight.T,
        context,
    )
    rows = lax.all_to_all(rows, "zh", 0, 0, tiled=True)
    maps, reads, base = call(
        chunk_kernel,
        [((4, 160, 256), BF), ((2, 256, 256), BF), ((256, 256), F32)],
        [SM] + [VM] * 8,
        flops=4 * 10**9,
    )(
        pos,
        queries,
        keys,
        values,
        rate,
        write,
        log_spike_added.T,
        head_decay_rate.reshape(32, 1),
        write_strength_bias.reshape(32, 1),
    )
    maps = call(pack_kernel, ((4, 160, 256), BF), [SM, VM, VM], aliases={1: 0})(
        pos, maps, rows
    )
    of_y = lax.all_to_all(maps, "y", 0, 0, tiled=True)
    low = call(low_kernel, ((4, 208, 256), BF), [SM, VM])(pos, of_y)
    of_low = lax.all_to_all(low, "zl", 0, 0, tiled=True)
    high = call(high_kernel, ((128, 256), BF), [SM, VM])(pos, of_low)
    of_high = []
    for d in (3, 2, 1):
        of_high.append(lax.ppermute(high, ("zh", "y", "c"), onward(d)))
    start = call(context_kernel, ((128, 128), F32), [SM] + [VM] * 4, flops=10**9)(
        pos,
        of_low,
        head_decay_rate.reshape(1, 32),
        write_strength_bias.reshape(1, 32),
        context_write_offset_bias.reshape(1, 32),
    )
    states = call(scan_kernel, ((4, 128, 128), BF), [SM] + [VM] * 6, flops=10**8)(
        pos, start, *of_high, of_low, of_y
    )
    states = lax.all_to_all(states, "y", 0, 0, tiled=True)
    branch = call(read_kernel, ((8, 32, D), BF), [SM] + [VM] * 5, flops=10**8)(
        pos, states, reads, base, head_norm_gain.reshape(1, 128), output_matrix
    )
    branch = lax.all_to_all(branch, TP, 0, 0, tiled=True)
    return call(output_kernel, ((32, D), BF), [VM] * 3, flops=10**8)(branch, fac, latent)


def solution(mesh):
    split = Mesh(mesh.devices.reshape(4, 4, 4, 4, 2), ALL)
    return jax.shard_map(
        per_device,
        mesh=split,
        in_specs=(
            P(ALL, None),
            P(),
            P(SP, None),
            P(),
            P(None, SP, TP),
            P(None, TP),
            P(None, TP),
            P(None, TP),
            P(),
            P(),
            P(),
            P(),
            P(),
            P(SP, None),
            P(),
            P(TP, None),
        ),
        out_specs=P(ALL, None),
        check_vma=False,
    )
```

```python
import jax
import jax.numpy as jnp
from jax import lax
from jax.experimental import pallas as pl
from jax.experimental.pallas import tpu as pltpu
from jax.sharding import Mesh
from jax.sharding import PartitionSpec as P


D = 2048
EPS = 1e-06
HI = lax.Precision.HIGHEST
F32 = jnp.float32
BF = jnp.bfloat16
Z = ("zh", "zl")
TP = ("x", "c")
SP = ("zh", "zl", "y")
ALL = ("zh", "zl", "y", "x", "c")
VM = pl.BlockSpec(memory_space=pltpu.VMEM)
SM = pl.BlockSpec(memory_space=pltpu.SMEM)
HB = pl.BlockSpec(memory_space=pltpu.HBM)


def mm(a, b, dims=((1,), (0,))):
    return lax.dot_general(
        a.astype(BF), b.astype(BF), (dims, ((), ())), preferred_element_type=F32
    )


def norm_rows(rows, scale, shift):
    wide = rows.astype(F32)
    centred = wide - jnp.mean(wide, axis=-1, keepdims=True)
    spread = jnp.mean(centred * centred, axis=-1, keepdims=True)
    return (centred * lax.rsqrt(spread + EPS) * (1.0 + scale) + shift).astype(BF)


def column(matrix, lane):
    lanes = lax.broadcasted_iota(jnp.int32, matrix.shape, 1)
    return jnp.sum(jnp.where(lanes == lane, matrix, 0.0), axis=1, keepdims=True)


def softplus(t):
    return jnp.maximum(t, 0.0) + jnp.log1p(jnp.exp(-jnp.abs(t)))


def sigmoid(t):
    return 1.0 / (1.0 + jnp.exp(-t))


def inverse_of(lower, row, col):
    eye = (row == col).astype(F32)
    own = (row // 16) == (col // 16)
    base = [jnp.where(own, m, 0.0) for m in lower]
    inv = [eye - m for m in base]
    power = [mm(m, m) for m in base]
    for step in range(3):
        inv = [p + mm(p, x) for p, x in zip(inv, power)]
        if step < 2:
            power = [mm(x, x) for x in power]
    size = 16
    while size < 256:
        here = ((row // (2 * size)) == (col // (2 * size))) & ((row // size) != (col // size))
        side = [mm(jnp.where(here, m, 0.0), p) for m, p in zip(lower, inv)]
        inv = [p - mm(p, s) for p, s in zip(inv, side)]
        size *= 2
    out = []
    for m, p in zip(lower, inv):
        first = p.astype(BF)
        high = m.astype(BF)
        low = (m - high.astype(F32)).astype(BF)
        wide = first.astype(F32)
        left = (eye - wide) - (mm(high, first) + mm(low, first))
        out.append(wide + mm(first, left))
    return out


def project_kernel(
    pos, one, two, fac, wq, wk, wv_h, wd_h, ww_h, ctx_h,
    p_o, c_o,
    hid, wv, wd, ww, ctx, sems,
):
    copies = [
        pltpu.make_async_copy(source, target, sems.at[i])
        for i, (source, target) in enumerate(((ctx_h, ctx), (wv_h, wv), (wd_h, wd), (ww_h, ww)))
    ]
    for copy in copies:
        copy.start()
    factors = [[], [], [], []]
    for t in range(8):
        f = (fac[t] + fac[8 + t]) + (fac[16 + t] + fac[24 + t])
        for slot, r in enumerate((0, 1, 3, 4)):
            factors[slot].append(f[r : r + 1])
    shift, scale, c_shift, c_scale = (jnp.concatenate(f, axis=1) for f in factors)
    for x in range(4):
        for i, lat in enumerate((one, two)):
            core = pos[6] if i == 0 else 1 - pos[6]
            spot = (2 * x + core) * 32
            hid[pl.ds(pl.multiple_of(spot, 32), 32)] = norm_rows(lat[x], scale, shift)
    copies[0].wait()
    hid[256:260] = norm_rows(ctx[...], c_scale, c_shift)
    hid[260:272] = jnp.zeros((12, D), BF)
    rows = hid[...]
    p_o[0:256] = mm(hid[0:256], wq[...]).astype(BF)
    keys = mm(rows, wk[...]).astype(BF)
    p_o[256:512] = keys[:256]
    for copy in copies[1:]:
        copy.wait()
    values = mm(rows, wv[...]).astype(BF)
    p_o[512:768] = values[:256]
    last_two = ((1,), (1,))
    p_o[768:800] = mm(wd[...], hid[0:256], last_two).astype(BF)
    p_o[800:832] = mm(ww[...], hid[0:256], last_two).astype(BF)
    rate = mm(hid[256:264], wd[...], last_two).astype(BF).astype(F32)
    write = mm(hid[256:264], ww[...], last_two).astype(BF).astype(F32)
    lanes = lax.broadcasted_iota(jnp.int32, (8, 256), 1)
    rank = lax.broadcasted_iota(jnp.int32, (8, 256), 0)
    spots = (lanes == rank + pos[5]) & (rank < 4)
    wide = [rows_of[256:264].astype(F32)[0:4] for rows_of in (keys, values)]
    pieces = [jnp.concatenate(wide, axis=1)]
    for j in range(4):
        lane = pos[1] * 4 + j
        gates = [
            jnp.sum(jnp.where(spots, column(g, lane), 0.0), axis=0, keepdims=True)
            for g in (rate, write)
        ]
        pieces.append(jnp.concatenate(gates, axis=1))
    out = jnp.concatenate(pieces, axis=0).astype(BF)
    for i in range(4):
        c_o[i] = out


def chunk_kernel(pos, packed, spike, small, m_o, r_o, o_o):
    row = lax.broadcasted_iota(jnp.int32, (256, 256), 0)
    col = lax.broadcasted_iota(jnp.int32, (256, 256), 1)
    eye = row == col
    entry = lax.broadcasted_iota(jnp.int32, (32, 128), 0)
    entry = entry == lax.broadcasted_iota(jnp.int32, (32, 128), 1)
    decay, bias = (
        jnp.sum(jnp.where(entry, small[i : i + 1], 0.0), axis=1, keepdims=True) for i in range(2)
    )
    logs = -decay * softplus(packed[768:800].astype(F32)) + spike[...]
    strength = sigmoid(packed[800:832].astype(F32) + bias)
    entry = lax.broadcasted_iota(jnp.int32, (32, 256), 0) - pos[1] * 4
    below = (row >= col).astype(F32)
    above = (row <= col).astype(F32)
    sums = (
        jnp.dot(logs, above, precision=HI, preferred_element_type=F32),
        jnp.dot(logs, below, precision=HI, preferred_element_type=F32),
    )

    def upright(line):
        return jnp.sum(jnp.where(eye, line, 0.0), axis=1, keepdims=True)

    lowers, parts = ([], [])
    for h in range(2):
        qh, kh, vh = (packed[256 * i : 256 * i + 256, 128 * h : 128 * h + 128] for i in range(3))
        kf = kh.astype(F32)
        unit = lax.rsqrt(jnp.sum(kf * kf, axis=1, keepdims=True) + EPS)
        unit_row = jnp.sum(jnp.where(eye, unit, 0.0), axis=0, keepdims=True)
        gram = mm(kh, kh, ((1,), (1,))) * unit_row
        cross = mm(qh, kh, ((1,), (1,))) * unit_row
        for e in range(2):
            j = 2 * h + e
            total_row = jnp.sum(jnp.where(entry == j, sums[e], 0.0), axis=0, keepdims=True)
            total = upright(total_row)
            b = upright(jnp.sum(jnp.where(entry == j, strength, 0.0), axis=0, keepdims=True))
            last = total[255:256] if e == 0 else total[0:1]
            inside = row >= col if e == 0 else row <= col
            fade = jnp.where(inside, jnp.exp(jnp.where(inside, total - total_row, 0.0)), 0.0)
            lowers.append(jnp.where(eye, 0.0, (b * unit) * gram * fade))
            grown = jnp.exp(total)
            right = jnp.concatenate(
                [
                    b * vh.astype(F32),
                    (b * unit * grown) * kf,
                ],
                axis=1,
            ).astype(BF)
            faded = (kf * (unit * jnp.exp(last - total))).astype(BF)
            scores = (cross * fade).astype(BF)
            parts.append((right, faded, scores, grown * qh.astype(F32), jnp.exp(last) - 1.0))
    solved = inverse_of(lowers, row, col)
    small = lax.broadcasted_iota(jnp.int32, (128, 128), 0) == lax.broadcasted_iota(
        jnp.int32, (128, 128), 1
    )
    outs = [None, None]
    for j in range(4):
        right, faded, scores, grown_q, short = parts[j]
        both = mm(solved[j], right).astype(BF)
        maps = mm(faded, both, ((0,), (0,)))
        read = mm(scores, both)
        to = (j + pos[4]) % 4
        m_o[to, 0:128, 0:128] = (jnp.where(small, short, 0.0) - maps[:, 128:]).astype(BF)
        m_o[to, 0:128, 128:256] = maps[:, :128].astype(BF)
        h, e = divmod(j, 2)
        r_o[h, :, 128 * e : 128 * e + 128] = (grown_q - read[:, 128:]).astype(BF)
        outs[h] = read[:, :128] if e == 0 else outs[h] + read[:, :128]
    m_o[:, 128:160] = jnp.zeros((4, 32, 256), BF)
    o_o[:, 0:128] = outs[0]
    o_o[:, 128:256] = outs[1]


def context_state(pos, rows, rate, write, decay, bias, extra):
    row = lax.broadcasted_iota(jnp.int32, (256, 256), 0)
    col = lax.broadcasted_iota(jnp.int32, (256, 256), 1)
    eye = row == col
    lane = pos[1] * 4 + pos[0]
    inside = (row - col) * (1 - 2 * (pos[0] % 2)) >= 0
    kh = rows[:, 0:128].astype(BF)
    kf = rows[:, 0:128]
    logs = -column(decay, lane) * softplus(rate)
    strength = sigmoid(write + column(bias, lane) + column(extra, lane))
    b = jnp.sum(jnp.where(eye, strength, 0.0), axis=1, keepdims=True)
    total = jnp.sum(jnp.where(inside, logs, 0.0), axis=1, keepdims=True)
    total_row = jnp.sum(jnp.where(eye, total, 0.0), axis=0, keepdims=True)
    last = jnp.sum(logs, axis=1, keepdims=True)
    unit = lax.rsqrt(jnp.sum(kf * kf, axis=1, keepdims=True) + EPS)
    unit_row = jnp.sum(jnp.where(eye, unit, 0.0), axis=0, keepdims=True)
    fade = jnp.where(inside, jnp.exp(jnp.where(inside, total - total_row, 0.0)), 0.0)
    lower = jnp.where(
        eye, 0.0, (b * unit) * (mm(kh, kh, ((1,), (1,))) * unit_row) * fade
    )
    solved = inverse_of([lower], row, col)[0]
    fresh = mm(solved, b * rows[:, 128:256])
    faded = kf * (unit * jnp.exp(last - total))
    return mm(faded, fresh, ((0,), (0,)))


def apply_to(linear, state):
    high = state.astype(BF)
    low = (state - high.astype(F32)).astype(BF)
    both = mm(linear, jnp.concatenate([high, low], axis=1))
    n = state.shape[1]
    return both[:, :n] + both[:, n:]


def pack_kernel(pos, maps, rows, o):
    wide = [rows[i].astype(F32) for i in range(4)]
    for j in range(4):
        h = j // 2
        to = (j + pos[4]) % 4
        parts = []
        for w in wide:
            sides = [w[0:4, at + 128 * h : at + 128 * h + 128] for at in (0, 256)]
            parts.append(jnp.concatenate(sides, axis=1))
        gates = sum(w[4 + j : 5 + j] for w in wide)
        parts += [gates[:, 0:256], gates[:, 256:512], jnp.zeros((14, 256), F32)]
        o[to, 128:160] = jnp.concatenate(parts, axis=0).astype(BF)


def composed(pos, maps):
    back = pos[0] % 2
    at = back * 3
    step = 1 - 2 * back
    total = maps[at][0:128].astype(F32)
    for _ in range(3):
        at = at + step
        total = total + maps[at][0:128].astype(F32) + apply_to(maps[at][0:128, 0:128], total)
    return total


def low_kernel(pos, maps, o):
    total = composed(pos, maps)
    wide = [maps[i][128:].astype(F32) for i in range(4)]
    parts = [w[4 * i : 4 * i + 4] for i in range(4) for w in wide]
    parts += [sum(w[16:18] for w in wide), jnp.zeros((14, 256), F32)]
    out = jnp.concatenate([total, *parts], axis=0).astype(BF)
    for i in range(4):
        o[i] = out


def high_kernel(pos, maps, o):
    o[...] = composed(pos, maps).astype(BF)


def context_kernel(pos, low, small, o):
    wide = [low[i][128:].astype(F32) for i in range(4)]
    rows = jnp.concatenate([w[16 * i : 16 * i + 16] for i in range(4) for w in wide], axis=0)
    gates = sum(w[64:66] for w in wide)
    o[...] = context_state(
        pos, rows, gates[0:1], gates[1:2], small[0:1], small[1:2], small[2:3]
    )


def moved(maps, state):
    return state + maps[:, 128:256].astype(F32) + apply_to(maps[:, 0:128], state)


def scan_kernel(pos, start, far, middle, near, low, own, o):
    back = pos[0] % 2
    step = 1 - 2 * back
    state = start[...]
    for maps in (far, middle, near):
        state = moved(maps[...], state)
    at = back * 3
    for _ in range(3):
        state = jnp.where((pos[3] - at) * step > 0, moved(low[at][0:128], state), state)
        at = at + step
    at = back * 3
    for i in range(4):
        o[at] = state.astype(BF)
        if i < 3:
            state = moved(own[at][0:128], state)
        at = at + step


def read_kernel(pos, states, reads, base, gain, weight, o):
    heads = []
    for h in range(2):
        first = states[(2 * h + pos[4]) % 4]
        second = states[(2 * h + 1 + pos[4]) % 4]
        total = base[:, 128 * h : 128 * h + 128] + (
            mm(reads[h][:, 0:128], first) + mm(reads[h][:, 128:256], second)
        )
        mean = jnp.mean(total * total, axis=1, keepdims=True)
        heads.append((total * lax.rsqrt(mean + EPS) * gain[3:4]).astype(BF))
    branch = mm(jnp.concatenate(heads, axis=1), weight[...]).astype(BF)
    for t in range(8):
        o[t] = branch[32 * t : 32 * t + 32]


def output_kernel(rows, fac, lat, o):
    branch = rows[0].astype(F32)
    for i in range(1, 8):
        branch = branch + rows[i].astype(F32)
    gates = []
    for t in range(8):
        f = (fac[t] + fac[8 + t]) + (fac[16 + t] + fac[24 + t])
        gates.append(f[2:3])
    gate = jnp.concatenate(gates, axis=1)
    o[...] = (lat[...].astype(F32) + gate * branch).astype(BF)


def call(kernel, outs, specs, scratch=(), flops=1, aliases=None):
    def shape(s):
        return jax.ShapeDtypeStruct(*s)

    many = isinstance(outs, list)
    return pl.pallas_call(
        kernel,
        out_shape=[shape(s) for s in outs] if many else shape(outs),
        in_specs=specs,
        out_specs=[VM] * len(outs) if many else VM,
        scratch_shapes=scratch,
        input_output_aliases=aliases or {},
        compiler_params=pltpu.CompilerParams(vmem_limit_bytes=24 * 2**20),
        cost_estimate=pl.CostEstimate(flops=flops, bytes_accessed=1, transcendentals=0),
    )


def to_all(value, axes, count):
    return lax.all_to_all(
        jnp.broadcast_to(value[None], (count, *value.shape)), axes, 0, 0, tiled=True
    )


def onward(d):
    pairs = []
    for zh in range(4):
        for y in range(4):
            for c in range(2):
                to = zh + d if (y + c) % 2 == 0 else zh - d
                if 0 <= to < 4:
                    pairs.append((zh * 8 + y * 2 + c, to * 8 + y * 2 + c))
    return pairs


def per_device(
    latent,
    condition,
    context,
    context_condition_vector,
    modulation_matrix,
    query_matrix,
    key_matrix,
    value_matrix,
    decay_input_weight,
    write_strength_weight,
    head_decay_rate,
    write_strength_bias,
    context_write_offset_bias,
    log_spike_added,
    head_norm_gain,
    output_matrix,
):
    zh, zl, y = (lax.axis_index("zh"), lax.axis_index("zl"), lax.axis_index("y"))
    x, c = (lax.axis_index("x"), lax.axis_index("c"))
    sp_index = lax.axis_index(SP)
    pos = jnp.stack([(y + c) % 4, x * 2 + c, zh, zl, (4 - c) % 4, sp_index * 4, c, x])
    pos = pos.astype(jnp.int32)
    mine = to_all(latent, "x", 4)
    other = lax.ppermute(mine, "c", [(0, 1), (1, 0)])
    signals = jnp.stack([condition, context_condition_vector])
    signals = lax.dynamic_slice_in_dim(jax.nn.silu(signals), sp_index * 32, 32, 1)
    mod = modulation_matrix.astype(F32)
    part = jnp.concatenate(
        [
            jnp.sum(mod * signals[0][None, :, None], axis=1),
            jnp.sum(mod[:2] * signals[1][None, :, None], axis=1),
        ]
    )
    part = to_all(part, Z, 16)
    part = jnp.sum(part, axis=0)
    fac = to_all(part, ("y", "x", "c"), 32)

    small = jnp.stack(
        [
            jnp.pad(head_decay_rate, (0, 96)),
            jnp.pad(write_strength_bias, (0, 96)),
            jnp.pad(context_write_offset_bias, (0, 96)),
            head_norm_gain,
        ]
    )
    packed, rows = call(
        project_kernel,
        [((832, 256), BF), ((4, 8, 512), BF)],
        [SM] + [VM] * 5 + [HB] * 4,
        [
            pltpu.VMEM((272, D), BF),
            pltpu.VMEM((D, 256), BF),
            pltpu.VMEM((32, D), BF),
            pltpu.VMEM((32, D), BF),
            pltpu.VMEM((4, D), BF),
            pltpu.SemaphoreType.DMA((4,)),
        ],
        flops=10**9,
    )(
        pos,
        mine,
        other,
        fac,
        query_matrix,
        key_matrix,
        *(
            pltpu.with_memory_space_constraint(a, pltpu.HBM)
            for a in (
                value_matrix,
                decay_input_weight.T,
                write_strength_weight.T,
                context,
            )
        ),
    )
    packed = pltpu.with_memory_space_constraint(packed, pltpu.HBM)
    rows = lax.all_to_all(rows, "zh", 0, 0, tiled=True)
    maps, reads, base = call(
        chunk_kernel,
        [((4, 160, 256), BF), ((2, 256, 256), BF), ((256, 256), F32)],
        [SM] + [VM] * 3,
        flops=4 * 10**9,
    )(
        pos,
        packed,
        log_spike_added.T,
        small,
    )
    maps = call(pack_kernel, ((4, 160, 256), BF), [SM, VM, VM], aliases={1: 0})(
        pos, maps, rows
    )
    of_y = lax.all_to_all(maps, "y", 0, 0, tiled=True)
    low = call(low_kernel, ((4, 208, 256), BF), [SM, VM])(pos, of_y)
    of_low = lax.all_to_all(low, "zl", 0, 0, tiled=True)
    high = call(high_kernel, ((128, 256), BF), [SM, VM])(pos, of_low)
    of_high = []
    for d in (3, 2, 1):
        of_high.append(lax.ppermute(high, ("zh", "y", "c"), onward(d)))
    start = call(context_kernel, ((128, 128), F32), [SM] + [VM] * 2, flops=10**9)(
        pos, of_low, small
    )
    states = call(scan_kernel, ((4, 128, 128), BF), [SM] + [VM] * 6, flops=10**8)(
        pos, start, *of_high, of_low, of_y
    )
    states = lax.all_to_all(states, "y", 0, 0, tiled=True)
    branch = call(read_kernel, ((8, 32, D), BF), [SM] + [VM] * 5, flops=10**8)(
        pos, states, reads, base, small, output_matrix
    )
    branch = lax.all_to_all(branch, TP, 0, 0, tiled=True)
    return call(output_kernel, ((32, D), BF), [VM] * 3, flops=10**8)(branch, fac, latent)


def solution(mesh):
    split = Mesh(mesh.devices.reshape(4, 4, 4, 4, 2), ALL)
    return jax.shard_map(
        per_device,
        mesh=split,
        in_specs=(
            P(ALL, None),
            P(),
            P(SP, None),
            P(),
            P(None, SP, TP),
            P(None, TP),
            P(None, TP),
            P(None, TP),
            P(),
            P(),
            P(),
            P(),
            P(),
            P(SP, None),
            P(),
            P(TP, None),
        ),
        out_specs=P(ALL, None),
        check_vma=False,
    )
```

```python
import jax
import jax.numpy as jnp
from jax import lax
from jax.experimental import pallas as pl
from jax.experimental.pallas import tpu as pltpu
from jax.sharding import Mesh
from jax.sharding import PartitionSpec as P


D = 2048
EPS = 1e-06
HI = lax.Precision.HIGHEST
F32 = jnp.float32
BF = jnp.bfloat16
Z = ("zh", "zl")
TP = ("x", "c")
SP = ("zh", "zl", "y")
ALL = ("zh", "zl", "y", "x", "c")
VM = pl.BlockSpec(memory_space=pltpu.VMEM)
SM = pl.BlockSpec(memory_space=pltpu.SMEM)
HB = pl.BlockSpec(memory_space=pltpu.HBM)


def mm(a, b, dims=((1,), (0,))):
    return lax.dot_general(
        a.astype(BF), b.astype(BF), (dims, ((), ())), preferred_element_type=F32
    )


def norm_rows(rows, scale, shift):
    wide = rows.astype(F32)
    centred = wide - jnp.mean(wide, axis=-1, keepdims=True)
    spread = jnp.mean(centred * centred, axis=-1, keepdims=True)
    return (centred * lax.rsqrt(spread + EPS) * (1.0 + scale) + shift).astype(BF)


def column(matrix, lane):
    lanes = lax.broadcasted_iota(jnp.int32, matrix.shape, 1)
    return jnp.sum(jnp.where(lanes == lane, matrix, 0.0), axis=1, keepdims=True)


def softplus(t):
    return jnp.maximum(t, 0.0) + jnp.log1p(jnp.exp(-jnp.abs(t)))


def sigmoid(t):
    return 1.0 / (1.0 + jnp.exp(-t))


def inverse_of(lower, row, col):
    eye = (row == col).astype(F32)
    own = (row // 16) == (col // 16)
    base = [jnp.where(own, m, 0.0) for m in lower]
    inv = [eye - m for m in base]
    power = [mm(m, m) for m in base]
    for step in range(3):
        inv = [p + mm(p, x) for p, x in zip(inv, power)]
        if step < 2:
            power = [mm(x, x) for x in power]
    size = 16
    while size < 256:
        here = ((row // (2 * size)) == (col // (2 * size))) & ((row // size) != (col // size))
        side = [mm(jnp.where(here, m, 0.0), p) for m, p in zip(lower, inv)]
        inv = [p - mm(p, s) for p, s in zip(inv, side)]
        size *= 2
    out = []
    for m, p in zip(lower, inv):
        first = p.astype(BF)
        high = m.astype(BF)
        low = (m - high.astype(F32)).astype(BF)
        wide = first.astype(F32)
        left = (eye - wide) - (mm(high, first) + mm(low, first))
        out.append(wide + mm(first, left))
    return out


def front_kernel(
    pos, one, two, ctx, fac, wq, wk, spike, small, wv_h, wd_h, ww_h,
    m_o, r_o, o_o,
    hid, packed, wv, wd, ww, sems,
):
    copies = [
        pltpu.make_async_copy(source, target, sems.at[i])
        for i, (source, target) in enumerate(((wv_h, wv), (wd_h, wd), (ww_h, ww)))
    ]
    for copy in copies:
        copy.start()
    factors = [[], [], [], []]
    for t in range(8):
        f = (fac[t] + fac[8 + t]) + (fac[16 + t] + fac[24 + t])
        for slot, r in enumerate((0, 1, 3, 4)):
            factors[slot].append(f[r : r + 1])
    shift, scale, c_shift, c_scale = (jnp.concatenate(f, axis=1) for f in factors)
    for d in range(4):
        for i, lat in enumerate((one, two)):
            core = pos[6] if i == 0 else 1 - pos[6]
            spot = (2 * ((pos[7] + 4 - d) % 4) + core) * 32
            hid[pl.ds(pl.multiple_of(spot, 32), 32)] = norm_rows(lat[d], scale, shift)
    context_rows = jnp.concatenate([ctx[i].astype(F32) for i in range(4)], axis=0)
    hid[256:272] = norm_rows(context_rows, c_scale, c_shift)
    rows = hid[...]
    packed[0:256] = mm(hid[0:256], wq[...]).astype(BF)
    keys = mm(rows, wk[...]).astype(BF)
    packed[256:512] = keys[:256]
    for copy in copies:
        copy.wait()
    values = mm(rows, wv[...]).astype(BF)
    packed[512:768] = values[:256]
    last_two = ((1,), (1,))
    packed[768:800] = mm(wd[...], hid[0:256], last_two).astype(BF)
    packed[800:832] = mm(ww[...], hid[0:256], last_two).astype(BF)
    rate = mm(hid[256:272], wd[...], last_two).astype(BF).astype(F32)
    write = mm(hid[256:272], ww[...], last_two).astype(BF).astype(F32)
    lanes = lax.broadcasted_iota(jnp.int32, (16, 256), 1)
    rank = lax.broadcasted_iota(jnp.int32, (16, 256), 0)
    spots = lanes == (rank // 4) * 64 + rank % 4 + pos[5]
    for j in range(4):
        h = j // 2
        to = (j + pos[4]) % 4
        lane = pos[1] * 4 + j
        m_o[to, 128:144, 0:128] = keys[256:272, 128 * h : 128 * h + 128]
        m_o[to, 128:144, 128:256] = values[256:272, 128 * h : 128 * h + 128]
        gates = [
            jnp.sum(jnp.where(spots, column(g, lane), 0.0), axis=0, keepdims=True)
            for g in (rate, write)
        ]
        gates.append(jnp.zeros((14, 256), F32))
        m_o[to, 144:160] = jnp.concatenate(gates, axis=0).astype(BF)
    chunk(pos, packed, spike, small, m_o, r_o, o_o)


def chunk(pos, packed, spike, small, m_o, r_o, o_o):
    row = lax.broadcasted_iota(jnp.int32, (256, 256), 0)
    col = lax.broadcasted_iota(jnp.int32, (256, 256), 1)
    eye = row == col
    entry = lax.broadcasted_iota(jnp.int32, (32, 128), 0)
    entry = entry == lax.broadcasted_iota(jnp.int32, (32, 128), 1)
    decay, bias = (
        jnp.sum(jnp.where(entry, small[i : i + 1], 0.0), axis=1, keepdims=True) for i in range(2)
    )
    logs = -decay * softplus(packed[768:800].astype(F32)) + spike[...]
    strength = sigmoid(packed[800:832].astype(F32) + bias)
    entry = lax.broadcasted_iota(jnp.int32, (32, 256), 0) - pos[1] * 4
    below = (row >= col).astype(F32)
    above = (row <= col).astype(F32)
    sums = (
        jnp.dot(logs, above, precision=HI, preferred_element_type=F32),
        jnp.dot(logs, below, precision=HI, preferred_element_type=F32),
    )

    def upright(line):
        return jnp.sum(jnp.where(eye, line, 0.0), axis=1, keepdims=True)

    lowers, parts = ([], [])
    for h in range(2):
        qh, kh, vh = (packed[256 * i : 256 * i + 256, 128 * h : 128 * h + 128] for i in range(3))
        kf = kh.astype(F32)
        unit = lax.rsqrt(jnp.sum(kf * kf, axis=1, keepdims=True) + EPS)
        unit_row = jnp.sum(jnp.where(eye, unit, 0.0), axis=0, keepdims=True)
        gram = mm(kh, kh, ((1,), (1,))) * unit_row
        cross = mm(qh, kh, ((1,), (1,))) * unit_row
        for e in range(2):
            j = 2 * h + e
            total_row = jnp.sum(jnp.where(entry == j, sums[e], 0.0), axis=0, keepdims=True)
            total = upright(total_row)
            b = upright(jnp.sum(jnp.where(entry == j, strength, 0.0), axis=0, keepdims=True))
            last = total[255:256] if e == 0 else total[0:1]
            inside = row >= col if e == 0 else row <= col
            fade = jnp.where(inside, jnp.exp(jnp.where(inside, total - total_row, 0.0)), 0.0)
            lowers.append(jnp.where(eye, 0.0, (b * unit) * gram * fade))
            grown = jnp.exp(total)
            right = jnp.concatenate(
                [
                    b * vh.astype(F32),
                    (b * unit * grown) * kf,
                ],
                axis=1,
            ).astype(BF)
            faded = (kf * (unit * jnp.exp(last - total))).astype(BF)
            scores = (cross * fade).astype(BF)
            parts.append((right, faded, scores, grown * qh.astype(F32), jnp.exp(last) - 1.0))
    solved = inverse_of(lowers, row, col)
    small = lax.broadcasted_iota(jnp.int32, (128, 128), 0) == lax.broadcasted_iota(
        jnp.int32, (128, 128), 1
    )
    outs = [None, None]
    for j in range(4):
        right, faded, scores, grown_q, short = parts[j]
        both = mm(solved[j], right).astype(BF)
        maps = mm(faded, both, ((0,), (0,)))
        read = mm(scores, both)
        to = (j + pos[4]) % 4
        m_o[to, 0:128, 0:128] = (jnp.where(small, short, 0.0) - maps[:, 128:]).astype(BF)
        m_o[to, 0:128, 128:256] = maps[:, :128].astype(BF)
        h, e = divmod(j, 2)
        r_o[h, :, 128 * e : 128 * e + 128] = (grown_q - read[:, 128:]).astype(BF)
        outs[h] = read[:, :128] if e == 0 else outs[h] + read[:, :128]
    o_o[:, 0:128] = outs[0]
    o_o[:, 128:256] = outs[1]


def context_state(pos, rows, rate, write, decay, bias, extra):
    row = lax.broadcasted_iota(jnp.int32, (256, 256), 0)
    col = lax.broadcasted_iota(jnp.int32, (256, 256), 1)
    eye = row == col
    lane = pos[1] * 4 + pos[0]
    inside = (row - col) * (1 - 2 * (pos[0] % 2)) >= 0
    kh = rows[:, 0:128].astype(BF)
    kf = rows[:, 0:128]
    logs = -column(decay, lane) * softplus(rate)
    strength = sigmoid(write + column(bias, lane) + column(extra, lane))
    b = jnp.sum(jnp.where(eye, strength, 0.0), axis=1, keepdims=True)
    total = jnp.sum(jnp.where(inside, logs, 0.0), axis=1, keepdims=True)
    total_row = jnp.sum(jnp.where(eye, total, 0.0), axis=0, keepdims=True)
    last = jnp.sum(logs, axis=1, keepdims=True)
    unit = lax.rsqrt(jnp.sum(kf * kf, axis=1, keepdims=True) + EPS)
    unit_row = jnp.sum(jnp.where(eye, unit, 0.0), axis=0, keepdims=True)
    fade = jnp.where(inside, jnp.exp(jnp.where(inside, total - total_row, 0.0)), 0.0)
    lower = jnp.where(
        eye, 0.0, (b * unit) * (mm(kh, kh, ((1,), (1,))) * unit_row) * fade
    )
    solved = inverse_of([lower], row, col)[0]
    fresh = mm(solved, b * rows[:, 128:256])
    faded = kf * (unit * jnp.exp(last - total))
    return mm(faded, fresh, ((0,), (0,)))


def apply_to(linear, state):
    high = state.astype(BF)
    low = (state - high.astype(F32)).astype(BF)
    both = mm(linear, jnp.concatenate([high, low], axis=1))
    n = state.shape[1]
    return both[:, :n] + both[:, n:]


def composed(pos, maps):
    back = pos[0] % 2
    at = back * 3
    step = 1 - 2 * back
    total = maps[at][0:128].astype(F32)
    for _ in range(3):
        at = at + step
        total = total + maps[at][0:128].astype(F32) + apply_to(maps[at][0:128, 0:128], total)
    return total


def low_kernel(pos, maps, o):
    total = composed(pos, maps)
    wide = [maps[i][128:].astype(F32) for i in range(4)]
    parts = [w[4 * i : 4 * i + 4] for i in range(4) for w in wide]
    parts += [sum(w[16:18] for w in wide), jnp.zeros((14, 256), F32)]
    out = jnp.concatenate([total, *parts], axis=0).astype(BF)
    for i in range(4):
        o[i] = out


def high_kernel(pos, maps, o):
    o[...] = composed(pos, maps).astype(BF)


def context_kernel(pos, low, small, o):
    wide = [low[i][128:].astype(F32) for i in range(4)]
    rows = jnp.concatenate([w[16 * i : 16 * i + 16] for i in range(4) for w in wide], axis=0)
    gates = sum(w[64:66] for w in wide)
    o[...] = context_state(
        pos, rows, gates[0:1], gates[1:2], small[0:1], small[1:2], small[2:3]
    )


def moved(maps, state):
    return state + maps[:, 128:256].astype(F32) + apply_to(maps[:, 0:128], state)


def scan_kernel(pos, start, far, middle, near, low, own, o):
    back = pos[0] % 2
    step = 1 - 2 * back
    state = start[...]
    for maps in (far, middle, near):
        state = moved(maps[...], state)
    at = back * 3
    for _ in range(3):
        state = jnp.where((pos[3] - at) * step > 0, moved(low[at][0:128], state), state)
        at = at + step
    at = back * 3
    for i in range(4):
        o[at] = state.astype(BF)
        if i < 3:
            state = moved(own[at][0:128], state)
        at = at + step


def read_kernel(pos, states, reads, base, gain, weight, o):
    heads = []
    for h in range(2):
        first = states[(2 * h + pos[4]) % 4]
        second = states[(2 * h + 1 + pos[4]) % 4]
        total = base[:, 128 * h : 128 * h + 128] + (
            mm(reads[h][:, 0:128], first) + mm(reads[h][:, 128:256], second)
        )
        mean = jnp.mean(total * total, axis=1, keepdims=True)
        heads.append((total * lax.rsqrt(mean + EPS) * gain[3:4]).astype(BF))
    branch = mm(jnp.concatenate(heads, axis=1), weight[...]).astype(BF)
    for t in range(8):
        o[t] = branch[32 * t : 32 * t + 32]


def output_kernel(rows, fac, lat, o):
    branch = rows[0].astype(F32)
    for i in range(1, 8):
        branch = branch + rows[i].astype(F32)
    gates = []
    for t in range(8):
        f = (fac[t] + fac[8 + t]) + (fac[16 + t] + fac[24 + t])
        gates.append(f[2:3])
    gate = jnp.concatenate(gates, axis=1)
    o[...] = (lat[...].astype(F32) + gate * branch).astype(BF)


def call(kernel, outs, specs, scratch=(), flops=1, aliases=None):
    def shape(s):
        return jax.ShapeDtypeStruct(*s)

    many = isinstance(outs, list)
    return pl.pallas_call(
        kernel,
        out_shape=[shape(s) for s in outs] if many else shape(outs),
        in_specs=specs,
        out_specs=[VM] * len(outs) if many else VM,
        scratch_shapes=scratch,
        input_output_aliases=aliases or {},
        compiler_params=pltpu.CompilerParams(vmem_limit_bytes=24 * 2**20),
        cost_estimate=pl.CostEstimate(flops=flops, bytes_accessed=1, transcendentals=0),
    )


def to_all(value, axes, count):
    return lax.all_to_all(
        jnp.broadcast_to(value[None], (count, *value.shape)), axes, 0, 0, tiled=True
    )


def onward(d):
    pairs = []
    for zh in range(4):
        for y in range(4):
            for c in range(2):
                to = zh + d if (y + c) % 2 == 0 else zh - d
                if 0 <= to < 4:
                    pairs.append((zh * 8 + y * 2 + c, to * 8 + y * 2 + c))
    return pairs


def per_device(
    latent,
    condition,
    context,
    context_condition_vector,
    modulation_matrix,
    query_matrix,
    key_matrix,
    value_matrix,
    decay_input_weight,
    write_strength_weight,
    head_decay_rate,
    write_strength_bias,
    context_write_offset_bias,
    log_spike_added,
    head_norm_gain,
    output_matrix,
):
    zh, zl, y = (lax.axis_index("zh"), lax.axis_index("zl"), lax.axis_index("y"))
    x, c = (lax.axis_index("x"), lax.axis_index("c"))
    sp_index = lax.axis_index(SP)
    pos = jnp.stack([(y + c) % 4, x * 2 + c, zh, zl, (4 - c) % 4, zl * 16 + y * 4, c, x])
    pos = pos.astype(jnp.int32)
    ctx = to_all(context, "zh", 4)
    parts = [latent]
    for d in range(1, 4):
        parts.append(lax.ppermute(latent, "x", [(i, (i + d) % 4) for i in range(4)]))
    mine = jnp.stack(parts)
    other = lax.ppermute(mine, "c", [(0, 1), (1, 0)])
    signals = jnp.stack([condition, context_condition_vector])
    signals = lax.dynamic_slice_in_dim(jax.nn.silu(signals), sp_index * 32, 32, 1)
    mod = modulation_matrix.astype(F32)
    part = jnp.concatenate(
        [
            jnp.sum(mod * signals[0][None, :, None], axis=1),
            jnp.sum(mod[:2] * signals[1][None, :, None], axis=1),
        ]
    )
    part = to_all(part, Z, 16)
    part = jnp.sum(part, axis=0)
    fac = to_all(part, ("y", "x", "c"), 32)

    small = jnp.stack(
        [
            jnp.pad(head_decay_rate, (0, 96)),
            jnp.pad(write_strength_bias, (0, 96)),
            jnp.pad(context_write_offset_bias, (0, 96)),
            head_norm_gain,
        ]
    )
    maps, reads, base = call(
        front_kernel,
        [((4, 160, 256), BF), ((2, 256, 256), BF), ((256, 256), F32)],
        [SM] + [VM] * 8 + [HB] * 3,
        [
            pltpu.VMEM((272, D), BF),
            pltpu.VMEM((832, 256), BF),
            pltpu.VMEM((D, 256), BF),
            pltpu.VMEM((32, D), BF),
            pltpu.VMEM((32, D), BF),
            pltpu.SemaphoreType.DMA((3,)),
        ],
        flops=5 * 10**9,
    )(
        pos,
        mine,
        other,
        ctx,
        fac,
        query_matrix,
        key_matrix,
        log_spike_added.T,
        small,
        *(
            pltpu.with_memory_space_constraint(a, pltpu.HBM)
            for a in (value_matrix, decay_input_weight.T, write_strength_weight.T)
        ),
    )
    of_y = lax.all_to_all(maps, "y", 0, 0, tiled=True)
    low = call(low_kernel, ((4, 208, 256), BF), [SM, VM])(pos, of_y)
    of_low = lax.all_to_all(low, "zl", 0, 0, tiled=True)
    high = call(high_kernel, ((128, 256), BF), [SM, VM])(pos, of_low)
    of_high = []
    for d in (3, 2, 1):
        of_high.append(lax.ppermute(high, ("zh", "y", "c"), onward(d)))
    start = call(context_kernel, ((128, 128), F32), [SM] + [VM] * 2, flops=10**9)(
        pos, of_low, small
    )
    states = call(scan_kernel, ((4, 128, 128), BF), [SM] + [VM] * 6, flops=10**8)(
        pos, start, *of_high, of_low, of_y
    )
    states = lax.all_to_all(states, "y", 0, 0, tiled=True)
    branch = call(read_kernel, ((8, 32, D), BF), [SM] + [VM] * 5, flops=10**8)(
        pos, states, reads, base, small, output_matrix
    )
    branch = lax.all_to_all(branch, TP, 0, 0, tiled=True)
    return call(output_kernel, ((32, D), BF), [VM] * 3, flops=10**8)(branch, fac, latent)


def solution(mesh):
    split = Mesh(mesh.devices.reshape(4, 4, 4, 4, 2), ALL)
    return jax.shard_map(
        per_device,
        mesh=split,
        in_specs=(
            P(ALL, None),
            P(),
            P(SP, None),
            P(),
            P(None, SP, TP),
            P(None, TP),
            P(None, TP),
            P(None, TP),
            P(),
            P(),
            P(),
            P(),
            P(),
            P(SP, None),
            P(),
            P(TP, None),
        ),
        out_specs=P(ALL, None),
        check_vma=False,
    )
```

```python
import jax
import jax.numpy as jnp
from jax import lax
from jax.experimental import pallas as pl
from jax.experimental.pallas import tpu as pltpu
from jax.sharding import Mesh
from jax.sharding import PartitionSpec as P


D = 2048
EPS = 1e-06
HI = lax.Precision.HIGHEST
F32 = jnp.float32
BF = jnp.bfloat16
Z = ("zh", "zl")
TP = ("x", "c")
SP = ("zh", "zl", "y")
ALL = ("zh", "zl", "y", "x", "c")
VM = pl.BlockSpec(memory_space=pltpu.VMEM)
SM = pl.BlockSpec(memory_space=pltpu.SMEM)
HB = pl.BlockSpec(memory_space=pltpu.HBM)


def mm(a, b, dims=((1,), (0,))):
    return lax.dot_general(
        a.astype(BF), b.astype(BF), (dims, ((), ())), preferred_element_type=F32
    )


def norm_rows(rows, scale, shift):
    wide = rows.astype(F32)
    centred = wide - jnp.mean(wide, axis=-1, keepdims=True)
    spread = jnp.mean(centred * centred, axis=-1, keepdims=True)
    return (centred * lax.rsqrt(spread + EPS) * (1.0 + scale) + shift).astype(BF)


def column(matrix, lane):
    lanes = lax.broadcasted_iota(jnp.int32, matrix.shape, 1)
    return jnp.sum(jnp.where(lanes == lane, matrix, 0.0), axis=1, keepdims=True)


def softplus(t):
    return jnp.maximum(t, 0.0) + jnp.log1p(jnp.exp(-jnp.abs(t)))


def sigmoid(t):
    return 1.0 / (1.0 + jnp.exp(-t))


def inverse_of(lower, row, col):
    eye = (row == col).astype(F32)
    own = (row // 16) == (col // 16)
    base = [jnp.where(own, m, 0.0) for m in lower]
    inv = [eye - m for m in base]
    power = [mm(m, m) for m in base]
    for step in range(3):
        inv = [p + mm(p, x) for p, x in zip(inv, power)]
        if step < 2:
            power = [mm(x, x) for x in power]
    size = 16
    while size < 256:
        here = ((row // (2 * size)) == (col // (2 * size))) & ((row // size) != (col // size))
        side = [mm(jnp.where(here, m, 0.0), p) for m, p in zip(lower, inv)]
        inv = [p - mm(p, s) for p, s in zip(inv, side)]
        size *= 2
    out = []
    for m, p in zip(lower, inv):
        first = p.astype(BF)
        high = m.astype(BF)
        low = (m - high.astype(F32)).astype(BF)
        wide = first.astype(F32)
        left = (eye - wide) - (mm(high, first) + mm(low, first))
        out.append(wide + mm(first, left))
    return out


def start_copies(sources, targets, sems):
    copies = [
        pltpu.make_async_copy(source, target, sems.at[i])
        for i, (source, target) in enumerate(zip(sources, targets))
    ]
    for copy in copies:
        copy.start()
    return copies


def factor(fac, r):
    parts = [(fac[t] + fac[8 + t]) + (fac[16 + t] + fac[24 + t]) for t in range(8)]
    return jnp.concatenate([f[r : r + 1] for f in parts], axis=1)


def rows_kernel(pos, ctx, fac, wk, wv_h, wd_h, ww_h, c_o, hid, wv, wd, ww, sems):
    copies = start_copies((wv_h, wd_h, ww_h), (wv, wd, ww), sems)
    hid[0:4] = norm_rows(ctx[...], factor(fac, 4), factor(fac, 3))
    hid[4:16] = jnp.zeros((12, D), BF)
    rows = hid[...]
    keys = mm(rows, wk[...]).astype(BF)
    for copy in copies:
        copy.wait()
    values = mm(rows, wv[...]).astype(BF)
    rate = mm(rows, wd[...], ((1,), (1,))).astype(BF).astype(F32)
    write = mm(rows, ww[...], ((1,), (1,))).astype(BF).astype(F32)
    lanes = lax.broadcasted_iota(jnp.int32, (16, 256), 1)
    rank = lax.broadcasted_iota(jnp.int32, (16, 256), 0)
    spots = (lanes == rank + pos[5]) & (rank < 4)
    wide = [side.astype(F32)[0:4] for side in (keys, values)]
    pieces = [jnp.concatenate(wide, axis=1)]
    for j in range(4):
        lane = pos[1] * 4 + j
        gates = [
            jnp.sum(jnp.where(spots, column(g, lane), 0.0), axis=0, keepdims=True)
            for g in (rate, write)
        ]
        pieces.append(jnp.concatenate(gates, axis=1))
    out = jnp.concatenate(pieces, axis=0).astype(BF)
    for i in range(4):
        c_o[i] = out


def front_kernel(
    pos, one, two, fac, wq, wk, spike, small, wv_h, wd_h, ww_h,
    m_o, r_o, o_o,
    hid, packed, wv, wd, ww, sems,
):
    copies = start_copies((wv_h, wd_h, ww_h), (wv, wd, ww), sems)
    shift, scale = (factor(fac, 0), factor(fac, 1))
    for d in range(4):
        for i, lat in enumerate((one, two)):
            core = pos[6] if i == 0 else 1 - pos[6]
            spot = (2 * ((pos[7] + 4 - d) % 4) + core) * 32
            hid[pl.ds(pl.multiple_of(spot, 32), 32)] = norm_rows(lat[d], scale, shift)
    rows = hid[...]
    packed[0:256] = mm(rows, wq[...]).astype(BF)
    packed[256:512] = mm(rows, wk[...]).astype(BF)
    for copy in copies:
        copy.wait()
    packed[512:768] = mm(rows, wv[...]).astype(BF)
    packed[768:800] = mm(wd[...], rows, ((1,), (1,))).astype(BF)
    packed[800:832] = mm(ww[...], rows, ((1,), (1,))).astype(BF)
    chunk(pos, packed, spike, small, m_o, r_o, o_o)


def chunk(pos, packed, spike, small, m_o, r_o, o_o):
    row = lax.broadcasted_iota(jnp.int32, (256, 256), 0)
    col = lax.broadcasted_iota(jnp.int32, (256, 256), 1)
    eye = row == col
    entry = lax.broadcasted_iota(jnp.int32, (32, 128), 0)
    entry = entry == lax.broadcasted_iota(jnp.int32, (32, 128), 1)
    decay, bias = (
        jnp.sum(jnp.where(entry, small[i : i + 1], 0.0), axis=1, keepdims=True) for i in range(2)
    )
    logs = -decay * softplus(packed[768:800].astype(F32)) + spike[...]
    strength = sigmoid(packed[800:832].astype(F32) + bias)
    entry = lax.broadcasted_iota(jnp.int32, (32, 256), 0) - pos[1] * 4
    below = (row >= col).astype(F32)
    above = (row <= col).astype(F32)
    sums = (
        jnp.dot(logs, above, precision=HI, preferred_element_type=F32),
        jnp.dot(logs, below, precision=HI, preferred_element_type=F32),
    )

    def upright(line):
        return jnp.sum(jnp.where(eye, line, 0.0), axis=1, keepdims=True)

    lowers, parts = ([], [])
    for h in range(2):
        qh, kh, vh = (packed[256 * i : 256 * i + 256, 128 * h : 128 * h + 128] for i in range(3))
        kf = kh.astype(F32)
        unit = lax.rsqrt(jnp.sum(kf * kf, axis=1, keepdims=True) + EPS)
        unit_row = jnp.sum(jnp.where(eye, unit, 0.0), axis=0, keepdims=True)
        gram = mm(kh, kh, ((1,), (1,))) * unit_row
        cross = mm(qh, kh, ((1,), (1,))) * unit_row
        for e in range(2):
            j = 2 * h + e
            total_row = jnp.sum(jnp.where(entry == j, sums[e], 0.0), axis=0, keepdims=True)
            total = upright(total_row)
            b = upright(jnp.sum(jnp.where(entry == j, strength, 0.0), axis=0, keepdims=True))
            last = total[255:256] if e == 0 else total[0:1]
            inside = row >= col if e == 0 else row <= col
            fade = jnp.where(inside, jnp.exp(jnp.where(inside, total - total_row, 0.0)), 0.0)
            lowers.append(jnp.where(eye, 0.0, (b * unit) * gram * fade))
            grown = jnp.exp(total)
            right = jnp.concatenate(
                [
                    b * vh.astype(F32),
                    (b * unit * grown) * kf,
                ],
                axis=1,
            ).astype(BF)
            faded = (kf * (unit * jnp.exp(last - total))).astype(BF)
            scores = (cross * fade).astype(BF)
            parts.append((right, faded, scores, grown * qh.astype(F32), jnp.exp(last) - 1.0))
    solved = inverse_of(lowers, row, col)
    small = lax.broadcasted_iota(jnp.int32, (128, 128), 0) == lax.broadcasted_iota(
        jnp.int32, (128, 128), 1
    )
    outs = [None, None]
    for j in range(4):
        right, faded, scores, grown_q, short = parts[j]
        both = mm(solved[j], right).astype(BF)
        maps = mm(faded, both, ((0,), (0,)))
        read = mm(scores, both)
        to = (j + pos[4]) % 4
        m_o[to, 0:128, 0:128] = (jnp.where(small, short, 0.0) - maps[:, 128:]).astype(BF)
        m_o[to, 0:128, 128:256] = maps[:, :128].astype(BF)
        h, e = divmod(j, 2)
        r_o[h, :, 128 * e : 128 * e + 128] = (grown_q - read[:, 128:]).astype(BF)
        outs[h] = read[:, :128] if e == 0 else outs[h] + read[:, :128]
    o_o[:, 0:128] = outs[0]
    o_o[:, 128:256] = outs[1]


def context_state(pos, rows, rate, write, decay, bias, extra):
    row = lax.broadcasted_iota(jnp.int32, (256, 256), 0)
    col = lax.broadcasted_iota(jnp.int32, (256, 256), 1)
    eye = row == col
    lane = pos[1] * 4 + pos[0]
    inside = (row - col) * (1 - 2 * (pos[0] % 2)) >= 0
    kh = rows[:, 0:128].astype(BF)
    kf = rows[:, 0:128]
    logs = -column(decay, lane) * softplus(rate)
    strength = sigmoid(write + column(bias, lane) + column(extra, lane))
    b = jnp.sum(jnp.where(eye, strength, 0.0), axis=1, keepdims=True)
    total = jnp.sum(jnp.where(inside, logs, 0.0), axis=1, keepdims=True)
    total_row = jnp.sum(jnp.where(eye, total, 0.0), axis=0, keepdims=True)
    last = jnp.sum(logs, axis=1, keepdims=True)
    unit = lax.rsqrt(jnp.sum(kf * kf, axis=1, keepdims=True) + EPS)
    unit_row = jnp.sum(jnp.where(eye, unit, 0.0), axis=0, keepdims=True)
    fade = jnp.where(inside, jnp.exp(jnp.where(inside, total - total_row, 0.0)), 0.0)
    lower = jnp.where(
        eye, 0.0, (b * unit) * (mm(kh, kh, ((1,), (1,))) * unit_row) * fade
    )
    solved = inverse_of([lower], row, col)[0]
    fresh = mm(solved, b * rows[:, 128:256])
    faded = kf * (unit * jnp.exp(last - total))
    return mm(faded, fresh, ((0,), (0,)))


def apply_to(linear, state):
    high = state.astype(BF)
    low = (state - high.astype(F32)).astype(BF)
    both = mm(linear, jnp.concatenate([high, low], axis=1))
    n = state.shape[1]
    return both[:, :n] + both[:, n:]


def pack_kernel(pos, maps, rows, o):
    wide = [rows[i].astype(F32) for i in range(4)]
    for j in range(4):
        h = j // 2
        to = (j + pos[4]) % 4
        parts = []
        for w in wide:
            sides = [w[0:4, at + 128 * h : at + 128 * h + 128] for at in (0, 256)]
            parts.append(jnp.concatenate(sides, axis=1))
        gates = sum(w[4 + j : 5 + j] for w in wide)
        parts += [gates[:, 0:256], gates[:, 256:512], jnp.zeros((14, 256), F32)]
        o[to, 128:160] = jnp.concatenate(parts, axis=0).astype(BF)


def composed(pos, maps):
    back = pos[0] % 2
    at = back * 3
    step = 1 - 2 * back
    total = maps[at][0:128].astype(F32)
    for _ in range(3):
        at = at + step
        total = total + maps[at][0:128].astype(F32) + apply_to(maps[at][0:128, 0:128], total)
    return total


def low_kernel(pos, maps, o):
    total = composed(pos, maps)
    wide = [maps[i][128:].astype(F32) for i in range(4)]
    parts = [w[4 * i : 4 * i + 4] for i in range(4) for w in wide]
    parts += [sum(w[16:18] for w in wide), jnp.zeros((14, 256), F32)]
    out = jnp.concatenate([total, *parts], axis=0).astype(BF)
    for i in range(4):
        o[i] = out


def high_kernel(pos, maps, o):
    o[...] = composed(pos, maps).astype(BF)


def context_kernel(pos, low, small, o):
    wide = [low[i][128:].astype(F32) for i in range(4)]
    rows = jnp.concatenate([w[16 * i : 16 * i + 16] for i in range(4) for w in wide], axis=0)
    gates = sum(w[64:66] for w in wide)
    o[...] = context_state(
        pos, rows, gates[0:1], gates[1:2], small[0:1], small[1:2], small[2:3]
    )


def moved(maps, state):
    return state + maps[:, 128:256].astype(F32) + apply_to(maps[:, 0:128], state)


def scan_kernel(pos, start, far, middle, near, low, own, o):
    back = pos[0] % 2
    step = 1 - 2 * back
    state = start[...]
    for maps in (far, middle, near):
        state = moved(maps[...], state)
    at = back * 3
    for _ in range(3):
        state = jnp.where((pos[3] - at) * step > 0, moved(low[at][0:128], state), state)
        at = at + step
    at = back * 3
    for i in range(4):
        o[at] = state.astype(BF)
        if i < 3:
            state = moved(own[at][0:128], state)
        at = at + step


def read_kernel(pos, states, reads, base, gain, weight, keep, give):
    heads = []
    for h in range(2):
        first = states[(2 * h + pos[4]) % 4]
        second = states[(2 * h + 1 + pos[4]) % 4]
        total = base[:, 128 * h : 128 * h + 128] + (
            mm(reads[h][:, 0:128], first) + mm(reads[h][:, 128:256], second)
        )
        mean = jnp.mean(total * total, axis=1, keepdims=True)
        heads.append((total * lax.rsqrt(mean + EPS) * gain[3:4]).astype(BF))
    branch = mm(jnp.concatenate(heads, axis=1), weight[...]).astype(BF)

    def split(even, odd):
        for i in range(4):
            even[i] = branch[64 * i : 64 * i + 32]
            odd[i] = branch[64 * i + 32 : 64 * i + 64]

    @pl.when(pos[6] == 0)
    def _():
        split(keep, give)

    @pl.when(pos[6] != 0)
    def _():
        split(give, keep)


def merge_kernel(keep, got, o):
    o[...] = (keep[...].astype(F32) + got[...].astype(F32)).astype(BF)


def output_kernel(rows, fac, lat, o):
    branch = (rows[0].astype(F32) + rows[1].astype(F32)) + (
        rows[2].astype(F32) + rows[3].astype(F32)
    )
    o[...] = (lat[...].astype(F32) + factor(fac, 2) * branch).astype(BF)


def call(kernel, outs, specs, scratch=(), flops=1, aliases=None):
    def shape(s):
        return jax.ShapeDtypeStruct(*s)

    many = isinstance(outs, list)
    return pl.pallas_call(
        kernel,
        out_shape=[shape(s) for s in outs] if many else shape(outs),
        in_specs=specs,
        out_specs=[VM] * len(outs) if many else VM,
        scratch_shapes=scratch,
        input_output_aliases=aliases or {},
        compiler_params=pltpu.CompilerParams(vmem_limit_bytes=24 * 2**20),
        cost_estimate=pl.CostEstimate(flops=flops, bytes_accessed=1, transcendentals=0),
    )


def to_all(value, axes, count):
    return lax.all_to_all(
        jnp.broadcast_to(value[None], (count, *value.shape)), axes, 0, 0, tiled=True
    )


def onward(d):
    pairs = []
    for zh in range(4):
        for y in range(4):
            for c in range(2):
                to = zh + d if (y + c) % 2 == 0 else zh - d
                if 0 <= to < 4:
                    pairs.append((zh * 8 + y * 2 + c, to * 8 + y * 2 + c))
    return pairs


def per_device(
    latent,
    condition,
    context,
    context_condition_vector,
    modulation_matrix,
    query_matrix,
    key_matrix,
    value_matrix,
    decay_input_weight,
    write_strength_weight,
    head_decay_rate,
    write_strength_bias,
    context_write_offset_bias,
    log_spike_added,
    head_norm_gain,
    output_matrix,
):
    zh, zl, y = (lax.axis_index("zh"), lax.axis_index("zl"), lax.axis_index("y"))
    x, c = (lax.axis_index("x"), lax.axis_index("c"))
    sp_index = lax.axis_index(SP)
    pos = jnp.stack([(y + c) % 4, x * 2 + c, zh, zl, (4 - c) % 4, sp_index * 4, c, x])
    pos = pos.astype(jnp.int32)
    parts = [latent]
    for d in range(1, 4):
        parts.append(lax.ppermute(latent, "x", [(i, (i + d) % 4) for i in range(4)]))
    mine = jnp.stack(parts)
    other = lax.ppermute(mine, "c", [(0, 1), (1, 0)])
    signals = jnp.stack([condition, context_condition_vector])
    signals = lax.dynamic_slice_in_dim(jax.nn.silu(signals), sp_index * 32, 32, 1)
    mod = modulation_matrix.astype(F32)
    part = jnp.concatenate(
        [
            jnp.sum(mod * signals[0][None, :, None], axis=1),
            jnp.sum(mod[:2] * signals[1][None, :, None], axis=1),
        ]
    )
    part = to_all(part, Z, 16)
    part = jnp.sum(part, axis=0)
    fac = to_all(part, ("y", "x", "c"), 32)

    small = jnp.stack(
        [
            jnp.pad(head_decay_rate, (0, 96)),
            jnp.pad(write_strength_bias, (0, 96)),
            jnp.pad(context_write_offset_bias, (0, 96)),
            head_norm_gain,
        ]
    )
    slow = [
        pltpu.with_memory_space_constraint(a, pltpu.HBM)
        for a in (value_matrix, decay_input_weight.T, write_strength_weight.T)
    ]
    room = [
        pltpu.VMEM((D, 256), BF),
        pltpu.VMEM((32, D), BF),
        pltpu.VMEM((32, D), BF),
        pltpu.SemaphoreType.DMA((3,)),
    ]
    rows = call(
        rows_kernel,
        ((4, 8, 512), BF),
        [SM] + [VM] * 3 + [HB] * 3,
        [pltpu.VMEM((16, D), BF), *room],
        flops=10**8,
    )(pos, context, fac, key_matrix, *slow)
    rows = lax.all_to_all(rows, "zh", 0, 0, tiled=True)
    maps, reads, base = call(
        front_kernel,
        [((4, 160, 256), BF), ((2, 256, 256), BF), ((256, 256), F32)],
        [SM] + [VM] * 7 + [HB] * 3,
        [pltpu.VMEM((256, D), BF), pltpu.VMEM((832, 256), BF), *room],
        flops=5 * 10**9,
    )(
        pos,
        mine,
        other,
        fac,
        query_matrix,
        key_matrix,
        log_spike_added.T,
        small,
        *slow,
    )
    maps = call(pack_kernel, ((4, 160, 256), BF), [SM, VM, VM], aliases={1: 0})(
        pos, maps, rows
    )
    of_y = lax.all_to_all(maps, "y", 0, 0, tiled=True)
    low = call(low_kernel, ((4, 208, 256), BF), [SM, VM])(pos, of_y)
    of_low = lax.all_to_all(low, "zl", 0, 0, tiled=True)
    high = call(high_kernel, ((128, 256), BF), [SM, VM])(pos, of_low)
    of_high = []
    for d in (3, 2, 1):
        of_high.append(lax.ppermute(high, ("zh", "y", "c"), onward(d)))
    start = call(context_kernel, ((128, 128), F32), [SM] + [VM] * 2, flops=10**9)(
        pos, of_low, small
    )
    states = call(scan_kernel, ((4, 128, 128), BF), [SM] + [VM] * 6, flops=10**8)(
        pos, start, *of_high, of_low, of_y
    )
    states = lax.all_to_all(states, "y", 0, 0, tiled=True)
    keep, give = call(
        read_kernel, [((4, 32, D), BF)] * 2, [SM] + [VM] * 5, flops=10**8
    )(pos, states, reads, base, small, output_matrix)
    got = lax.ppermute(give, "c", [(0, 1), (1, 0)])
    branch = call(merge_kernel, ((4, 32, D), BF), [VM] * 2)(keep, got)
    branch = lax.all_to_all(branch, "x", 0, 0, tiled=True)
    return call(output_kernel, ((32, D), BF), [VM] * 3, flops=10**8)(branch, fac, latent)


def solution(mesh):
    split = Mesh(mesh.devices.reshape(4, 4, 4, 4, 2), ALL)
    return jax.shard_map(
        per_device,
        mesh=split,
        in_specs=(
            P(ALL, None),
            P(),
            P(SP, None),
            P(),
            P(None, SP, TP),
            P(None, TP),
            P(None, TP),
            P(None, TP),
            P(),
            P(),
            P(),
            P(),
            P(),
            P(SP, None),
            P(),
            P(TP, None),
        ),
        out_specs=P(ALL, None),
        check_vma=False,
    )
```

```python
import jax
import jax.numpy as jnp
from jax import lax
from jax.experimental import pallas as pl
from jax.experimental.pallas import tpu as pltpu
from jax.sharding import Mesh
from jax.sharding import PartitionSpec as P


D = 2048
EPS = 1e-06
HI = lax.Precision.HIGHEST
F32 = jnp.float32
BF = jnp.bfloat16
Z = ("zh", "zl")
TP = ("x", "c")
SP = ("zh", "zl", "y")
ALL = ("zh", "zl", "y", "x", "c")
VM = pl.BlockSpec(memory_space=pltpu.VMEM)
SM = pl.BlockSpec(memory_space=pltpu.SMEM)
HB = pl.BlockSpec(memory_space=pltpu.HBM)


def mm(a, b, dims=((1,), (0,))):
    return lax.dot_general(
        a.astype(BF), b.astype(BF), (dims, ((), ())), preferred_element_type=F32
    )


def norm_rows(rows, scale, shift):
    wide = rows.astype(F32)
    centred = wide - jnp.mean(wide, axis=-1, keepdims=True)
    spread = jnp.mean(centred * centred, axis=-1, keepdims=True)
    return (centred * lax.rsqrt(spread + EPS) * (1.0 + scale) + shift).astype(BF)


def column(matrix, lane):
    lanes = lax.broadcasted_iota(jnp.int32, matrix.shape, 1)
    return jnp.sum(jnp.where(lanes == lane, matrix, 0.0), axis=1, keepdims=True)


def softplus(t):
    return jnp.maximum(t, 0.0) + jnp.log1p(jnp.exp(-jnp.abs(t)))


def sigmoid(t):
    return 1.0 / (1.0 + jnp.exp(-t))


def inverse_of(lower, row, col):
    eye = (row == col).astype(F32)
    own = (row // 16) == (col // 16)
    base = [jnp.where(own, m, 0.0) for m in lower]
    inv = [eye - m for m in base]
    power = [mm(m, m) for m in base]
    for step in range(3):
        inv = [p + mm(p, x) for p, x in zip(inv, power)]
        if step < 2:
            power = [mm(x, x) for x in power]
    size = 16
    while size < 256:
        here = ((row // (2 * size)) == (col // (2 * size))) & ((row // size) != (col // size))
        side = [mm(jnp.where(here, m, 0.0), p) for m, p in zip(lower, inv)]
        inv = [p - mm(p, s) for p, s in zip(inv, side)]
        size *= 2
    out = []
    for m, p in zip(lower, inv):
        first = p.astype(BF)
        high = m.astype(BF)
        low = (m - high.astype(F32)).astype(BF)
        wide = first.astype(F32)
        left = (eye - wide) - (mm(high, first) + mm(low, first))
        out.append(wide + mm(first, left))
    return out


def start_copies(sources, targets, sems):
    copies = [
        pltpu.make_async_copy(source, target, sems.at[i])
        for i, (source, target) in enumerate(zip(sources, targets))
    ]
    for copy in copies:
        copy.start()
    return copies


def factor(fac, r):
    parts = [(fac[t] + fac[8 + t]) + (fac[16 + t] + fac[24 + t]) for t in range(8)]
    return jnp.concatenate([f[r : r + 1] for f in parts], axis=1)


def front_kernel(
    pos, one, two, fac, small, ctx_h, wq_h, wk_h, wv_h, wd_h, ww_h, spike_h,
    m_o, r_o, o_o,
    hid, packed, ctx, wq, wk, wv, wd, ww, spike, sems,
):
    copies = start_copies(
        (ctx_h, wq_h, wk_h, wv_h, wd_h, ww_h, spike_h), (ctx, wq, wk, wv, wd, ww, spike), sems
    )
    shift, scale = (factor(fac, 0), factor(fac, 1))
    for d in range(4):
        for i, lat in enumerate((one, two)):
            core = pos[6] if i == 0 else 1 - pos[6]
            spot = (2 * ((pos[7] + 4 - d) % 4) + core) * 32
            hid[pl.ds(pl.multiple_of(spot, 32), 32)] = norm_rows(lat[d], scale, shift)
    copies[0].wait()
    hid[256:260] = norm_rows(ctx[...], factor(fac, 4), factor(fac, 3))
    hid[260:272] = jnp.zeros((12, D), BF)
    rows = hid[...]
    copies[1].wait()
    packed[0:256] = mm(hid[0:256], wq[...]).astype(BF)
    copies[2].wait()
    keys = mm(rows, wk[...]).astype(BF)
    packed[256:512] = keys[:256]
    for copy in copies[3:]:
        copy.wait()
    values = mm(rows, wv[...]).astype(BF)
    packed[512:768] = values[:256]
    packed[768:800] = mm(wd[...], hid[0:256], ((1,), (1,))).astype(BF)
    packed[800:832] = mm(ww[...], hid[0:256], ((1,), (1,))).astype(BF)
    rate = mm(hid[256:272], wd[...], ((1,), (1,))).astype(BF).astype(F32)
    write = mm(hid[256:272], ww[...], ((1,), (1,))).astype(BF).astype(F32)
    lanes = lax.broadcasted_iota(jnp.int32, (16, 256), 1)
    rank = lax.broadcasted_iota(jnp.int32, (16, 256), 0)
    spots = (lanes == rank + pos[5]) & (rank < 4)
    wide = [side[256:272].astype(F32)[0:4] for side in (keys, values)]
    for j in range(4):
        h = j // 2
        lane = pos[1] * 4 + j
        pieces = [jnp.concatenate([w[:, 128 * h : 128 * h + 128] for w in wide], axis=1)]
        pieces += [
            jnp.sum(jnp.where(spots, column(g, lane), 0.0), axis=0, keepdims=True)
            for g in (rate, write)
        ]
        pieces.append(jnp.zeros((10, 256), F32))
        m_o[(j + pos[4]) % 4, 128:144] = jnp.concatenate(pieces, axis=0).astype(BF)
    chunk(pos, packed, spike, small, m_o, r_o, o_o)


def chunk(pos, packed, spike, small, m_o, r_o, o_o):
    row = lax.broadcasted_iota(jnp.int32, (256, 256), 0)
    col = lax.broadcasted_iota(jnp.int32, (256, 256), 1)
    eye = row == col
    entry = lax.broadcasted_iota(jnp.int32, (32, 128), 0)
    entry = entry == lax.broadcasted_iota(jnp.int32, (32, 128), 1)
    decay, bias = (
        jnp.sum(jnp.where(entry, small[i : i + 1], 0.0), axis=1, keepdims=True) for i in range(2)
    )
    logs = -decay * softplus(packed[768:800].astype(F32)) + spike[...]
    strength = sigmoid(packed[800:832].astype(F32) + bias)
    entry = lax.broadcasted_iota(jnp.int32, (32, 256), 0) - pos[1] * 4
    below = (row >= col).astype(F32)
    above = (row <= col).astype(F32)
    sums = (
        jnp.dot(logs, above, precision=HI, preferred_element_type=F32),
        jnp.dot(logs, below, precision=HI, preferred_element_type=F32),
    )

    def upright(line):
        return jnp.sum(jnp.where(eye, line, 0.0), axis=1, keepdims=True)

    lowers, parts = ([], [])
    for h in range(2):
        qh, kh, vh = (packed[256 * i : 256 * i + 256, 128 * h : 128 * h + 128] for i in range(3))
        kf = kh.astype(F32)
        unit = lax.rsqrt(jnp.sum(kf * kf, axis=1, keepdims=True) + EPS)
        unit_row = jnp.sum(jnp.where(eye, unit, 0.0), axis=0, keepdims=True)
        gram = mm(kh, kh, ((1,), (1,))) * unit_row
        cross = mm(qh, kh, ((1,), (1,))) * unit_row
        for e in range(2):
            j = 2 * h + e
            total_row = jnp.sum(jnp.where(entry == j, sums[e], 0.0), axis=0, keepdims=True)
            total = upright(total_row)
            b = upright(jnp.sum(jnp.where(entry == j, strength, 0.0), axis=0, keepdims=True))
            last = total[255:256] if e == 0 else total[0:1]
            inside = row >= col if e == 0 else row <= col
            fade = jnp.where(inside, jnp.exp(jnp.where(inside, total - total_row, 0.0)), 0.0)
            lowers.append(jnp.where(eye, 0.0, (b * unit) * gram * fade))
            grown = jnp.exp(total)
            right = jnp.concatenate(
                [
                    b * vh.astype(F32),
                    (b * unit * grown) * kf,
                ],
                axis=1,
            ).astype(BF)
            faded = (kf * (unit * jnp.exp(last - total))).astype(BF)
            scores = (cross * fade).astype(BF)
            parts.append((right, faded, scores, grown * qh.astype(F32), jnp.exp(last) - 1.0))
    solved = inverse_of(lowers, row, col)
    small = lax.broadcasted_iota(jnp.int32, (128, 128), 0) == lax.broadcasted_iota(
        jnp.int32, (128, 128), 1
    )
    outs = [None, None]
    for j in range(4):
        right, faded, scores, grown_q, short = parts[j]
        both = mm(solved[j], right).astype(BF)
        maps = mm(faded, both, ((0,), (0,)))
        read = mm(scores, both)
        to = (j + pos[4]) % 4
        m_o[to, 0:128, 0:128] = (jnp.where(small, short, 0.0) - maps[:, 128:]).astype(BF)
        m_o[to, 0:128, 128:256] = maps[:, :128].astype(BF)
        h, e = divmod(j, 2)
        r_o[h, :, 128 * e : 128 * e + 128] = (grown_q - read[:, 128:]).astype(BF)
        outs[h] = read[:, :128] if e == 0 else outs[h] + read[:, :128]
    o_o[:, 0:128] = outs[0]
    o_o[:, 128:256] = outs[1]


def context_state(pos, rows, rate, write, decay, bias, extra):
    row = lax.broadcasted_iota(jnp.int32, (256, 256), 0)
    col = lax.broadcasted_iota(jnp.int32, (256, 256), 1)
    eye = row == col
    lane = pos[1] * 4 + pos[0]
    inside = (row - col) * (1 - 2 * (pos[0] % 2)) >= 0
    kh = rows[:, 0:128].astype(BF)
    kf = rows[:, 0:128]
    logs = -column(decay, lane) * softplus(rate)
    strength = sigmoid(write + column(bias, lane) + column(extra, lane))
    b = jnp.sum(jnp.where(eye, strength, 0.0), axis=1, keepdims=True)
    total = jnp.sum(jnp.where(inside, logs, 0.0), axis=1, keepdims=True)
    total_row = jnp.sum(jnp.where(eye, total, 0.0), axis=0, keepdims=True)
    last = jnp.sum(logs, axis=1, keepdims=True)
    unit = lax.rsqrt(jnp.sum(kf * kf, axis=1, keepdims=True) + EPS)
    unit_row = jnp.sum(jnp.where(eye, unit, 0.0), axis=0, keepdims=True)
    fade = jnp.where(inside, jnp.exp(jnp.where(inside, total - total_row, 0.0)), 0.0)
    lower = jnp.where(
        eye, 0.0, (b * unit) * (mm(kh, kh, ((1,), (1,))) * unit_row) * fade
    )
    solved = inverse_of([lower], row, col)[0]
    fresh = mm(solved, b * rows[:, 128:256])
    faded = kf * (unit * jnp.exp(last - total))
    return mm(faded, fresh, ((0,), (0,)))


def apply_to(linear, state):
    high = state.astype(BF)
    low = (state - high.astype(F32)).astype(BF)
    both = mm(linear, jnp.concatenate([high, low], axis=1))
    n = state.shape[1]
    return both[:, :n] + both[:, n:]


def composed(pos, maps):
    back = pos[0] % 2
    at = back * 3
    step = 1 - 2 * back
    total = maps[at][0:128].astype(F32)
    for _ in range(3):
        at = at + step
        total = total + maps[at][0:128].astype(F32) + apply_to(maps[at][0:128, 0:128], total)
    return total


def low_kernel(pos, maps, o):
    total = composed(pos, maps)
    wide = [maps[i][128:].astype(F32) for i in range(4)]
    parts = [w[0:4] for w in wide]
    parts += [sum(w[4:6] for w in wide), jnp.zeros((14, 256), F32)]
    out = jnp.concatenate([total, *parts], axis=0).astype(BF)
    for i in range(4):
        o[i] = out


def high_kernel(pos, maps, o, rows):
    wide = [maps[i][128:].astype(F32) for i in range(4)]
    parts = [w[0:16] for w in wide]
    parts += [sum(w[16:18] for w in wide), jnp.zeros((6, 256), F32)]
    out = jnp.concatenate(parts, axis=0).astype(BF)
    for i in range(4):
        rows[i] = out
    o[...] = composed(pos, maps).astype(BF)


def context_kernel(pos, all_rows, small, o):
    wide = [all_rows[i].astype(F32) for i in range(4)]
    rows = jnp.concatenate([w[0:64] for w in wide], axis=0)
    gates = sum(w[64:66] for w in wide)
    o[...] = context_state(
        pos, rows, gates[0:1], gates[1:2], small[0:1], small[1:2], small[2:3]
    )


def moved(maps, state):
    return state + maps[:, 128:256].astype(F32) + apply_to(maps[:, 0:128], state)


def scan_kernel(pos, start, far, middle, near, low, own, o):
    back = pos[0] % 2
    step = 1 - 2 * back
    state = start[...]
    for maps in (far, middle, near):
        state = moved(maps[...], state)
    at = back * 3
    for _ in range(3):
        state = jnp.where((pos[3] - at) * step > 0, moved(low[at][0:128], state), state)
        at = at + step
    at = back * 3
    for i in range(4):
        o[at] = state.astype(BF)
        if i < 3:
            state = moved(own[at][0:128], state)
        at = at + step


def read_kernel(pos, states, reads, base, gain, weight, keep, give):
    heads = []
    for h in range(2):
        first = states[(2 * h + pos[4]) % 4]
        second = states[(2 * h + 1 + pos[4]) % 4]
        total = base[:, 128 * h : 128 * h + 128] + (
            mm(reads[h][:, 0:128], first) + mm(reads[h][:, 128:256], second)
        )
        mean = jnp.mean(total * total, axis=1, keepdims=True)
        heads.append((total * lax.rsqrt(mean + EPS) * gain[3:4]).astype(BF))
    branch = mm(jnp.concatenate(heads, axis=1), weight[...]).astype(BF)

    def split(even, odd):
        for i in range(4):
            even[i] = branch[64 * i : 64 * i + 32]
            odd[i] = branch[64 * i + 32 : 64 * i + 64]

    @pl.when(pos[6] == 0)
    def _():
        split(keep, give)

    @pl.when(pos[6] != 0)
    def _():
        split(give, keep)


def merge_kernel(keep, got, o):
    o[...] = (keep[...].astype(F32) + got[...].astype(F32)).astype(BF)


def output_kernel(rows, fac, lat, o):
    branch = (rows[0].astype(F32) + rows[1].astype(F32)) + (
        rows[2].astype(F32) + rows[3].astype(F32)
    )
    o[...] = (lat[...].astype(F32) + factor(fac, 2) * branch).astype(BF)


def call(kernel, outs, specs, scratch=(), flops=1, aliases=None):
    def shape(s):
        return jax.ShapeDtypeStruct(*s)

    many = isinstance(outs, list)
    return pl.pallas_call(
        kernel,
        out_shape=[shape(s) for s in outs] if many else shape(outs),
        in_specs=specs,
        out_specs=[VM] * len(outs) if many else VM,
        scratch_shapes=scratch,
        input_output_aliases=aliases or {},
        compiler_params=pltpu.CompilerParams(vmem_limit_bytes=24 * 2**20),
        cost_estimate=pl.CostEstimate(flops=flops, bytes_accessed=1, transcendentals=0),
    )


def to_all(value, axes, count):
    return lax.all_to_all(
        jnp.broadcast_to(value[None], (count, *value.shape)), axes, 0, 0, tiled=True
    )


def onward(d):
    pairs = []
    for zh in range(4):
        for y in range(4):
            for c in range(2):
                to = zh + d if (y + c) % 2 == 0 else zh - d
                if 0 <= to < 4:
                    pairs.append((zh * 8 + y * 2 + c, to * 8 + y * 2 + c))
    return pairs


def per_device(
    latent,
    condition,
    context,
    context_condition_vector,
    modulation_matrix,
    query_matrix,
    key_matrix,
    value_matrix,
    decay_input_weight,
    write_strength_weight,
    head_decay_rate,
    write_strength_bias,
    context_write_offset_bias,
    log_spike_added,
    head_norm_gain,
    output_matrix,
):
    zh, zl, y = (lax.axis_index("zh"), lax.axis_index("zl"), lax.axis_index("y"))
    x, c = (lax.axis_index("x"), lax.axis_index("c"))
    sp_index = lax.axis_index(SP)
    pos = jnp.stack([(y + c) % 4, x * 2 + c, zh, zl, (4 - c) % 4, sp_index * 4, c, x])
    pos = pos.astype(jnp.int32)
    parts = [latent]
    for d in range(1, 4):
        parts.append(lax.ppermute(latent, "x", [(i, (i + d) % 4) for i in range(4)]))
    mine = jnp.stack(parts)
    other = lax.ppermute(mine, "c", [(0, 1), (1, 0)])
    signals = jnp.stack([condition, context_condition_vector])
    signals = lax.dynamic_slice_in_dim(jax.nn.silu(signals), sp_index * 32, 32, 1)
    mod = modulation_matrix.astype(F32)
    part = jnp.concatenate(
        [
            jnp.sum(mod * signals[0][None, :, None], axis=1),
            jnp.sum(mod[:2] * signals[1][None, :, None], axis=1),
        ]
    )
    part = to_all(part, Z, 16)
    part = jnp.sum(part, axis=0)
    fac = to_all(part, ("y", "x", "c"), 32)

    small = jnp.stack(
        [
            jnp.pad(head_decay_rate, (0, 96)),
            jnp.pad(write_strength_bias, (0, 96)),
            jnp.pad(context_write_offset_bias, (0, 96)),
            head_norm_gain,
        ]
    )
    slow = [
        pltpu.with_memory_space_constraint(a, pltpu.HBM)
        for a in (
            context,
            query_matrix,
            key_matrix,
            value_matrix,
            decay_input_weight.T,
            write_strength_weight.T,
            log_spike_added.T,
        )
    ]
    room = [
        pltpu.VMEM((4, D), BF),
        pltpu.VMEM((D, 256), BF),
        pltpu.VMEM((D, 256), BF),
        pltpu.VMEM((D, 256), BF),
        pltpu.VMEM((32, D), BF),
        pltpu.VMEM((32, D), BF),
        pltpu.VMEM((32, 256), F32),
        pltpu.SemaphoreType.DMA((7,)),
    ]
    maps, reads, base = call(
        front_kernel,
        [((4, 144, 256), BF), ((2, 256, 256), BF), ((256, 256), F32)],
        [SM] + [VM] * 4 + [HB] * 7,
        [pltpu.VMEM((272, D), BF), pltpu.VMEM((832, 256), BF), *room],
        flops=5 * 10**9,
    )(
        pos,
        mine,
        other,
        fac,
        small,
        *slow,
    )
    of_y = lax.all_to_all(maps, "y", 0, 0, tiled=True)
    low = call(low_kernel, ((4, 160, 256), BF), [SM, VM])(pos, of_y)
    of_low = lax.all_to_all(low, "zl", 0, 0, tiled=True)
    high, rows = call(high_kernel, [((128, 256), BF), ((4, 72, 256), BF)], [SM, VM])(pos, of_low)
    rows = lax.all_to_all(rows, "zh", 0, 0, tiled=True)
    of_high = []
    for d in (3, 2, 1):
        of_high.append(lax.ppermute(high, ("zh", "y", "c"), onward(d)))
    start = call(context_kernel, ((128, 128), F32), [SM] + [VM] * 2, flops=10**9)(pos, rows, small)
    states = call(scan_kernel, ((4, 128, 128), BF), [SM] + [VM] * 6, flops=10**8)(
        pos, start, *of_high, of_low, of_y
    )
    states = lax.all_to_all(states, "y", 0, 0, tiled=True)
    keep, give = call(
        read_kernel, [((4, 32, D), BF)] * 2, [SM] + [VM] * 5, flops=10**8
    )(pos, states, reads, base, small, output_matrix)
    got = lax.ppermute(give, "c", [(0, 1), (1, 0)])
    branch = call(merge_kernel, ((4, 32, D), BF), [VM] * 2)(keep, got)
    branch = lax.all_to_all(branch, "x", 0, 0, tiled=True)
    return call(output_kernel, ((32, D), BF), [VM] * 3, flops=10**8)(branch, fac, latent)


def solution(mesh):
    split = Mesh(mesh.devices.reshape(4, 4, 4, 4, 2), ALL)
    return jax.shard_map(
        per_device,
        mesh=split,
        in_specs=(
            P(ALL, None),
            P(),
            P(SP, None),
            P(),
            P(None, SP, TP),
            P(None, TP),
            P(None, TP),
            P(None, TP),
            P(),
            P(),
            P(),
            P(),
            P(),
            P(SP, None),
            P(),
            P(TP, None),
        ),
        out_specs=P(ALL, None),
        check_vma=False,
    )
```

```python
import jax
import jax.numpy as jnp
from jax import lax
from jax.experimental import pallas as pl
from jax.experimental.pallas import tpu as pltpu
from jax.sharding import Mesh
from jax.sharding import PartitionSpec as P


D = 2048
EPS = 1e-06
HI = lax.Precision.HIGHEST
F32 = jnp.float32
BF = jnp.bfloat16
Z = ("zh", "zl")
TP = ("x", "c")
SP = ("zh", "zl", "y")
ALL = ("zh", "zl", "y", "x", "c")
VM = pl.BlockSpec(memory_space=pltpu.VMEM)
SM = pl.BlockSpec(memory_space=pltpu.SMEM)
HB = pl.BlockSpec(memory_space=pltpu.HBM)


def mm(a, b, dims=((1,), (0,))):
    return lax.dot_general(
        a.astype(BF), b.astype(BF), (dims, ((), ())), preferred_element_type=F32
    )


def norm_rows(rows, scale, shift):
    wide = rows.astype(F32)
    centred = wide - jnp.mean(wide, axis=-1, keepdims=True)
    spread = jnp.mean(centred * centred, axis=-1, keepdims=True)
    return (centred * lax.rsqrt(spread + EPS) * (1.0 + scale) + shift).astype(BF)


def column(matrix, lane):
    lanes = lax.broadcasted_iota(jnp.int32, matrix.shape, 1)
    return jnp.sum(jnp.where(lanes == lane, matrix, 0.0), axis=1, keepdims=True)


def softplus(t):
    return jnp.maximum(t, 0.0) + jnp.log1p(jnp.exp(-jnp.abs(t)))


def sigmoid(t):
    return 1.0 / (1.0 + jnp.exp(-t))


def inverse_of(lower, row, col):
    eye = (row == col).astype(F32)
    own = (row // 16) == (col // 16)
    base = [jnp.where(own, m, 0.0) for m in lower]
    inv = [eye - m for m in base]
    power = [mm(m, m) for m in base]
    for step in range(3):
        inv = [p + mm(p, x) for p, x in zip(inv, power)]
        if step < 2:
            power = [mm(x, x) for x in power]
    size = 16
    while size < 256:
        here = ((row // (2 * size)) == (col // (2 * size))) & ((row // size) != (col // size))
        side = [mm(jnp.where(here, m, 0.0), p) for m, p in zip(lower, inv)]
        inv = [p - mm(p, s) for p, s in zip(inv, side)]
        size *= 2
    out = []
    for m, p in zip(lower, inv):
        first = p.astype(BF)
        high = m.astype(BF)
        low = (m - high.astype(F32)).astype(BF)
        wide = first.astype(F32)
        left = (eye - wide) - (mm(high, first) + mm(low, first))
        out.append(wide + mm(first, left))
    return out


def start_copies(sources, targets, sems):
    copies = [
        pltpu.make_async_copy(source, target, sems.at[i])
        for i, (source, target) in enumerate(zip(sources, targets))
    ]
    for copy in copies:
        copy.start()
    return copies


def factor(fac, r):
    parts = [(fac[t] + fac[8 + t]) + (fac[16 + t] + fac[24 + t]) for t in range(8)]
    return jnp.concatenate([f[r : r + 1] for f in parts], axis=1)


def front_kernel(
    pos, one, two, fac, small, ctx_h, wq_h, wk_h, wv_h, wd_h, ww_h, spike_h,
    m_o, r_o, o_o,
    hid, packed, ctx, wq, wk, wv, wd, ww, spike, sems,
):
    copies = start_copies(
        (ctx_h, wq_h, wk_h, wv_h, wd_h, ww_h, spike_h), (ctx, wq, wk, wv, wd, ww, spike), sems
    )
    shift, scale = (factor(fac, 0), factor(fac, 1))
    for d in range(4):
        for i, lat in enumerate((one, two)):
            core = pos[6] if i == 0 else 1 - pos[6]
            spot = (2 * ((pos[7] + 4 - d) % 4) + core) * 32
            hid[pl.ds(pl.multiple_of(spot, 32), 32)] = norm_rows(lat[d], scale, shift)
    copies[0].wait()
    hid[256:260] = norm_rows(ctx[...], factor(fac, 4), factor(fac, 3))
    hid[260:272] = jnp.zeros((12, D), BF)
    rows = hid[...]
    copies[1].wait()
    packed[0:256] = mm(hid[0:256], wq[...]).astype(BF)
    copies[2].wait()
    keys = mm(rows, wk[...]).astype(BF)
    packed[256:512] = keys[:256]
    for copy in copies[3:]:
        copy.wait()
    values = mm(rows, wv[...]).astype(BF)
    packed[512:768] = values[:256]
    packed[768:800] = mm(wd[...], hid[0:256], ((1,), (1,))).astype(BF)
    packed[800:832] = mm(ww[...], hid[0:256], ((1,), (1,))).astype(BF)
    rate = mm(hid[256:272], wd[...], ((1,), (1,))).astype(BF).astype(F32)
    write = mm(hid[256:272], ww[...], ((1,), (1,))).astype(BF).astype(F32)
    lanes = lax.broadcasted_iota(jnp.int32, (16, 256), 1)
    rank = lax.broadcasted_iota(jnp.int32, (16, 256), 0)
    spots = (lanes == rank + pos[5]) & (rank < 4)
    wide = [side[256:272].astype(F32)[0:4] for side in (keys, values)]
    for j in range(4):
        h = j // 2
        lane = pos[1] * 4 + j
        pieces = [jnp.concatenate([w[:, 128 * h : 128 * h + 128] for w in wide], axis=1)]
        pieces += [
            jnp.sum(jnp.where(spots, column(g, lane), 0.0), axis=0, keepdims=True)
            for g in (rate, write)
        ]
        pieces.append(jnp.zeros((10, 256), F32))
        m_o[(j + pos[4]) % 4, 128:144] = jnp.concatenate(pieces, axis=0).astype(BF)
    chunk(pos, packed, spike, small, m_o, r_o, o_o)


def chunk(pos, packed, spike, small, m_o, r_o, o_o):
    row = lax.broadcasted_iota(jnp.int32, (256, 256), 0)
    col = lax.broadcasted_iota(jnp.int32, (256, 256), 1)
    eye = row == col
    entry = lax.broadcasted_iota(jnp.int32, (32, 128), 0)
    entry = entry == lax.broadcasted_iota(jnp.int32, (32, 128), 1)
    decay, bias = (
        jnp.sum(jnp.where(entry, small[i : i + 1], 0.0), axis=1, keepdims=True) for i in range(2)
    )
    logs = -decay * softplus(packed[768:800].astype(F32)) + spike[...]
    strength = sigmoid(packed[800:832].astype(F32) + bias)
    entry = lax.broadcasted_iota(jnp.int32, (32, 256), 0) - pos[1] * 4
    below = (row >= col).astype(F32)
    above = (row <= col).astype(F32)
    sums = (
        jnp.dot(logs, above, precision=HI, preferred_element_type=F32),
        jnp.dot(logs, below, precision=HI, preferred_element_type=F32),
    )

    def upright(line):
        return jnp.sum(jnp.where(eye, line, 0.0), axis=1, keepdims=True)

    lowers, parts = ([], [])
    for h in range(2):
        qh, kh, vh = (packed[256 * i : 256 * i + 256, 128 * h : 128 * h + 128] for i in range(3))
        kf = kh.astype(F32)
        unit = lax.rsqrt(jnp.sum(kf * kf, axis=1, keepdims=True) + EPS)
        unit_row = jnp.sum(jnp.where(eye, unit, 0.0), axis=0, keepdims=True)
        gram = mm(kh, kh, ((1,), (1,))) * unit_row
        cross = mm(qh, kh, ((1,), (1,))) * unit_row
        for e in range(2):
            j = 2 * h + e
            total_row = jnp.sum(jnp.where(entry == j, sums[e], 0.0), axis=0, keepdims=True)
            total = upright(total_row)
            b = upright(jnp.sum(jnp.where(entry == j, strength, 0.0), axis=0, keepdims=True))
            last = total[255:256] if e == 0 else total[0:1]
            inside = row >= col if e == 0 else row <= col
            fade = jnp.where(inside, jnp.exp(jnp.where(inside, total - total_row, 0.0)), 0.0)
            lowers.append(jnp.where(eye, 0.0, (b * unit) * gram * fade))
            grown = jnp.exp(total)
            right = jnp.concatenate(
                [
                    b * vh.astype(F32),
                    (b * unit * grown) * kf,
                ],
                axis=1,
            ).astype(BF)
            faded = (kf * (unit * jnp.exp(last - total))).astype(BF)
            scores = (cross * fade).astype(BF)
            parts.append((right, faded, scores, grown * qh.astype(F32), jnp.exp(last) - 1.0))
    solved = inverse_of(lowers, row, col)
    small = lax.broadcasted_iota(jnp.int32, (128, 128), 0) == lax.broadcasted_iota(
        jnp.int32, (128, 128), 1
    )
    outs = [None, None]
    for j in range(4):
        right, faded, scores, grown_q, short = parts[j]
        both = mm(solved[j], right).astype(BF)
        maps = mm(faded, both, ((0,), (0,)))
        read = mm(scores, both)
        to = (j + pos[4]) % 4
        m_o[to, 0:128, 0:128] = (jnp.where(small, short, 0.0) - maps[:, 128:]).astype(BF)
        m_o[to, 0:128, 128:256] = maps[:, :128].astype(BF)
        h, e = divmod(j, 2)
        r_o[h, :, 128 * e : 128 * e + 128] = (grown_q - read[:, 128:]).astype(BF)
        outs[h] = read[:, :128] if e == 0 else outs[h] + read[:, :128]
    o_o[:, 0:128] = outs[0]
    o_o[:, 128:256] = outs[1]


def context_state(pos, rows, rate, write, decay, bias, extra):
    row = lax.broadcasted_iota(jnp.int32, (256, 256), 0)
    col = lax.broadcasted_iota(jnp.int32, (256, 256), 1)
    eye = row == col
    lane = pos[1] * 4 + pos[0]
    inside = (row - col) * (1 - 2 * (pos[0] % 2)) >= 0
    kh = rows[:, 0:128].astype(BF)
    kf = rows[:, 0:128]
    logs = -column(decay, lane) * softplus(rate)
    strength = sigmoid(write + column(bias, lane) + column(extra, lane))
    b = jnp.sum(jnp.where(eye, strength, 0.0), axis=1, keepdims=True)
    total = jnp.sum(jnp.where(inside, logs, 0.0), axis=1, keepdims=True)
    total_row = jnp.sum(jnp.where(eye, total, 0.0), axis=0, keepdims=True)
    last = jnp.sum(logs, axis=1, keepdims=True)
    unit = lax.rsqrt(jnp.sum(kf * kf, axis=1, keepdims=True) + EPS)
    unit_row = jnp.sum(jnp.where(eye, unit, 0.0), axis=0, keepdims=True)
    fade = jnp.where(inside, jnp.exp(jnp.where(inside, total - total_row, 0.0)), 0.0)
    lower = jnp.where(
        eye, 0.0, (b * unit) * (mm(kh, kh, ((1,), (1,))) * unit_row) * fade
    )
    solved = inverse_of([lower], row, col)[0]
    fresh = mm(solved, b * rows[:, 128:256])
    faded = kf * (unit * jnp.exp(last - total))
    return mm(faded, fresh, ((0,), (0,)))


def apply_to(linear, state):
    high = state.astype(BF)
    low = (state - high.astype(F32)).astype(BF)
    both = mm(linear, jnp.concatenate([high, low], axis=1))
    n = state.shape[1]
    return both[:, :n] + both[:, n:]


def composed(pos, maps):
    back = pos[0] % 2
    at = back * 3
    step = 1 - 2 * back
    total = maps[at][0:128].astype(F32)
    for _ in range(3):
        at = at + step
        total = total + maps[at][0:128].astype(F32) + apply_to(maps[at][0:128, 0:128], total)
    return total


def low_kernel(pos, maps, o, rows):
    wide = [maps[i][128:].astype(F32) for i in range(4)]
    parts = [w[0:4] for w in wide]
    parts += [sum(w[4:6] for w in wide), jnp.zeros((6, 256), F32)]
    rows[...] = jnp.concatenate(parts, axis=0).astype(BF)
    out = composed(pos, maps).astype(BF)
    for i in range(4):
        o[i] = out


def high_kernel(pos, maps, r0, r1, r2, r3, o, rows):
    gates = jnp.zeros((2, 256), F32)
    for d, part in enumerate((r0, r1, r2, r3)):
        wide = part[...].astype(F32)
        gates = gates + wide[16:18]
        spot = pl.multiple_of(((pos[2] + 4 - d) % 4) * 16, 16)
        for i in range(4):
            rows[i, pl.ds(spot, 16)] = part[0:16]
    tail = jnp.concatenate([gates, jnp.zeros((14, 256), F32)], axis=0).astype(BF)
    for i in range(4):
        rows[i, 64:80] = tail
    o[...] = composed(pos, maps).astype(BF)


def context_kernel(pos, all_rows, small, o):
    wide = [all_rows[i].astype(F32) for i in range(4)]
    rows = jnp.concatenate([w[16 * i : 16 * i + 16] for i in range(4) for w in wide], axis=0)
    gates = sum(w[64:66] for w in wide)
    o[...] = context_state(
        pos, rows, gates[0:1], gates[1:2], small[0:1], small[1:2], small[2:3]
    )


def moved(maps, state):
    return state + maps[:, 128:256].astype(F32) + apply_to(maps[:, 0:128], state)


def scan_kernel(pos, start, far, middle, near, low, own, o):
    back = pos[0] % 2
    step = 1 - 2 * back
    state = start[...]
    for maps in (far, middle, near):
        state = moved(maps[...], state)
    at = back * 3
    for _ in range(3):
        state = jnp.where((pos[3] - at) * step > 0, moved(low[at][0:128], state), state)
        at = at + step
    at = back * 3
    for i in range(4):
        o[at] = state.astype(BF)
        if i < 3:
            state = moved(own[at][0:128], state)
        at = at + step


def read_kernel(pos, states, reads, base, gain, weight, keep, give):
    heads = []
    for h in range(2):
        first = states[(2 * h + pos[4]) % 4]
        second = states[(2 * h + 1 + pos[4]) % 4]
        total = base[:, 128 * h : 128 * h + 128] + (
            mm(reads[h][:, 0:128], first) + mm(reads[h][:, 128:256], second)
        )
        mean = jnp.mean(total * total, axis=1, keepdims=True)
        heads.append((total * lax.rsqrt(mean + EPS) * gain[3:4]).astype(BF))
    branch = mm(jnp.concatenate(heads, axis=1), weight[...]).astype(BF)

    def split(even, odd):
        for i in range(4):
            even[i] = branch[64 * i : 64 * i + 32]
            odd[i] = branch[64 * i + 32 : 64 * i + 64]

    @pl.when(pos[6] == 0)
    def _():
        split(keep, give)

    @pl.when(pos[6] != 0)
    def _():
        split(give, keep)


def merge_kernel(keep, got, o):
    o[...] = (keep[...].astype(F32) + got[...].astype(F32)).astype(BF)


def output_kernel(rows, fac, lat, o):
    branch = (rows[0].astype(F32) + rows[1].astype(F32)) + (
        rows[2].astype(F32) + rows[3].astype(F32)
    )
    o[...] = (lat[...].astype(F32) + factor(fac, 2) * branch).astype(BF)


def call(kernel, outs, specs, scratch=(), flops=1, aliases=None):
    def shape(s):
        return jax.ShapeDtypeStruct(*s)

    many = isinstance(outs, list)
    return pl.pallas_call(
        kernel,
        out_shape=[shape(s) for s in outs] if many else shape(outs),
        in_specs=specs,
        out_specs=[VM] * len(outs) if many else VM,
        scratch_shapes=scratch,
        input_output_aliases=aliases or {},
        compiler_params=pltpu.CompilerParams(vmem_limit_bytes=24 * 2**20),
        cost_estimate=pl.CostEstimate(flops=flops, bytes_accessed=1, transcendentals=0),
    )


def to_all(value, axes, count):
    return lax.all_to_all(
        jnp.broadcast_to(value[None], (count, *value.shape)), axes, 0, 0, tiled=True
    )


def onward(d):
    pairs = []
    for zh in range(4):
        for y in range(4):
            for c in range(2):
                to = zh + d if (y + c) % 2 == 0 else zh - d
                if 0 <= to < 4:
                    pairs.append((zh * 8 + y * 2 + c, to * 8 + y * 2 + c))
    return pairs


def per_device(
    latent,
    condition,
    context,
    context_condition_vector,
    modulation_matrix,
    query_matrix,
    key_matrix,
    value_matrix,
    decay_input_weight,
    write_strength_weight,
    head_decay_rate,
    write_strength_bias,
    context_write_offset_bias,
    log_spike_added,
    head_norm_gain,
    output_matrix,
):
    zh, zl, y = (lax.axis_index("zh"), lax.axis_index("zl"), lax.axis_index("y"))
    x, c = (lax.axis_index("x"), lax.axis_index("c"))
    sp_index = lax.axis_index(SP)
    pos = jnp.stack([(y + c) % 4, x * 2 + c, zh, zl, (4 - c) % 4, sp_index * 4, c, x])
    pos = pos.astype(jnp.int32)
    parts = [latent]
    for d in range(1, 4):
        parts.append(lax.ppermute(latent, "x", [(i, (i + d) % 4) for i in range(4)]))
    mine = jnp.stack(parts)
    other = lax.ppermute(mine, "c", [(0, 1), (1, 0)])
    signals = jnp.stack([condition, context_condition_vector])
    signals = lax.dynamic_slice_in_dim(jax.nn.silu(signals), sp_index * 32, 32, 1)
    mod = modulation_matrix.astype(F32)
    part = jnp.concatenate(
        [
            jnp.sum(mod * signals[0][None, :, None], axis=1),
            jnp.sum(mod[:2] * signals[1][None, :, None], axis=1),
        ]
    )
    part = to_all(part, Z, 16)
    part = jnp.sum(part, axis=0)
    fac = to_all(part, ("y", "x", "c"), 32)

    small = jnp.stack(
        [
            jnp.pad(head_decay_rate, (0, 96)),
            jnp.pad(write_strength_bias, (0, 96)),
            jnp.pad(context_write_offset_bias, (0, 96)),
            head_norm_gain,
        ]
    )
    slow = [
        pltpu.with_memory_space_constraint(a, pltpu.HBM)
        for a in (
            context,
            query_matrix,
            key_matrix,
            value_matrix,
            decay_input_weight.T,
            write_strength_weight.T,
            log_spike_added.T,
        )
    ]
    room = [
        pltpu.VMEM((4, D), BF),
        pltpu.VMEM((D, 256), BF),
        pltpu.VMEM((D, 256), BF),
        pltpu.VMEM((D, 256), BF),
        pltpu.VMEM((32, D), BF),
        pltpu.VMEM((32, D), BF),
        pltpu.VMEM((32, 256), F32),
        pltpu.SemaphoreType.DMA((7,)),
    ]
    maps, reads, base = call(
        front_kernel,
        [((4, 144, 256), BF), ((2, 256, 256), BF), ((256, 256), F32)],
        [SM] + [VM] * 4 + [HB] * 7,
        [pltpu.VMEM((272, D), BF), pltpu.VMEM((832, 256), BF), *room],
        flops=5 * 10**9,
    )(
        pos,
        mine,
        other,
        fac,
        small,
        *slow,
    )
    of_y = lax.all_to_all(maps, "y", 0, 0, tiled=True)
    low, rows = call(
        low_kernel, [((4, 128, 256), BF), ((24, 256), BF)], [SM, VM]
    )(pos, of_y)
    of_low = lax.all_to_all(low, "zl", 0, 0, tiled=True)
    parts = [rows]
    for d in range(1, 4):
        parts.append(lax.ppermute(rows, "zh", [(i, (i + d) % 4) for i in range(4)]))
    high, rows = call(
        high_kernel, [((128, 256), BF), ((4, 80, 256), BF)], [SM] + [VM] * 5
    )(pos, of_low, *parts)
    rows = lax.all_to_all(rows, "zl", 0, 0, tiled=True)
    of_high = []
    for d in (3, 2, 1):
        of_high.append(lax.ppermute(high, ("zh", "y", "c"), onward(d)))
    start = call(context_kernel, ((128, 128), F32), [SM] + [VM] * 2, flops=10**9)(pos, rows, small)
    states = call(scan_kernel, ((4, 128, 128), BF), [SM] + [VM] * 6, flops=10**8)(
        pos, start, *of_high, of_low, of_y
    )
    states = lax.all_to_all(states, "y", 0, 0, tiled=True)
    keep, give = call(
        read_kernel, [((4, 32, D), BF)] * 2, [SM] + [VM] * 5, flops=10**8
    )(pos, states, reads, base, small, output_matrix)
    got = lax.ppermute(give, "c", [(0, 1), (1, 0)])
    branch = call(merge_kernel, ((4, 32, D), BF), [VM] * 2)(keep, got)
    branch = lax.all_to_all(branch, "x", 0, 0, tiled=True)
    return call(output_kernel, ((32, D), BF), [VM] * 3, flops=10**8)(branch, fac, latent)


def solution(mesh):
    split = Mesh(mesh.devices.reshape(4, 4, 4, 4, 2), ALL)
    return jax.shard_map(
        per_device,
        mesh=split,
        in_specs=(
            P(ALL, None),
            P(),
            P(SP, None),
            P(),
            P(None, SP, TP),
            P(None, TP),
            P(None, TP),
            P(None, TP),
            P(),
            P(),
            P(),
            P(),
            P(),
            P(SP, None),
            P(),
            P(TP, None),
        ),
        out_specs=P(ALL, None),
        check_vma=False,
    )
```

```python
import jax
import jax.numpy as jnp
from jax import lax
from jax.experimental import pallas as pl
from jax.experimental.pallas import tpu as pltpu
from jax.sharding import Mesh
from jax.sharding import PartitionSpec as P


D = 2048
EPS = 1e-06
HI = lax.Precision.HIGHEST
F32 = jnp.float32
BF = jnp.bfloat16
Z = ("zh", "zl")
TP = ("x", "c")
SP = ("zh", "zl", "y")
ALL = ("zh", "zl", "y", "x", "c")
VM = pl.BlockSpec(memory_space=pltpu.VMEM)
SM = pl.BlockSpec(memory_space=pltpu.SMEM)
HB = pl.BlockSpec(memory_space=pltpu.HBM)


def mm(a, b, dims=((1,), (0,))):
    return lax.dot_general(
        a.astype(BF), b.astype(BF), (dims, ((), ())), preferred_element_type=F32
    )


def norm_rows(rows, scale, shift):
    wide = rows.astype(F32)
    centred = wide - jnp.mean(wide, axis=-1, keepdims=True)
    spread = jnp.mean(centred * centred, axis=-1, keepdims=True)
    return (centred * lax.rsqrt(spread + EPS) * (1.0 + scale) + shift).astype(BF)


def column(matrix, lane):
    lanes = lax.broadcasted_iota(jnp.int32, matrix.shape, 1)
    return jnp.sum(jnp.where(lanes == lane, matrix, 0.0), axis=1, keepdims=True)


def softplus(t):
    return jnp.maximum(t, 0.0) + jnp.log1p(jnp.exp(-jnp.abs(t)))


def sigmoid(t):
    return 1.0 / (1.0 + jnp.exp(-t))


def inverse_of(lower, row, col):
    eye = (row == col).astype(F32)
    own = (row // 16) == (col // 16)
    base = [jnp.where(own, m, 0.0) for m in lower]
    inv = [eye - m for m in base]
    power = [mm(m, m) for m in base]
    for step in range(3):
        inv = [p + mm(p, x) for p, x in zip(inv, power)]
        if step < 2:
            power = [mm(x, x) for x in power]
    size = 16
    while size < 256:
        here = ((row // (2 * size)) == (col // (2 * size))) & ((row // size) != (col // size))
        side = [mm(jnp.where(here, m, 0.0), p) for m, p in zip(lower, inv)]
        inv = [p - mm(p, s) for p, s in zip(inv, side)]
        size *= 2
    out = []
    for m, p in zip(lower, inv):
        first = p.astype(BF)
        high = m.astype(BF)
        low = (m - high.astype(F32)).astype(BF)
        wide = first.astype(F32)
        left = (eye - wide) - (mm(high, first) + mm(low, first))
        out.append(wide + mm(first, left))
    return out


def start_copies(sources, targets, sems):
    copies = [
        pltpu.make_async_copy(source, target, sems.at[i])
        for i, (source, target) in enumerate(zip(sources, targets))
    ]
    for copy in copies:
        copy.start()
    return copies


def factor(fac, r):
    parts = [(fac[t] + fac[8 + t]) + (fac[16 + t] + fac[24 + t]) for t in range(8)]
    return jnp.concatenate([f[r : r + 1] for f in parts], axis=1)


def front_kernel(
    pos, one, two, fac, small, ctx, wq_h, wk_h, wv_h, wd_h, ww_h, spike_h,
    m_o, r_o, o_o,
    hid, packed, wq, wk, wv, wd, ww, spike, sems,
):
    copies = start_copies(
        (wq_h, wk_h, wv_h, wd_h, ww_h, spike_h), (wq, wk, wv, wd, ww, spike), sems
    )
    shift, scale = (factor(fac, 0), factor(fac, 1))
    for d in range(4):
        for i, lat in enumerate((one, two)):
            core = pos[6] if i == 0 else 1 - pos[6]
            spot = (2 * ((pos[7] + 4 - d) % 4) + core) * 32
            hid[pl.ds(pl.multiple_of(spot, 32), 32)] = norm_rows(lat[d], scale, shift)
    hid[256:320] = norm_rows(ctx[...], factor(fac, 4), factor(fac, 3))
    rows = hid[...]
    copies[0].wait()
    packed[0:256] = mm(hid[0:256], wq[...]).astype(BF)
    copies[1].wait()
    keys = mm(rows, wk[...]).astype(BF)
    packed[256:512] = keys[:256]
    for copy in copies[2:]:
        copy.wait()
    values = mm(rows, wv[...]).astype(BF)
    packed[512:768] = values[:256]
    packed[768:800] = mm(wd[...], hid[0:256], ((1,), (1,))).astype(BF)
    packed[800:832] = mm(ww[...], hid[0:256], ((1,), (1,))).astype(BF)
    rate = mm(hid[256:320], wd[...], ((1,), (1,))).astype(BF).astype(F32)
    write = mm(hid[256:320], ww[...], ((1,), (1,))).astype(BF).astype(F32)
    lanes = lax.broadcasted_iota(jnp.int32, (64, 256), 1)
    rank = lax.broadcasted_iota(jnp.int32, (64, 256), 0)
    spots = lanes == (rank // 4) * 16 + rank % 4 + pos[5]
    for j in range(4):
        h = j // 2
        lane = pos[1] * 4 + j
        to = (j + pos[4]) % 4
        m_o[to, 128:192, 0:128] = keys[256:320, 128 * h : 128 * h + 128]
        m_o[to, 128:192, 128:256] = values[256:320, 128 * h : 128 * h + 128]
        pieces = [
            jnp.sum(jnp.where(spots, column(g, lane), 0.0), axis=0, keepdims=True)
            for g in (rate, write)
        ]
        pieces.append(jnp.zeros((14, 256), F32))
        m_o[to, 192:208] = jnp.concatenate(pieces, axis=0).astype(BF)
    chunk(pos, packed, spike, small, m_o, r_o, o_o)


def chunk(pos, packed, spike, small, m_o, r_o, o_o):
    row = lax.broadcasted_iota(jnp.int32, (256, 256), 0)
    col = lax.broadcasted_iota(jnp.int32, (256, 256), 1)
    eye = row == col
    entry = lax.broadcasted_iota(jnp.int32, (32, 128), 0)
    entry = entry == lax.broadcasted_iota(jnp.int32, (32, 128), 1)
    decay, bias = (
        jnp.sum(jnp.where(entry, small[i : i + 1], 0.0), axis=1, keepdims=True) for i in range(2)
    )
    logs = -decay * softplus(packed[768:800].astype(F32)) + spike[...]
    strength = sigmoid(packed[800:832].astype(F32) + bias)
    entry = lax.broadcasted_iota(jnp.int32, (32, 256), 0) - pos[1] * 4
    below = (row >= col).astype(F32)
    above = (row <= col).astype(F32)
    sums = (
        jnp.dot(logs, above, precision=HI, preferred_element_type=F32),
        jnp.dot(logs, below, precision=HI, preferred_element_type=F32),
    )

    def upright(line):
        return jnp.sum(jnp.where(eye, line, 0.0), axis=1, keepdims=True)

    lowers, parts = ([], [])
    for h in range(2):
        qh, kh, vh = (packed[256 * i : 256 * i + 256, 128 * h : 128 * h + 128] for i in range(3))
        kf = kh.astype(F32)
        unit = lax.rsqrt(jnp.sum(kf * kf, axis=1, keepdims=True) + EPS)
        unit_row = jnp.sum(jnp.where(eye, unit, 0.0), axis=0, keepdims=True)
        gram = mm(kh, kh, ((1,), (1,))) * unit_row
        cross = mm(qh, kh, ((1,), (1,))) * unit_row
        for e in range(2):
            j = 2 * h + e
            total_row = jnp.sum(jnp.where(entry == j, sums[e], 0.0), axis=0, keepdims=True)
            total = upright(total_row)
            b = upright(jnp.sum(jnp.where(entry == j, strength, 0.0), axis=0, keepdims=True))
            last = total[255:256] if e == 0 else total[0:1]
            inside = row >= col if e == 0 else row <= col
            fade = jnp.where(inside, jnp.exp(jnp.where(inside, total - total_row, 0.0)), 0.0)
            lowers.append(jnp.where(eye, 0.0, (b * unit) * gram * fade))
            grown = jnp.exp(total)
            right = jnp.concatenate(
                [
                    b * vh.astype(F32),
                    (b * unit * grown) * kf,
                ],
                axis=1,
            ).astype(BF)
            faded = (kf * (unit * jnp.exp(last - total))).astype(BF)
            scores = (cross * fade).astype(BF)
            parts.append((right, faded, scores, grown * qh.astype(F32), jnp.exp(last) - 1.0))
    solved = inverse_of(lowers, row, col)
    small = lax.broadcasted_iota(jnp.int32, (128, 128), 0) == lax.broadcasted_iota(
        jnp.int32, (128, 128), 1
    )
    outs = [None, None]
    for j in range(4):
        right, faded, scores, grown_q, short = parts[j]
        both = mm(solved[j], right).astype(BF)
        maps = mm(faded, both, ((0,), (0,)))
        read = mm(scores, both)
        to = (j + pos[4]) % 4
        m_o[to, 0:128, 0:128] = (jnp.where(small, short, 0.0) - maps[:, 128:]).astype(BF)
        m_o[to, 0:128, 128:256] = maps[:, :128].astype(BF)
        h, e = divmod(j, 2)
        r_o[h, :, 128 * e : 128 * e + 128] = (grown_q - read[:, 128:]).astype(BF)
        outs[h] = read[:, :128] if e == 0 else outs[h] + read[:, :128]
    o_o[:, 0:128] = outs[0]
    o_o[:, 128:256] = outs[1]


def context_state(pos, rows, rate, write, decay, bias, extra):
    row = lax.broadcasted_iota(jnp.int32, (256, 256), 0)
    col = lax.broadcasted_iota(jnp.int32, (256, 256), 1)
    eye = row == col
    lane = pos[1] * 4 + pos[0]
    inside = (row - col) * (1 - 2 * (pos[0] % 2)) >= 0
    kh = rows[:, 0:128].astype(BF)
    kf = rows[:, 0:128]
    logs = -column(decay, lane) * softplus(rate)
    strength = sigmoid(write + column(bias, lane) + column(extra, lane))
    b = jnp.sum(jnp.where(eye, strength, 0.0), axis=1, keepdims=True)
    total = jnp.sum(jnp.where(inside, logs, 0.0), axis=1, keepdims=True)
    total_row = jnp.sum(jnp.where(eye, total, 0.0), axis=0, keepdims=True)
    last = jnp.sum(logs, axis=1, keepdims=True)
    unit = lax.rsqrt(jnp.sum(kf * kf, axis=1, keepdims=True) + EPS)
    unit_row = jnp.sum(jnp.where(eye, unit, 0.0), axis=0, keepdims=True)
    fade = jnp.where(inside, jnp.exp(jnp.where(inside, total - total_row, 0.0)), 0.0)
    lower = jnp.where(
        eye, 0.0, (b * unit) * (mm(kh, kh, ((1,), (1,))) * unit_row) * fade
    )
    solved = inverse_of([lower], row, col)[0]
    fresh = mm(solved, b * rows[:, 128:256])
    faded = kf * (unit * jnp.exp(last - total))
    return mm(faded, fresh, ((0,), (0,)))


def apply_to(linear, state):
    high = state.astype(BF)
    low = (state - high.astype(F32)).astype(BF)
    both = mm(linear, jnp.concatenate([high, low], axis=1))
    n = state.shape[1]
    return both[:, :n] + both[:, n:]


def composed(pos, maps):
    back = pos[0] % 2
    at = back * 3
    step = 1 - 2 * back
    total = maps[at][0:128].astype(F32)
    for _ in range(3):
        at = at + step
        total = total + maps[at][0:128].astype(F32) + apply_to(maps[at][0:128, 0:128], total)
    return total


def low_kernel(pos, maps, o):
    out = composed(pos, maps).astype(BF)
    for i in range(4):
        o[i] = out


def high_kernel(pos, maps, o):
    o[...] = composed(pos, maps).astype(BF)


def context_kernel(pos, maps, small, o):
    wide = [maps[i][128:].astype(F32) for i in range(4)]
    rows = jnp.concatenate([w[4 * i : 4 * i + 4] for i in range(16) for w in wide], axis=0)
    gates = sum(w[64:66] for w in wide)
    o[...] = context_state(
        pos, rows, gates[0:1], gates[1:2], small[0:1], small[1:2], small[2:3]
    )


def moved(maps, state):
    return state + maps[:, 128:256].astype(F32) + apply_to(maps[:, 0:128], state)


def scan_kernel(pos, start, far, middle, near, low, own, o):
    back = pos[0] % 2
    step = 1 - 2 * back
    state = start[...]
    for maps in (far, middle, near):
        state = moved(maps[...], state)
    at = back * 3
    for _ in range(3):
        state = jnp.where((pos[3] - at) * step > 0, moved(low[at][0:128], state), state)
        at = at + step
    at = back * 3
    for i in range(4):
        o[at] = state.astype(BF)
        if i < 3:
            state = moved(own[at][0:128], state)
        at = at + step


def read_kernel(pos, states, reads, base, gain, weight, keep, give):
    heads = []
    for h in range(2):
        first = states[(2 * h + pos[4]) % 4]
        second = states[(2 * h + 1 + pos[4]) % 4]
        total = base[:, 128 * h : 128 * h + 128] + (
            mm(reads[h][:, 0:128], first) + mm(reads[h][:, 128:256], second)
        )
        mean = jnp.mean(total * total, axis=1, keepdims=True)
        heads.append((total * lax.rsqrt(mean + EPS) * gain[3:4]).astype(BF))
    branch = mm(jnp.concatenate(heads, axis=1), weight[...]).astype(BF)

    def split(even, odd):
        for i in range(4):
            even[i] = branch[64 * i : 64 * i + 32]
            odd[i] = branch[64 * i + 32 : 64 * i + 64]

    @pl.when(pos[6] == 0)
    def _():
        split(keep, give)

    @pl.when(pos[6] != 0)
    def _():
        split(give, keep)


def merge_kernel(keep, got, o):
    o[...] = (keep[...].astype(F32) + got[...].astype(F32)).astype(BF)


def output_kernel(rows, fac, lat, o):
    branch = (rows[0].astype(F32) + rows[1].astype(F32)) + (
        rows[2].astype(F32) + rows[3].astype(F32)
    )
    o[...] = (lat[...].astype(F32) + factor(fac, 2) * branch).astype(BF)


def call(kernel, outs, specs, scratch=(), flops=1, aliases=None):
    def shape(s):
        return jax.ShapeDtypeStruct(*s)

    many = isinstance(outs, list)
    return pl.pallas_call(
        kernel,
        out_shape=[shape(s) for s in outs] if many else shape(outs),
        in_specs=specs,
        out_specs=[VM] * len(outs) if many else VM,
        scratch_shapes=scratch,
        input_output_aliases=aliases or {},
        compiler_params=pltpu.CompilerParams(vmem_limit_bytes=24 * 2**20),
        cost_estimate=pl.CostEstimate(flops=flops, bytes_accessed=1, transcendentals=0),
    )


def to_all(value, axes, count):
    return lax.all_to_all(
        jnp.broadcast_to(value[None], (count, *value.shape)), axes, 0, 0, tiled=True
    )


def onward(d):
    pairs = []
    for zh in range(4):
        for y in range(4):
            for c in range(2):
                to = zh + d if (y + c) % 2 == 0 else zh - d
                if 0 <= to < 4:
                    pairs.append((zh * 8 + y * 2 + c, to * 8 + y * 2 + c))
    return pairs


def per_device(
    latent,
    condition,
    context,
    context_condition_vector,
    modulation_matrix,
    query_matrix,
    key_matrix,
    value_matrix,
    decay_input_weight,
    write_strength_weight,
    head_decay_rate,
    write_strength_bias,
    context_write_offset_bias,
    log_spike_added,
    head_norm_gain,
    output_matrix,
):
    zh, zl, y = (lax.axis_index("zh"), lax.axis_index("zl"), lax.axis_index("y"))
    x, c = (lax.axis_index("x"), lax.axis_index("c"))
    sp_index = lax.axis_index(SP)
    pos = jnp.stack([(y + c) % 4, x * 2 + c, zh, zl, (4 - c) % 4, y * 4, c, x])
    pos = pos.astype(jnp.int32)
    parts = [latent]
    for d in range(1, 4):
        parts.append(lax.ppermute(latent, "x", [(i, (i + d) % 4) for i in range(4)]))
    mine = jnp.stack(parts)
    other = lax.ppermute(mine, "c", [(0, 1), (1, 0)])
    signals = jnp.stack([condition, context_condition_vector])
    signals = lax.dynamic_slice_in_dim(jax.nn.silu(signals), sp_index * 32, 32, 1)
    mod = modulation_matrix.astype(F32)
    part = jnp.concatenate(
        [
            jnp.sum(mod * signals[0][None, :, None], axis=1),
            jnp.sum(mod[:2] * signals[1][None, :, None], axis=1),
        ]
    )
    high = lax.reduce_precision(part, 8, 7)
    sent = jnp.concatenate(
        [
            high.astype(BF),
            (part - high).astype(BF),
            jnp.zeros((6, 256), BF),
            context.reshape(32, 256),
        ]
    )
    sent = to_all(sent, Z, 16)
    part = jnp.sum(sent[:, 0:5].astype(F32) + sent[:, 5:10].astype(F32), axis=0)
    ctx = sent[:, 16:48].reshape(64, D)
    fac = to_all(part, ("y", "x", "c"), 32)

    small = jnp.stack(
        [
            jnp.pad(head_decay_rate, (0, 96)),
            jnp.pad(write_strength_bias, (0, 96)),
            jnp.pad(context_write_offset_bias, (0, 96)),
            head_norm_gain,
        ]
    )
    slow = [
        pltpu.with_memory_space_constraint(a, pltpu.HBM)
        for a in (
            query_matrix,
            key_matrix,
            value_matrix,
            decay_input_weight.T,
            write_strength_weight.T,
            log_spike_added.T,
        )
    ]
    room = [
        pltpu.VMEM((D, 256), BF),
        pltpu.VMEM((D, 256), BF),
        pltpu.VMEM((D, 256), BF),
        pltpu.VMEM((32, D), BF),
        pltpu.VMEM((32, D), BF),
        pltpu.VMEM((32, 256), F32),
        pltpu.SemaphoreType.DMA((6,)),
    ]
    maps, reads, base = call(
        front_kernel,
        [((4, 208, 256), BF), ((2, 256, 256), BF), ((256, 256), F32)],
        [SM] + [VM] * 5 + [HB] * 6,
        [pltpu.VMEM((320, D), BF), pltpu.VMEM((832, 256), BF), *room],
        flops=5 * 10**9,
    )(
        pos,
        mine,
        other,
        fac,
        small,
        ctx,
        *slow,
    )
    of_y = lax.all_to_all(maps, "y", 0, 0, tiled=True)
    low = call(low_kernel, ((4, 128, 256), BF), [SM, VM])(pos, of_y)
    of_low = lax.all_to_all(low, "zl", 0, 0, tiled=True)
    high = call(high_kernel, ((128, 256), BF), [SM, VM])(pos, of_low)
    of_high = []
    for d in (3, 2, 1):
        of_high.append(lax.ppermute(high, ("zh", "y", "c"), onward(d)))
    start = call(context_kernel, ((128, 128), F32), [SM] + [VM] * 2, flops=10**9)(pos, of_y, small)
    states = call(scan_kernel, ((4, 128, 128), BF), [SM] + [VM] * 6, flops=10**8)(
        pos, start, *of_high, of_low, of_y
    )
    states = lax.all_to_all(states, "y", 0, 0, tiled=True)
    keep, give = call(
        read_kernel, [((4, 32, D), BF)] * 2, [SM] + [VM] * 5, flops=10**8
    )(pos, states, reads, base, small, output_matrix)
    got = lax.ppermute(give, "c", [(0, 1), (1, 0)])
    branch = call(merge_kernel, ((4, 32, D), BF), [VM] * 2)(keep, got)
    branch = lax.all_to_all(branch, "x", 0, 0, tiled=True)
    return call(output_kernel, ((32, D), BF), [VM] * 3, flops=10**8)(branch, fac, latent)


def solution(mesh):
    split = Mesh(mesh.devices.reshape(4, 4, 4, 4, 2), ALL)
    return jax.shard_map(
        per_device,
        mesh=split,
        in_specs=(
            P(ALL, None),
            P(),
            P(SP, None),
            P(),
            P(None, SP, TP),
            P(None, TP),
            P(None, TP),
            P(None, TP),
            P(),
            P(),
            P(),
            P(),
            P(),
            P(SP, None),
            P(),
            P(TP, None),
        ),
        out_specs=P(ALL, None),
        check_vma=False,
    )
```

```python
import jax
import jax.numpy as jnp
from jax import lax
from jax.experimental import pallas as pl
from jax.experimental.pallas import tpu as pltpu
from jax.sharding import Mesh
from jax.sharding import PartitionSpec as P


D = 2048
EPS = 1e-06
HI = lax.Precision.HIGHEST
F32 = jnp.float32
BF = jnp.bfloat16
Z = ("zh", "zl")
TP = ("x", "c")
SP = ("zh", "zl", "y")
ALL = ("zh", "zl", "y", "x", "c")
VM = pl.BlockSpec(memory_space=pltpu.VMEM)
SM = pl.BlockSpec(memory_space=pltpu.SMEM)
HB = pl.BlockSpec(memory_space=pltpu.HBM)


def mm(a, b, dims=((1,), (0,))):
    return lax.dot_general(
        a.astype(BF), b.astype(BF), (dims, ((), ())), preferred_element_type=F32
    )


def norm_rows(rows, scale, shift):
    wide = rows.astype(F32)
    centred = wide - jnp.mean(wide, axis=-1, keepdims=True)
    spread = jnp.mean(centred * centred, axis=-1, keepdims=True)
    return (centred * lax.rsqrt(spread + EPS) * (1.0 + scale) + shift).astype(BF)


def column(matrix, lane):
    lanes = lax.broadcasted_iota(jnp.int32, matrix.shape, 1)
    return jnp.sum(jnp.where(lanes == lane, matrix, 0.0), axis=1, keepdims=True)


def softplus(t):
    return jnp.maximum(t, 0.0) + jnp.log1p(jnp.exp(-jnp.abs(t)))


def sigmoid(t):
    return 1.0 / (1.0 + jnp.exp(-t))


def inverse_of(lower, row, col):
    eye = (row == col).astype(F32)
    own = (row // 16) == (col // 16)
    base = [jnp.where(own, m, 0.0) for m in lower]
    inv = [eye - m for m in base]
    power = [mm(m, m) for m in base]
    for step in range(3):
        inv = [p + mm(p, x) for p, x in zip(inv, power)]
        if step < 2:
            power = [mm(x, x) for x in power]
    size = 16
    while size < 256:
        here = ((row // (2 * size)) == (col // (2 * size))) & ((row // size) != (col // size))
        side = [mm(jnp.where(here, m, 0.0), p) for m, p in zip(lower, inv)]
        inv = [p - mm(p, s) for p, s in zip(inv, side)]
        size *= 2
    out = []
    for m, p in zip(lower, inv):
        first = p.astype(BF)
        high = m.astype(BF)
        low = (m - high.astype(F32)).astype(BF)
        wide = first.astype(F32)
        left = (eye - wide) - (mm(high, first) + mm(low, first))
        out.append(wide + mm(first, left))
    return out


def start_copies(sources, targets, sems):
    copies = [
        pltpu.make_async_copy(source, target, sems.at[i])
        for i, (source, target) in enumerate(zip(sources, targets))
    ]
    for copy in copies:
        copy.start()
    return copies


def factor(fac, r):
    parts = [(fac[t] + fac[8 + t]) + (fac[16 + t] + fac[24 + t]) for t in range(8)]
    return jnp.concatenate([f[r : r + 1] for f in parts], axis=1)


def front_kernel(
    pos, one, two, fac, small, half, rest, wq_h, wk_h, wv_h, wd_h, ww_h, spike_h,
    m_o, r_o, o_o,
    hid, packed, wq, wk, wv, wd, ww, spike, sems,
):
    copies = start_copies(
        (wq_h, wk_h, wv_h, wd_h, ww_h, spike_h), (wq, wk, wv, wd, ww, spike), sems
    )
    shift, scale = (factor(fac, 0), factor(fac, 1))
    for d in range(4):
        for i, lat in enumerate((one, two)):
            core = pos[6] if i == 0 else 1 - pos[6]
            spot = (2 * ((pos[7] + 4 - d) % 4) + core) * 32
            hid[pl.ds(pl.multiple_of(spot, 32), 32)] = norm_rows(lat[d], scale, shift)
    first = pos[6] == 0
    sides = (half[...].astype(F32), rest[...].astype(F32))
    left, right = (jnp.where(first, *pair) for pair in (sides, sides[::-1]))
    context_rows = jnp.concatenate([left, right], axis=1)
    hid[256:320] = norm_rows(context_rows, factor(fac, 4), factor(fac, 3))
    rows = hid[...]
    copies[0].wait()
    packed[0:256] = mm(hid[0:256], wq[...]).astype(BF)
    copies[1].wait()
    keys = mm(rows, wk[...]).astype(BF)
    packed[256:512] = keys[:256]
    for copy in copies[2:]:
        copy.wait()
    values = mm(rows, wv[...]).astype(BF)
    packed[512:768] = values[:256]
    packed[768:800] = mm(wd[...], hid[0:256], ((1,), (1,))).astype(BF)
    packed[800:832] = mm(ww[...], hid[0:256], ((1,), (1,))).astype(BF)
    rate = mm(hid[256:320], wd[...], ((1,), (1,))).astype(BF).astype(F32)
    write = mm(hid[256:320], ww[...], ((1,), (1,))).astype(BF).astype(F32)
    lanes = lax.broadcasted_iota(jnp.int32, (64, 256), 1)
    rank = lax.broadcasted_iota(jnp.int32, (64, 256), 0)
    spots = lanes == (rank // 4) * 16 + rank % 4 + pos[5]
    for j in range(4):
        h = j // 2
        lane = pos[1] * 4 + j
        to = (j + pos[4]) % 4
        m_o[to, 128:192, 0:128] = keys[256:320, 128 * h : 128 * h + 128]
        m_o[to, 128:192, 128:256] = values[256:320, 128 * h : 128 * h + 128]
        pieces = [
            jnp.sum(jnp.where(spots, column(g, lane), 0.0), axis=0, keepdims=True)
            for g in (rate, write)
        ]
        pieces.append(jnp.zeros((14, 256), F32))
        m_o[to, 192:208] = jnp.concatenate(pieces, axis=0).astype(BF)
    chunk(pos, packed, spike, small, m_o, r_o, o_o)


def chunk(pos, packed, spike, small, m_o, r_o, o_o):
    row = lax.broadcasted_iota(jnp.int32, (256, 256), 0)
    col = lax.broadcasted_iota(jnp.int32, (256, 256), 1)
    eye = row == col
    entry = lax.broadcasted_iota(jnp.int32, (32, 128), 0)
    entry = entry == lax.broadcasted_iota(jnp.int32, (32, 128), 1)
    decay, bias = (
        jnp.sum(jnp.where(entry, small[i : i + 1], 0.0), axis=1, keepdims=True) for i in range(2)
    )
    logs = -decay * softplus(packed[768:800].astype(F32)) + spike[...]
    strength = sigmoid(packed[800:832].astype(F32) + bias)
    entry = lax.broadcasted_iota(jnp.int32, (32, 256), 0) - pos[1] * 4
    below = (row >= col).astype(F32)
    above = (row <= col).astype(F32)
    sums = (
        jnp.dot(logs, above, precision=HI, preferred_element_type=F32),
        jnp.dot(logs, below, precision=HI, preferred_element_type=F32),
    )

    def upright(line):
        return jnp.sum(jnp.where(eye, line, 0.0), axis=1, keepdims=True)

    lowers, parts = ([], [])
    for h in range(2):
        qh, kh, vh = (packed[256 * i : 256 * i + 256, 128 * h : 128 * h + 128] for i in range(3))
        kf = kh.astype(F32)
        unit = lax.rsqrt(jnp.sum(kf * kf, axis=1, keepdims=True) + EPS)
        unit_row = jnp.sum(jnp.where(eye, unit, 0.0), axis=0, keepdims=True)
        gram = mm(kh, kh, ((1,), (1,))) * unit_row
        cross = mm(qh, kh, ((1,), (1,))) * unit_row
        for e in range(2):
            j = 2 * h + e
            total_row = jnp.sum(jnp.where(entry == j, sums[e], 0.0), axis=0, keepdims=True)
            total = upright(total_row)
            b = upright(jnp.sum(jnp.where(entry == j, strength, 0.0), axis=0, keepdims=True))
            last = total[255:256] if e == 0 else total[0:1]
            inside = row >= col if e == 0 else row <= col
            fade = jnp.where(inside, jnp.exp(jnp.where(inside, total - total_row, 0.0)), 0.0)
            lowers.append(jnp.where(eye, 0.0, (b * unit) * gram * fade))
            grown = jnp.exp(total)
            right = jnp.concatenate(
                [
                    b * vh.astype(F32),
                    (b * unit * grown) * kf,
                ],
                axis=1,
            ).astype(BF)
            faded = (kf * (unit * jnp.exp(last - total))).astype(BF)
            scores = (cross * fade).astype(BF)
            parts.append((right, faded, scores, grown * qh.astype(F32), jnp.exp(last) - 1.0))
    solved = inverse_of(lowers, row, col)
    small = lax.broadcasted_iota(jnp.int32, (128, 128), 0) == lax.broadcasted_iota(
        jnp.int32, (128, 128), 1
    )
    outs = [None, None]
    for j in range(4):
        right, faded, scores, grown_q, short = parts[j]
        both = mm(solved[j], right).astype(BF)
        maps = mm(faded, both, ((0,), (0,)))
        read = mm(scores, both)
        to = (j + pos[4]) % 4
        m_o[to, 0:128, 0:128] = (jnp.where(small, short, 0.0) - maps[:, 128:]).astype(BF)
        m_o[to, 0:128, 128:256] = maps[:, :128].astype(BF)
        h, e = divmod(j, 2)
        r_o[h, :, 128 * e : 128 * e + 128] = (grown_q - read[:, 128:]).astype(BF)
        outs[h] = read[:, :128] if e == 0 else outs[h] + read[:, :128]
    o_o[:, 0:128] = outs[0]
    o_o[:, 128:256] = outs[1]


def context_state(pos, rows, rate, write, decay, bias, extra):
    row = lax.broadcasted_iota(jnp.int32, (256, 256), 0)
    col = lax.broadcasted_iota(jnp.int32, (256, 256), 1)
    eye = row == col
    lane = pos[1] * 4 + pos[0]
    inside = (row - col) * (1 - 2 * (pos[0] % 2)) >= 0
    kh = rows[:, 0:128].astype(BF)
    kf = rows[:, 0:128]
    logs = -column(decay, lane) * softplus(rate)
    strength = sigmoid(write + column(bias, lane) + column(extra, lane))
    b = jnp.sum(jnp.where(eye, strength, 0.0), axis=1, keepdims=True)
    total = jnp.sum(jnp.where(inside, logs, 0.0), axis=1, keepdims=True)
    total_row = jnp.sum(jnp.where(eye, total, 0.0), axis=0, keepdims=True)
    last = jnp.sum(logs, axis=1, keepdims=True)
    unit = lax.rsqrt(jnp.sum(kf * kf, axis=1, keepdims=True) + EPS)
    unit_row = jnp.sum(jnp.where(eye, unit, 0.0), axis=0, keepdims=True)
    fade = jnp.where(inside, jnp.exp(jnp.where(inside, total - total_row, 0.0)), 0.0)
    lower = jnp.where(
        eye, 0.0, (b * unit) * (mm(kh, kh, ((1,), (1,))) * unit_row) * fade
    )
    solved = inverse_of([lower], row, col)[0]
    fresh = mm(solved, b * rows[:, 128:256])
    faded = kf * (unit * jnp.exp(last - total))
    return mm(faded, fresh, ((0,), (0,)))


def apply_to(linear, state):
    high = state.astype(BF)
    low = (state - high.astype(F32)).astype(BF)
    both = mm(linear, jnp.concatenate([high, low], axis=1))
    n = state.shape[1]
    return both[:, :n] + both[:, n:]


def composed(pos, maps):
    back = pos[0] % 2
    at = back * 3
    step = 1 - 2 * back
    total = maps[at][0:128].astype(F32)
    for _ in range(3):
        at = at + step
        total = total + maps[at][0:128].astype(F32) + apply_to(maps[at][0:128, 0:128], total)
    return total


def low_kernel(pos, maps, o):
    out = composed(pos, maps).astype(BF)
    for i in range(4):
        o[i] = out


def high_kernel(pos, maps, o):
    o[...] = composed(pos, maps).astype(BF)


def context_kernel(pos, maps, small, o):
    wide = [maps[i][128:].astype(F32) for i in range(4)]
    rows = jnp.concatenate([w[4 * i : 4 * i + 4] for i in range(16) for w in wide], axis=0)
    gates = sum(w[64:66] for w in wide)
    o[...] = context_state(
        pos, rows, gates[0:1], gates[1:2], small[0:1], small[1:2], small[2:3]
    )


def moved(maps, state):
    return state + maps[:, 128:256].astype(F32) + apply_to(maps[:, 0:128], state)


def scan_kernel(pos, start, far, middle, near, low, own, o):
    back = pos[0] % 2
    step = 1 - 2 * back
    state = start[...]
    for maps in (far, middle, near):
        state = moved(maps[...], state)
    at = back * 3
    for _ in range(3):
        state = jnp.where((pos[3] - at) * step > 0, moved(low[at][0:128], state), state)
        at = at + step
    at = back * 3
    for i in range(4):
        o[at] = state.astype(BF)
        if i < 3:
            state = moved(own[at][0:128], state)
        at = at + step


def read_kernel(pos, states, reads, base, gain, weight, keep, give):
    heads = []
    for h in range(2):
        first = states[(2 * h + pos[4]) % 4]
        second = states[(2 * h + 1 + pos[4]) % 4]
        total = base[:, 128 * h : 128 * h + 128] + (
            mm(reads[h][:, 0:128], first) + mm(reads[h][:, 128:256], second)
        )
        mean = jnp.mean(total * total, axis=1, keepdims=True)
        heads.append((total * lax.rsqrt(mean + EPS) * gain[3:4]).astype(BF))
    branch = mm(jnp.concatenate(heads, axis=1), weight[...]).astype(BF)

    def split(even, odd):
        for i in range(4):
            even[i] = branch[64 * i : 64 * i + 32]
            odd[i] = branch[64 * i + 32 : 64 * i + 64]

    @pl.when(pos[6] == 0)
    def _():
        split(keep, give)

    @pl.when(pos[6] != 0)
    def _():
        split(give, keep)


def merge_kernel(keep, got, o):
    o[...] = (keep[...].astype(F32) + got[...].astype(F32)).astype(BF)


def output_kernel(rows, fac, lat, o):
    branch = (rows[0].astype(F32) + rows[1].astype(F32)) + (
        rows[2].astype(F32) + rows[3].astype(F32)
    )
    o[...] = (lat[...].astype(F32) + factor(fac, 2) * branch).astype(BF)


def call(kernel, outs, specs, scratch=(), flops=1, aliases=None):
    def shape(s):
        return jax.ShapeDtypeStruct(*s)

    many = isinstance(outs, list)
    return pl.pallas_call(
        kernel,
        out_shape=[shape(s) for s in outs] if many else shape(outs),
        in_specs=specs,
        out_specs=[VM] * len(outs) if many else VM,
        scratch_shapes=scratch,
        input_output_aliases=aliases or {},
        compiler_params=pltpu.CompilerParams(vmem_limit_bytes=24 * 2**20),
        cost_estimate=pl.CostEstimate(flops=flops, bytes_accessed=1, transcendentals=0),
    )


def to_all(value, axes, count):
    return lax.all_to_all(
        jnp.broadcast_to(value[None], (count, *value.shape)), axes, 0, 0, tiled=True
    )


def onward(d):
    pairs = []
    for zh in range(4):
        for y in range(4):
            for c in range(2):
                to = zh + d if (y + c) % 2 == 0 else zh - d
                if 0 <= to < 4:
                    pairs.append((zh * 8 + y * 2 + c, to * 8 + y * 2 + c))
    return pairs


def per_device(
    latent,
    condition,
    context,
    context_condition_vector,
    modulation_matrix,
    query_matrix,
    key_matrix,
    value_matrix,
    decay_input_weight,
    write_strength_weight,
    head_decay_rate,
    write_strength_bias,
    context_write_offset_bias,
    log_spike_added,
    head_norm_gain,
    output_matrix,
):
    zh, zl, y = (lax.axis_index("zh"), lax.axis_index("zl"), lax.axis_index("y"))
    x, c = (lax.axis_index("x"), lax.axis_index("c"))
    sp_index = lax.axis_index(SP)
    pos = jnp.stack([(y + c) % 4, x * 2 + c, zh, zl, (4 - c) % 4, y * 4, c, x])
    pos = pos.astype(jnp.int32)
    parts = [latent]
    for d in range(1, 4):
        parts.append(lax.ppermute(latent, "x", [(i, (i + d) % 4) for i in range(4)]))
    mine = jnp.stack(parts)
    other = lax.ppermute(mine, "c", [(0, 1), (1, 0)])
    signals = jnp.stack([condition, context_condition_vector])
    signals = lax.dynamic_slice_in_dim(jax.nn.silu(signals), sp_index * 32, 32, 1)
    mod = modulation_matrix.astype(F32)
    part = jnp.concatenate(
        [
            jnp.sum(mod * signals[0][None, :, None], axis=1),
            jnp.sum(mod[:2] * signals[1][None, :, None], axis=1),
        ]
    )
    high = lax.reduce_precision(part, 8, 7)
    sent = jnp.concatenate(
        [
            high.astype(BF),
            (part - high).astype(BF),
            jnp.zeros((6, 256), BF),
            lax.dynamic_slice_in_dim(context, c * (D // 2), D // 2, 1).reshape(16, 256),
        ]
    )
    sent = to_all(sent, Z, 16)
    part = jnp.sum(sent[:, 0:5].astype(F32) + sent[:, 5:10].astype(F32), axis=0)
    ctx = sent[:, 16:32].reshape(64, D // 2)
    rest = lax.ppermute(ctx, "c", [(0, 1), (1, 0)])
    fac = to_all(part, ("y", "x", "c"), 32)

    small = jnp.stack(
        [
            jnp.pad(head_decay_rate, (0, 96)),
            jnp.pad(write_strength_bias, (0, 96)),
            jnp.pad(context_write_offset_bias, (0, 96)),
            head_norm_gain,
        ]
    )
    slow = [
        pltpu.with_memory_space_constraint(a, pltpu.HBM)
        for a in (
            query_matrix,
            key_matrix,
            value_matrix,
            decay_input_weight.T,
            write_strength_weight.T,
            log_spike_added.T,
        )
    ]
    room = [
        pltpu.VMEM((D, 256), BF),
        pltpu.VMEM((D, 256), BF),
        pltpu.VMEM((D, 256), BF),
        pltpu.VMEM((32, D), BF),
        pltpu.VMEM((32, D), BF),
        pltpu.VMEM((32, 256), F32),
        pltpu.SemaphoreType.DMA((6,)),
    ]
    maps, reads, base = call(
        front_kernel,
        [((4, 208, 256), BF), ((2, 256, 256), BF), ((256, 256), F32)],
        [SM] + [VM] * 6 + [HB] * 6,
        [pltpu.VMEM((320, D), BF), pltpu.VMEM((832, 256), BF), *room],
        flops=5 * 10**9,
    )(
        pos,
        mine,
        other,
        fac,
        small,
        ctx,
        rest,
        *slow,
    )
    of_y = lax.all_to_all(maps, "y", 0, 0, tiled=True)
    low = call(low_kernel, ((4, 128, 256), BF), [SM, VM])(pos, of_y)
    of_low = lax.all_to_all(low, "zl", 0, 0, tiled=True)
    high = call(high_kernel, ((128, 256), BF), [SM, VM])(pos, of_low)
    of_high = []
    for d in (3, 2, 1):
        of_high.append(lax.ppermute(high, ("zh", "y", "c"), onward(d)))
    start = call(context_kernel, ((128, 128), F32), [SM] + [VM] * 2, flops=10**9)(pos, of_y, small)
    states = call(scan_kernel, ((4, 128, 128), BF), [SM] + [VM] * 6, flops=10**8)(
        pos, start, *of_high, of_low, of_y
    )
    states = lax.all_to_all(states, "y", 0, 0, tiled=True)
    keep, give = call(
        read_kernel, [((4, 32, D), BF)] * 2, [SM] + [VM] * 5, flops=10**8
    )(pos, states, reads, base, small, output_matrix)
    got = lax.ppermute(give, "c", [(0, 1), (1, 0)])
    branch = call(merge_kernel, ((4, 32, D), BF), [VM] * 2)(keep, got)
    branch = lax.all_to_all(branch, "x", 0, 0, tiled=True)
    return call(output_kernel, ((32, D), BF), [VM] * 3, flops=10**8)(branch, fac, latent)


def solution(mesh):
    split = Mesh(mesh.devices.reshape(4, 4, 4, 4, 2), ALL)
    return jax.shard_map(
        per_device,
        mesh=split,
        in_specs=(
            P(ALL, None),
            P(),
            P(SP, None),
            P(),
            P(None, SP, TP),
            P(None, TP),
            P(None, TP),
            P(None, TP),
            P(),
            P(),
            P(),
            P(),
            P(),
            P(SP, None),
            P(),
            P(TP, None),
        ),
        out_specs=P(ALL, None),
        check_vma=False,
    )
```

```python
import jax
import jax.numpy as jnp
from jax import lax
from jax.experimental import pallas as pl
from jax.experimental.pallas import tpu as pltpu
from jax.sharding import Mesh
from jax.sharding import PartitionSpec as P


D = 2048
EPS = 1e-06
HI = lax.Precision.HIGHEST
F32 = jnp.float32
BF = jnp.bfloat16
Z = ("zh", "zl")
TP = ("x", "c")
SP = ("zh", "zl", "y")
ALL = ("zh", "zl", "y", "x", "c")
VM = pl.BlockSpec(memory_space=pltpu.VMEM)
SM = pl.BlockSpec(memory_space=pltpu.SMEM)
HB = pl.BlockSpec(memory_space=pltpu.HBM)


def mm(a, b, dims=((1,), (0,))):
    return lax.dot_general(
        a.astype(BF), b.astype(BF), (dims, ((), ())), preferred_element_type=F32
    )


def norm_rows(rows, scale, shift):
    wide = rows.astype(F32)
    centred = wide - jnp.mean(wide, axis=-1, keepdims=True)
    spread = jnp.mean(centred * centred, axis=-1, keepdims=True)
    return (centred * lax.rsqrt(spread + EPS) * (1.0 + scale) + shift).astype(BF)


def column(matrix, lane):
    lanes = lax.broadcasted_iota(jnp.int32, matrix.shape, 1)
    return jnp.sum(jnp.where(lanes == lane, matrix, 0.0), axis=1, keepdims=True)


def softplus(t):
    return jnp.maximum(t, 0.0) + jnp.log1p(jnp.exp(-jnp.abs(t)))


def sigmoid(t):
    return 1.0 / (1.0 + jnp.exp(-t))


def inverse_of(lower, row, col):
    eye = (row == col).astype(F32)
    own = (row // 16) == (col // 16)
    base = [jnp.where(own, m, 0.0) for m in lower]
    inv = [eye - m for m in base]
    power = [mm(m, m) for m in base]
    for step in range(3):
        inv = [p + mm(p, x) for p, x in zip(inv, power)]
        if step < 2:
            power = [mm(x, x) for x in power]
    size = 16
    while size < 256:
        here = ((row // (2 * size)) == (col // (2 * size))) & ((row // size) != (col // size))
        side = [mm(jnp.where(here, m, 0.0), p) for m, p in zip(lower, inv)]
        inv = [p - mm(p, s) for p, s in zip(inv, side)]
        size *= 2
    out = []
    for m, p in zip(lower, inv):
        first = p.astype(BF)
        high = m.astype(BF)
        low = (m - high.astype(F32)).astype(BF)
        wide = first.astype(F32)
        left = (eye - wide) - (mm(high, first) + mm(low, first))
        out.append(wide + mm(first, left))
    return out


def start_copies(sources, targets, sems):
    copies = [
        pltpu.make_async_copy(source, target, sems.at[i])
        for i, (source, target) in enumerate(zip(sources, targets))
    ]
    for copy in copies:
        copy.start()
    return copies


def factor(fac, r):
    parts = [(fac[t] + fac[8 + t]) + (fac[16 + t] + fac[24 + t]) for t in range(8)]
    return jnp.concatenate([f[r : r + 1] for f in parts], axis=1)


def front_kernel(
    pos, one, two, fac, small, half, rest, wq_h, wk_h, wv_h, wd_h, ww_h, spike_h,
    m_o, r_o, o_o,
    hid, packed, wq, wk, wv, wd, ww, spike, sems,
):
    copies = start_copies(
        (wq_h, wk_h, wv_h, wd_h, ww_h, spike_h), (wq, wk, wv, wd, ww, spike), sems
    )
    shift, scale = (factor(fac, 0), factor(fac, 1))
    for d in range(4):
        for i, lat in enumerate((one, two)):
            core = pos[6] if i == 0 else 1 - pos[6]
            spot = (2 * ((pos[7] + 4 - d) % 4) + core) * 32
            hid[pl.ds(pl.multiple_of(spot, 32), 32)] = norm_rows(lat[d], scale, shift)
    first = pos[6] == 0
    sides = (half[...].astype(F32), rest[...].astype(F32))
    left, right = (jnp.where(first, *pair) for pair in (sides, sides[::-1]))
    context_rows = jnp.concatenate([left, right], axis=1)
    hid[256:320] = norm_rows(context_rows, factor(fac, 4), factor(fac, 3))
    rows = hid[...]
    copies[0].wait()
    packed[0:256] = mm(hid[0:256], wq[...]).astype(BF)
    copies[1].wait()
    keys = mm(rows, wk[...]).astype(BF)
    packed[256:512] = keys[:256]
    for copy in copies[2:]:
        copy.wait()
    values = mm(rows, wv[...]).astype(BF)
    packed[512:768] = values[:256]
    packed[768:800] = mm(wd[...], hid[0:256], ((1,), (1,))).astype(BF)
    packed[800:832] = mm(ww[...], hid[0:256], ((1,), (1,))).astype(BF)
    rate = mm(hid[256:320], wd[...], ((1,), (1,))).astype(BF).astype(F32)
    write = mm(hid[256:320], ww[...], ((1,), (1,))).astype(BF).astype(F32)
    lanes = lax.broadcasted_iota(jnp.int32, (64, 256), 1)
    rank = lax.broadcasted_iota(jnp.int32, (64, 256), 0)
    spots = lanes == (rank // 4) * 16 + rank % 4 + pos[5]
    for j in range(4):
        h = j // 2
        lane = pos[1] * 4 + j
        to = (j + pos[4]) % 4
        m_o[to, 128:192, 0:128] = keys[256:320, 128 * h : 128 * h + 128]
        m_o[to, 128:192, 128:256] = values[256:320, 128 * h : 128 * h + 128]
        pieces = [
            jnp.sum(jnp.where(spots, column(g, lane), 0.0), axis=0, keepdims=True)
            for g in (rate, write)
        ]
        pieces.append(jnp.zeros((14, 256), F32))
        m_o[to, 192:208] = jnp.concatenate(pieces, axis=0).astype(BF)
    chunk(pos, packed, spike, small, m_o, r_o, o_o)


def chunk(pos, packed, spike, small, m_o, r_o, o_o):
    row = lax.broadcasted_iota(jnp.int32, (256, 256), 0)
    col = lax.broadcasted_iota(jnp.int32, (256, 256), 1)
    eye = row == col
    entry = lax.broadcasted_iota(jnp.int32, (32, 128), 0)
    entry = entry == lax.broadcasted_iota(jnp.int32, (32, 128), 1)
    decay, bias = (
        jnp.sum(jnp.where(entry, small[i : i + 1], 0.0), axis=1, keepdims=True) for i in range(2)
    )
    logs = -decay * softplus(packed[768:800].astype(F32)) + spike[...]
    strength = sigmoid(packed[800:832].astype(F32) + bias)
    entry = lax.broadcasted_iota(jnp.int32, (32, 256), 0) - pos[1] * 4
    below = (row >= col).astype(F32)
    above = (row <= col).astype(F32)
    sums = (
        jnp.dot(logs, above, precision=HI, preferred_element_type=F32),
        jnp.dot(logs, below, precision=HI, preferred_element_type=F32),
    )

    def upright(line):
        return jnp.sum(jnp.where(eye, line, 0.0), axis=1, keepdims=True)

    lowers, parts = ([], [])
    for h in range(2):
        qh, kh, vh = (packed[256 * i : 256 * i + 256, 128 * h : 128 * h + 128] for i in range(3))
        kf = kh.astype(F32)
        unit = lax.rsqrt(jnp.sum(kf * kf, axis=1, keepdims=True) + EPS)
        unit_row = jnp.sum(jnp.where(eye, unit, 0.0), axis=0, keepdims=True)
        gram = mm(kh, kh, ((1,), (1,))) * unit_row
        cross = mm(qh, kh, ((1,), (1,))) * unit_row
        for e in range(2):
            j = 2 * h + e
            total_row = jnp.sum(jnp.where(entry == j, sums[e], 0.0), axis=0, keepdims=True)
            total = upright(total_row)
            b = upright(jnp.sum(jnp.where(entry == j, strength, 0.0), axis=0, keepdims=True))
            last = total[255:256] if e == 0 else total[0:1]
            inside = row >= col if e == 0 else row <= col
            fade = jnp.where(inside, jnp.exp(jnp.where(inside, total - total_row, 0.0)), 0.0)
            lowers.append(jnp.where(eye, 0.0, (b * unit) * gram * fade))
            grown = jnp.exp(total)
            right = jnp.concatenate(
                [
                    b * vh.astype(F32),
                    (b * unit * grown) * kf,
                ],
                axis=1,
            ).astype(BF)
            faded = (kf * (unit * jnp.exp(last - total))).astype(BF)
            scores = (cross * fade).astype(BF)
            parts.append((right, faded, scores, grown * qh.astype(F32), jnp.exp(last) - 1.0))
    solved = inverse_of(lowers, row, col)
    small = lax.broadcasted_iota(jnp.int32, (128, 128), 0) == lax.broadcasted_iota(
        jnp.int32, (128, 128), 1
    )
    outs = [None, None]
    for j in range(4):
        right, faded, scores, grown_q, short = parts[j]
        both = mm(solved[j], right).astype(BF)
        maps = mm(faded, both, ((0,), (0,)))
        read = mm(scores, both)
        to = (j + pos[4]) % 4
        m_o[to, 0:128, 0:128] = (jnp.where(small, short, 0.0) - maps[:, 128:]).astype(BF)
        m_o[to, 0:128, 128:256] = maps[:, :128].astype(BF)
        h, e = divmod(j, 2)
        r_o[h, :, 128 * e : 128 * e + 128] = (grown_q - read[:, 128:]).astype(BF)
        outs[h] = read[:, :128] if e == 0 else outs[h] + read[:, :128]
    o_o[:, 0:128] = outs[0]
    o_o[:, 128:256] = outs[1]


def context_state(pos, rows, rate, write, decay, bias, extra):
    row = lax.broadcasted_iota(jnp.int32, (256, 256), 0)
    col = lax.broadcasted_iota(jnp.int32, (256, 256), 1)
    eye = row == col
    lane = pos[1] * 4 + pos[0]
    inside = (row - col) * (1 - 2 * (pos[0] % 2)) >= 0
    kh = rows[:, 0:128].astype(BF)
    kf = rows[:, 0:128]
    logs = -column(decay, lane) * softplus(rate)
    strength = sigmoid(write + column(bias, lane) + column(extra, lane))
    b = jnp.sum(jnp.where(eye, strength, 0.0), axis=1, keepdims=True)
    total = jnp.sum(jnp.where(inside, logs, 0.0), axis=1, keepdims=True)
    total_row = jnp.sum(jnp.where(eye, total, 0.0), axis=0, keepdims=True)
    last = jnp.sum(logs, axis=1, keepdims=True)
    unit = lax.rsqrt(jnp.sum(kf * kf, axis=1, keepdims=True) + EPS)
    unit_row = jnp.sum(jnp.where(eye, unit, 0.0), axis=0, keepdims=True)
    fade = jnp.where(inside, jnp.exp(jnp.where(inside, total - total_row, 0.0)), 0.0)
    lower = jnp.where(
        eye, 0.0, (b * unit) * (mm(kh, kh, ((1,), (1,))) * unit_row) * fade
    )
    solved = inverse_of([lower], row, col)[0]
    fresh = mm(solved, b * rows[:, 128:256])
    faded = kf * (unit * jnp.exp(last - total))
    return mm(faded, fresh, ((0,), (0,)))


def apply_to(linear, state):
    high = state.astype(BF)
    low = (state - high.astype(F32)).astype(BF)
    both = mm(linear, jnp.concatenate([high, low], axis=1))
    n = state.shape[1]
    return both[:, :n] + both[:, n:]


def composed(pos, maps):
    back = pos[0] % 2
    at = back * 3
    step = 1 - 2 * back
    total = maps[at][0:128].astype(F32)
    for _ in range(3):
        at = at + step
        total = total + maps[at][0:128].astype(F32) + apply_to(maps[at][0:128, 0:128], total)
    return total


def low_kernel(pos, maps, o):
    out = composed(pos, maps).astype(BF)
    for i in range(4):
        o[i] = out


def high_kernel(pos, maps, o):
    o[...] = composed(pos, maps).astype(BF)


def context_kernel(pos, maps, small, o):
    wide = [maps[i][128:].astype(F32) for i in range(4)]
    rows = jnp.concatenate([w[4 * i : 4 * i + 4] for i in range(16) for w in wide], axis=0)
    gates = sum(w[64:66] for w in wide)
    o[...] = context_state(
        pos, rows, gates[0:1], gates[1:2], small[0:1], small[1:2], small[2:3]
    )


def moved(maps, state):
    return state + maps[:, 128:256].astype(F32) + apply_to(maps[:, 0:128], state)


def scan_kernel(pos, start, far, middle, near, low, own, o):
    back = pos[0] % 2
    step = 1 - 2 * back
    state = start[...]
    for maps in (far, middle, near):
        state = moved(maps[...], state)
    at = back * 3
    for _ in range(3):
        state = jnp.where((pos[3] - at) * step > 0, moved(low[at][0:128], state), state)
        at = at + step
    at = back * 3
    for i in range(4):
        o[at] = state.astype(BF)
        if i < 3:
            state = moved(own[at][0:128], state)
        at = at + step


def read_kernel(pos, states, reads, base, gain, weight, keep, give):
    heads = []
    for h in range(2):
        first = states[(2 * h + pos[4]) % 4]
        second = states[(2 * h + 1 + pos[4]) % 4]
        total = base[:, 128 * h : 128 * h + 128] + (
            mm(reads[h][:, 0:128], first) + mm(reads[h][:, 128:256], second)
        )
        mean = jnp.mean(total * total, axis=1, keepdims=True)
        heads.append((total * lax.rsqrt(mean + EPS) * gain[3:4]).astype(BF))
    branch = mm(jnp.concatenate(heads, axis=1), weight[...]).astype(BF)

    def split(even, odd):
        for i in range(4):
            even[i] = branch[64 * i : 64 * i + 32]
            odd[i] = branch[64 * i + 32 : 64 * i + 64]

    @pl.when(pos[6] == 0)
    def _():
        split(keep, give)

    @pl.when(pos[6] != 0)
    def _():
        split(give, keep)


def merge_kernel(keep, got, o):
    o[...] = (keep[...].astype(F32) + got[...].astype(F32)).astype(BF)


def output_kernel(rows, fac, lat, o):
    branch = (rows[0].astype(F32) + rows[1].astype(F32)) + (
        rows[2].astype(F32) + rows[3].astype(F32)
    )
    o[...] = (lat[...].astype(F32) + factor(fac, 2) * branch).astype(BF)


def call(kernel, outs, specs, scratch=(), flops=1, aliases=None):
    def shape(s):
        return jax.ShapeDtypeStruct(*s)

    many = isinstance(outs, list)
    return pl.pallas_call(
        kernel,
        out_shape=[shape(s) for s in outs] if many else shape(outs),
        in_specs=specs,
        out_specs=[VM] * len(outs) if many else VM,
        scratch_shapes=scratch,
        input_output_aliases=aliases or {},
        compiler_params=pltpu.CompilerParams(vmem_limit_bytes=24 * 2**20),
        cost_estimate=pl.CostEstimate(flops=flops, bytes_accessed=1, transcendentals=0),
    )


def to_all(value, axes, count):
    return lax.all_to_all(
        jnp.broadcast_to(value[None], (count, *value.shape)), axes, 0, 0, tiled=True
    )


def onward(d):
    pairs = []
    for zh in range(4):
        for y in range(4):
            for c in range(2):
                to = zh + d if (y + c) % 2 == 0 else zh - d
                if 0 <= to < 4:
                    pairs.append((zh * 8 + y * 2 + c, to * 8 + y * 2 + c))
    return pairs


def per_device(
    latent,
    condition,
    context,
    context_condition_vector,
    modulation_matrix,
    query_matrix,
    key_matrix,
    value_matrix,
    decay_input_weight,
    write_strength_weight,
    head_decay_rate,
    write_strength_bias,
    context_write_offset_bias,
    log_spike_added,
    head_norm_gain,
    output_matrix,
):
    zh, zl, y = (lax.axis_index("zh"), lax.axis_index("zl"), lax.axis_index("y"))
    x, c = (lax.axis_index("x"), lax.axis_index("c"))
    sp_index = lax.axis_index(SP)
    pos = jnp.stack([(y + c) % 4, x * 2 + c, zh, zl, (4 - c) % 4, y * 4, c, x])
    pos = pos.astype(jnp.int32)
    parts = [latent]
    for d in range(1, 4):
        parts.append(lax.ppermute(latent, "x", [(i, (i + d) % 4) for i in range(4)]))
    mine = jnp.stack(parts)
    other = lax.ppermute(mine, "c", [(0, 1), (1, 0)])
    signals = jnp.stack([condition, context_condition_vector])
    signals = lax.dynamic_slice_in_dim(jax.nn.silu(signals), sp_index * 32, 32, 1)
    mod = modulation_matrix.astype(F32)
    part = jnp.concatenate(
        [
            jnp.sum(mod * signals[0][None, :, None], axis=1),
            jnp.sum(mod[:2] * signals[1][None, :, None], axis=1),
        ]
    )
    sent = jnp.concatenate(
        [
            part.astype(BF),
            jnp.zeros((3, 256), BF),
            lax.dynamic_slice_in_dim(context, c * (D // 2), D // 2, 1).reshape(16, 256),
        ]
    )
    sent = to_all(sent, Z, 16)
    part = jnp.sum(sent[:, 0:5].astype(F32), axis=0)
    ctx = sent[:, 8:24].reshape(64, D // 2)
    rest = lax.ppermute(ctx, "c", [(0, 1), (1, 0)])
    fac = to_all(part, ("y", "x", "c"), 32)

    small = jnp.stack(
        [
            jnp.pad(head_decay_rate, (0, 96)),
            jnp.pad(write_strength_bias, (0, 96)),
            jnp.pad(context_write_offset_bias, (0, 96)),
            head_norm_gain,
        ]
    )
    slow = [
        pltpu.with_memory_space_constraint(a, pltpu.HBM)
        for a in (
            query_matrix,
            key_matrix,
            value_matrix,
            decay_input_weight.T,
            write_strength_weight.T,
            log_spike_added.T,
        )
    ]
    room = [
        pltpu.VMEM((D, 256), BF),
        pltpu.VMEM((D, 256), BF),
        pltpu.VMEM((D, 256), BF),
        pltpu.VMEM((32, D), BF),
        pltpu.VMEM((32, D), BF),
        pltpu.VMEM((32, 256), F32),
        pltpu.SemaphoreType.DMA((6,)),
    ]
    maps, reads, base = call(
        front_kernel,
        [((4, 208, 256), BF), ((2, 256, 256), BF), ((256, 256), F32)],
        [SM] + [VM] * 6 + [HB] * 6,
        [pltpu.VMEM((320, D), BF), pltpu.VMEM((832, 256), BF), *room],
        flops=5 * 10**9,
    )(
        pos,
        mine,
        other,
        fac,
        small,
        ctx,
        rest,
        *slow,
    )
    of_y = lax.all_to_all(maps, "y", 0, 0, tiled=True)
    low = call(low_kernel, ((4, 128, 256), BF), [SM, VM])(pos, of_y)
    of_low = lax.all_to_all(low, "zl", 0, 0, tiled=True)
    high = call(high_kernel, ((128, 256), BF), [SM, VM])(pos, of_low)
    of_high = []
    for d in (3, 2, 1):
        of_high.append(lax.ppermute(high, ("zh", "y", "c"), onward(d)))
    start = call(context_kernel, ((128, 128), F32), [SM] + [VM] * 2, flops=10**9)(pos, of_y, small)
    states = call(scan_kernel, ((4, 128, 128), BF), [SM] + [VM] * 6, flops=10**8)(
        pos, start, *of_high, of_low, of_y
    )
    states = lax.all_to_all(states, "y", 0, 0, tiled=True)
    keep, give = call(
        read_kernel, [((4, 32, D), BF)] * 2, [SM] + [VM] * 5, flops=10**8
    )(pos, states, reads, base, small, output_matrix)
    got = lax.ppermute(give, "c", [(0, 1), (1, 0)])
    branch = call(merge_kernel, ((4, 32, D), BF), [VM] * 2)(keep, got)
    branch = lax.all_to_all(branch, "x", 0, 0, tiled=True)
    return call(output_kernel, ((32, D), BF), [VM] * 3, flops=10**8)(branch, fac, latent)


def solution(mesh):
    split = Mesh(mesh.devices.reshape(4, 4, 4, 4, 2), ALL)
    return jax.shard_map(
        per_device,
        mesh=split,
        in_specs=(
            P(ALL, None),
            P(),
            P(SP, None),
            P(),
            P(None, SP, TP),
            P(None, TP),
            P(None, TP),
            P(None, TP),
            P(),
            P(),
            P(),
            P(),
            P(),
            P(SP, None),
            P(),
            P(TP, None),
        ),
        out_specs=P(ALL, None),
        check_vma=False,
    )
```

```python
import jax
import jax.numpy as jnp
from jax import lax
from jax.experimental import pallas as pl
from jax.experimental.pallas import tpu as pltpu
from jax.sharding import Mesh
from jax.sharding import PartitionSpec as P


D = 2048
EPS = 1e-06
HI = lax.Precision.HIGHEST
F32 = jnp.float32
BF = jnp.bfloat16
Z = ("zh", "zl")
TP = ("x", "c")
SP = ("zh", "zl", "y")
ALL = ("zh", "zl", "y", "x", "c")
VM = pl.BlockSpec(memory_space=pltpu.VMEM)
SM = pl.BlockSpec(memory_space=pltpu.SMEM)
HB = pl.BlockSpec(memory_space=pltpu.HBM)


def mm(a, b, dims=((1,), (0,))):
    return lax.dot_general(
        a.astype(BF), b.astype(BF), (dims, ((), ())), preferred_element_type=F32
    )


def norm_rows(rows, scale, shift):
    wide = rows.astype(F32)
    centred = wide - jnp.mean(wide, axis=-1, keepdims=True)
    spread = jnp.mean(centred * centred, axis=-1, keepdims=True)
    return (centred * lax.rsqrt(spread + EPS) * (1.0 + scale) + shift).astype(BF)


def column(matrix, lane):
    lanes = lax.broadcasted_iota(jnp.int32, matrix.shape, 1)
    return jnp.sum(jnp.where(lanes == lane, matrix, 0.0), axis=1, keepdims=True)


def softplus(t):
    return jnp.maximum(t, 0.0) + jnp.log1p(jnp.exp(-jnp.abs(t)))


def sigmoid(t):
    return 1.0 / (1.0 + jnp.exp(-t))


def inverse_of(lower, row, col):
    eye = (row == col).astype(F32)
    own = (row // 16) == (col // 16)
    base = [jnp.where(own, m, 0.0) for m in lower]
    inv = [eye - m for m in base]
    power = [mm(m, m) for m in base]
    for step in range(3):
        inv = [p + mm(p, x) for p, x in zip(inv, power)]
        if step < 2:
            power = [mm(x, x) for x in power]
    size = 16
    while size < 256:
        here = ((row // (2 * size)) == (col // (2 * size))) & ((row // size) != (col // size))
        side = [mm(jnp.where(here, m, 0.0), p) for m, p in zip(lower, inv)]
        inv = [p - mm(p, s) for p, s in zip(inv, side)]
        size *= 2
    out = []
    for m, p in zip(lower, inv):
        first = p.astype(BF)
        high = m.astype(BF)
        low = (m - high.astype(F32)).astype(BF)
        wide = first.astype(F32)
        left = (eye - wide) - (mm(high, first) + mm(low, first))
        out.append(wide + mm(first, left))
    return out


def start_copies(sources, targets, sems):
    copies = [
        pltpu.make_async_copy(source, target, sems.at[i])
        for i, (source, target) in enumerate(zip(sources, targets))
    ]
    for copy in copies:
        copy.start()
    return copies


def factor(fac, r):
    wide = [fac[i].astype(F32) for i in range(32)]
    parts = [(wide[t] + wide[8 + t]) + (wide[16 + t] + wide[24 + t]) for t in range(8)]
    return jnp.concatenate([f[r : r + 1] for f in parts], axis=1)


def front_kernel(
    pos, one, two, fac, small, half, rest, wq_h, wk_h, wv_h, wd_h, ww_h, spike_h,
    m_o, r_o, o_o,
    hid, packed, wq, wk, wv, wd, ww, spike, sems,
):
    copies = start_copies(
        (wq_h, wk_h, wv_h, wd_h, ww_h, spike_h), (wq, wk, wv, wd, ww, spike), sems
    )
    shift, scale = (factor(fac, 0), factor(fac, 1))
    for d in range(4):
        for i, lat in enumerate((one, two)):
            core = pos[6] if i == 0 else 1 - pos[6]
            spot = (2 * ((pos[7] + 4 - d) % 4) + core) * 32
            hid[pl.ds(pl.multiple_of(spot, 32), 32)] = norm_rows(lat[d], scale, shift)
    first = pos[6] == 0
    sides = (half[...].astype(F32), rest[...].astype(F32))
    left, right = (jnp.where(first, *pair) for pair in (sides, sides[::-1]))
    context_rows = jnp.concatenate([left, right], axis=1)
    hid[256:320] = norm_rows(context_rows, factor(fac, 4), factor(fac, 3))
    rows = hid[...]
    copies[0].wait()
    packed[0:256] = mm(hid[0:256], wq[...]).astype(BF)
    copies[1].wait()
    keys = mm(rows, wk[...]).astype(BF)
    packed[256:512] = keys[:256]
    for copy in copies[2:]:
        copy.wait()
    values = mm(rows, wv[...]).astype(BF)
    packed[512:768] = values[:256]
    packed[768:800] = mm(wd[...], hid[0:256], ((1,), (1,))).astype(BF)
    packed[800:832] = mm(ww[...], hid[0:256], ((1,), (1,))).astype(BF)
    rate = mm(hid[256:320], wd[...], ((1,), (1,))).astype(BF).astype(F32)
    write = mm(hid[256:320], ww[...], ((1,), (1,))).astype(BF).astype(F32)
    lanes = lax.broadcasted_iota(jnp.int32, (64, 256), 1)
    rank = lax.broadcasted_iota(jnp.int32, (64, 256), 0)
    spots = lanes == (rank // 4) * 16 + rank % 4 + pos[5]
    for j in range(4):
        h = j // 2
        lane = pos[1] * 4 + j
        to = (j + pos[4]) % 4
        m_o[to, 128:192, 0:128] = keys[256:320, 128 * h : 128 * h + 128]
        m_o[to, 128:192, 128:256] = values[256:320, 128 * h : 128 * h + 128]
        pieces = [
            jnp.sum(jnp.where(spots, column(g, lane), 0.0), axis=0, keepdims=True)
            for g in (rate, write)
        ]
        pieces.append(jnp.zeros((14, 256), F32))
        m_o[to, 192:208] = jnp.concatenate(pieces, axis=0).astype(BF)
    chunk(pos, packed, spike, small, m_o, r_o, o_o)


def chunk(pos, packed, spike, small, m_o, r_o, o_o):
    row = lax.broadcasted_iota(jnp.int32, (256, 256), 0)
    col = lax.broadcasted_iota(jnp.int32, (256, 256), 1)
    eye = row == col
    entry = lax.broadcasted_iota(jnp.int32, (32, 128), 0)
    entry = entry == lax.broadcasted_iota(jnp.int32, (32, 128), 1)
    decay, bias = (
        jnp.sum(jnp.where(entry, small[i : i + 1], 0.0), axis=1, keepdims=True) for i in range(2)
    )
    logs = -decay * softplus(packed[768:800].astype(F32)) + spike[...]
    strength = sigmoid(packed[800:832].astype(F32) + bias)
    entry = lax.broadcasted_iota(jnp.int32, (32, 256), 0) - pos[1] * 4
    below = (row >= col).astype(F32)
    above = (row <= col).astype(F32)
    sums = (
        jnp.dot(logs, above, precision=HI, preferred_element_type=F32),
        jnp.dot(logs, below, precision=HI, preferred_element_type=F32),
    )

    def upright(line):
        return jnp.sum(jnp.where(eye, line, 0.0), axis=1, keepdims=True)

    lowers, parts = ([], [])
    for h in range(2):
        qh, kh, vh = (packed[256 * i : 256 * i + 256, 128 * h : 128 * h + 128] for i in range(3))
        kf = kh.astype(F32)
        unit = lax.rsqrt(jnp.sum(kf * kf, axis=1, keepdims=True) + EPS)
        unit_row = jnp.sum(jnp.where(eye, unit, 0.0), axis=0, keepdims=True)
        gram = mm(kh, kh, ((1,), (1,))) * unit_row
        cross = mm(qh, kh, ((1,), (1,))) * unit_row
        for e in range(2):
            j = 2 * h + e
            total_row = jnp.sum(jnp.where(entry == j, sums[e], 0.0), axis=0, keepdims=True)
            total = upright(total_row)
            b = upright(jnp.sum(jnp.where(entry == j, strength, 0.0), axis=0, keepdims=True))
            last = total[255:256] if e == 0 else total[0:1]
            inside = row >= col if e == 0 else row <= col
            fade = jnp.where(inside, jnp.exp(jnp.where(inside, total - total_row, 0.0)), 0.0)
            lowers.append(jnp.where(eye, 0.0, (b * unit) * gram * fade))
            grown = jnp.exp(total)
            right = jnp.concatenate(
                [
                    b * vh.astype(F32),
                    (b * unit * grown) * kf,
                ],
                axis=1,
            ).astype(BF)
            faded = (kf * (unit * jnp.exp(last - total))).astype(BF)
            scores = (cross * fade).astype(BF)
            parts.append((right, faded, scores, grown * qh.astype(F32), jnp.exp(last) - 1.0))
    solved = inverse_of(lowers, row, col)
    small = lax.broadcasted_iota(jnp.int32, (128, 128), 0) == lax.broadcasted_iota(
        jnp.int32, (128, 128), 1
    )
    outs = [None, None]
    for j in range(4):
        right, faded, scores, grown_q, short = parts[j]
        both = mm(solved[j], right).astype(BF)
        maps = mm(faded, both, ((0,), (0,)))
        read = mm(scores, both)
        to = (j + pos[4]) % 4
        m_o[to, 0:128, 0:128] = (jnp.where(small, short, 0.0) - maps[:, 128:]).astype(BF)
        m_o[to, 0:128, 128:256] = maps[:, :128].astype(BF)
        h, e = divmod(j, 2)
        r_o[h, :, 128 * e : 128 * e + 128] = (grown_q - read[:, 128:]).astype(BF)
        outs[h] = read[:, :128] if e == 0 else outs[h] + read[:, :128]
    o_o[:, 0:128] = outs[0]
    o_o[:, 128:256] = outs[1]


def context_state(pos, rows, rate, write, decay, bias, extra):
    row = lax.broadcasted_iota(jnp.int32, (256, 256), 0)
    col = lax.broadcasted_iota(jnp.int32, (256, 256), 1)
    eye = row == col
    lane = pos[1] * 4 + pos[0]
    inside = (row - col) * (1 - 2 * (pos[0] % 2)) >= 0
    kh = rows[:, 0:128].astype(BF)
    kf = rows[:, 0:128]
    logs = -column(decay, lane) * softplus(rate)
    strength = sigmoid(write + column(bias, lane) + column(extra, lane))
    b = jnp.sum(jnp.where(eye, strength, 0.0), axis=1, keepdims=True)
    total = jnp.sum(jnp.where(inside, logs, 0.0), axis=1, keepdims=True)
    total_row = jnp.sum(jnp.where(eye, total, 0.0), axis=0, keepdims=True)
    last = jnp.sum(logs, axis=1, keepdims=True)
    unit = lax.rsqrt(jnp.sum(kf * kf, axis=1, keepdims=True) + EPS)
    unit_row = jnp.sum(jnp.where(eye, unit, 0.0), axis=0, keepdims=True)
    fade = jnp.where(inside, jnp.exp(jnp.where(inside, total - total_row, 0.0)), 0.0)
    lower = jnp.where(
        eye, 0.0, (b * unit) * (mm(kh, kh, ((1,), (1,))) * unit_row) * fade
    )
    solved = inverse_of([lower], row, col)[0]
    fresh = mm(solved, b * rows[:, 128:256])
    faded = kf * (unit * jnp.exp(last - total))
    return mm(faded, fresh, ((0,), (0,)))


def apply_to(linear, state):
    high = state.astype(BF)
    low = (state - high.astype(F32)).astype(BF)
    both = mm(linear, jnp.concatenate([high, low], axis=1))
    n = state.shape[1]
    return both[:, :n] + both[:, n:]


def composed(pos, maps):
    back = pos[0] % 2
    at = back * 3
    step = 1 - 2 * back
    total = maps[at][0:128].astype(F32)
    for _ in range(3):
        at = at + step
        total = total + maps[at][0:128].astype(F32) + apply_to(maps[at][0:128, 0:128], total)
    return total


def low_kernel(pos, maps, o):
    out = composed(pos, maps).astype(BF)
    for i in range(4):
        o[i] = out


def high_kernel(pos, maps, o):
    o[...] = composed(pos, maps).astype(BF)


def context_kernel(pos, maps, small, o):
    wide = [maps[i][128:].astype(F32) for i in range(4)]
    rows = jnp.concatenate([w[4 * i : 4 * i + 4] for i in range(16) for w in wide], axis=0)
    gates = sum(w[64:66] for w in wide)
    o[...] = context_state(
        pos, rows, gates[0:1], gates[1:2], small[0:1], small[1:2], small[2:3]
    )


def moved(maps, state):
    return state + maps[:, 128:256].astype(F32) + apply_to(maps[:, 0:128], state)


def scan_kernel(pos, start, far, middle, near, low, own, o):
    back = pos[0] % 2
    step = 1 - 2 * back
    state = start[...]
    for maps in (far, middle, near):
        state = moved(maps[...], state)
    at = back * 3
    for _ in range(3):
        state = jnp.where((pos[3] - at) * step > 0, moved(low[at][0:128], state), state)
        at = at + step
    at = back * 3
    for i in range(4):
        o[at] = state.astype(BF)
        if i < 3:
            state = moved(own[at][0:128], state)
        at = at + step


def read_kernel(pos, states, reads, base, gain, weight, keep, give):
    heads = []
    for h in range(2):
        first = states[(2 * h + pos[4]) % 4]
        second = states[(2 * h + 1 + pos[4]) % 4]
        total = base[:, 128 * h : 128 * h + 128] + (
            mm(reads[h][:, 0:128], first) + mm(reads[h][:, 128:256], second)
        )
        mean = jnp.mean(total * total, axis=1, keepdims=True)
        heads.append((total * lax.rsqrt(mean + EPS) * gain[3:4]).astype(BF))
    branch = mm(jnp.concatenate(heads, axis=1), weight[...]).astype(BF)

    def split(even, odd):
        for i in range(4):
            even[i] = branch[64 * i : 64 * i + 32]
            odd[i] = branch[64 * i + 32 : 64 * i + 64]

    @pl.when(pos[6] == 0)
    def _():
        split(keep, give)

    @pl.when(pos[6] != 0)
    def _():
        split(give, keep)


def merge_kernel(keep, got, o):
    o[...] = (keep[...].astype(F32) + got[...].astype(F32)).astype(BF)


def output_kernel(rows, fac, lat, o):
    branch = (rows[0].astype(F32) + rows[1].astype(F32)) + (
        rows[2].astype(F32) + rows[3].astype(F32)
    )
    o[...] = (lat[...].astype(F32) + factor(fac, 2) * branch).astype(BF)


def call(kernel, outs, specs, scratch=(), flops=1, aliases=None):
    def shape(s):
        return jax.ShapeDtypeStruct(*s)

    many = isinstance(outs, list)
    return pl.pallas_call(
        kernel,
        out_shape=[shape(s) for s in outs] if many else shape(outs),
        in_specs=specs,
        out_specs=[VM] * len(outs) if many else VM,
        scratch_shapes=scratch,
        input_output_aliases=aliases or {},
        compiler_params=pltpu.CompilerParams(vmem_limit_bytes=24 * 2**20),
        cost_estimate=pl.CostEstimate(flops=flops, bytes_accessed=1, transcendentals=0),
    )


def to_all(value, axes, count):
    return lax.all_to_all(
        jnp.broadcast_to(value[None], (count, *value.shape)), axes, 0, 0, tiled=True
    )


def onward(d):
    pairs = []
    for zh in range(4):
        for y in range(4):
            for c in range(2):
                to = zh + d if (y + c) % 2 == 0 else zh - d
                if 0 <= to < 4:
                    pairs.append((zh * 8 + y * 2 + c, to * 8 + y * 2 + c))
    return pairs


def per_device(
    latent,
    condition,
    context,
    context_condition_vector,
    modulation_matrix,
    query_matrix,
    key_matrix,
    value_matrix,
    decay_input_weight,
    write_strength_weight,
    head_decay_rate,
    write_strength_bias,
    context_write_offset_bias,
    log_spike_added,
    head_norm_gain,
    output_matrix,
):
    zh, zl, y = (lax.axis_index("zh"), lax.axis_index("zl"), lax.axis_index("y"))
    x, c = (lax.axis_index("x"), lax.axis_index("c"))
    sp_index = lax.axis_index(SP)
    pos = jnp.stack([(y + c) % 4, x * 2 + c, zh, zl, (4 - c) % 4, y * 4, c, x])
    pos = pos.astype(jnp.int32)
    parts = [latent]
    for d in range(1, 4):
        parts.append(lax.ppermute(latent, "x", [(i, (i + d) % 4) for i in range(4)]))
    mine = jnp.stack(parts)
    other = lax.ppermute(mine, "c", [(0, 1), (1, 0)])
    signals = jnp.stack([condition, context_condition_vector])
    signals = lax.dynamic_slice_in_dim(jax.nn.silu(signals), sp_index * 32, 32, 1)
    mod = modulation_matrix.astype(F32)
    part = jnp.concatenate(
        [
            jnp.sum(mod * signals[0][None, :, None], axis=1),
            jnp.sum(mod[:2] * signals[1][None, :, None], axis=1),
        ]
    )
    sent = jnp.concatenate(
        [
            part.astype(BF),
            jnp.zeros((3, 256), BF),
            lax.dynamic_slice_in_dim(context, c * (D // 2), D // 2, 1).reshape(16, 256),
        ]
    )
    sent = to_all(sent, Z, 16)
    part = jnp.sum(sent[:, 0:5].astype(F32), axis=0)
    ctx = sent[:, 8:24].reshape(64, D // 2)
    rest = lax.ppermute(ctx, "c", [(0, 1), (1, 0)])
    fac = to_all(part.astype(BF), ("y", "x", "c"), 32)

    small = jnp.stack(
        [
            jnp.pad(head_decay_rate, (0, 96)),
            jnp.pad(write_strength_bias, (0, 96)),
            jnp.pad(context_write_offset_bias, (0, 96)),
            head_norm_gain,
        ]
    )
    slow = [
        pltpu.with_memory_space_constraint(a, pltpu.HBM)
        for a in (
            query_matrix,
            key_matrix,
            value_matrix,
            decay_input_weight.T,
            write_strength_weight.T,
            log_spike_added.T,
        )
    ]
    room = [
        pltpu.VMEM((D, 256), BF),
        pltpu.VMEM((D, 256), BF),
        pltpu.VMEM((D, 256), BF),
        pltpu.VMEM((32, D), BF),
        pltpu.VMEM((32, D), BF),
        pltpu.VMEM((32, 256), F32),
        pltpu.SemaphoreType.DMA((6,)),
    ]
    maps, reads, base = call(
        front_kernel,
        [((4, 208, 256), BF), ((2, 256, 256), BF), ((256, 256), F32)],
        [SM] + [VM] * 6 + [HB] * 6,
        [pltpu.VMEM((320, D), BF), pltpu.VMEM((832, 256), BF), *room],
        flops=5 * 10**9,
    )(
        pos,
        mine,
        other,
        fac,
        small,
        ctx,
        rest,
        *slow,
    )
    of_y = lax.all_to_all(maps, "y", 0, 0, tiled=True)
    low = call(low_kernel, ((4, 128, 256), BF), [SM, VM])(pos, of_y)
    of_low = lax.all_to_all(low, "zl", 0, 0, tiled=True)
    high = call(high_kernel, ((128, 256), BF), [SM, VM])(pos, of_low)
    of_high = []
    for d in (3, 2, 1):
        of_high.append(lax.ppermute(high, ("zh", "y", "c"), onward(d)))
    start = call(context_kernel, ((128, 128), F32), [SM] + [VM] * 2, flops=10**9)(pos, of_y, small)
    states = call(scan_kernel, ((4, 128, 128), BF), [SM] + [VM] * 6, flops=10**8)(
        pos, start, *of_high, of_low, of_y
    )
    states = lax.all_to_all(states, "y", 0, 0, tiled=True)
    keep, give = call(
        read_kernel, [((4, 32, D), BF)] * 2, [SM] + [VM] * 5, flops=10**8
    )(pos, states, reads, base, small, output_matrix)
    got = lax.ppermute(give, "c", [(0, 1), (1, 0)])
    branch = call(merge_kernel, ((4, 32, D), BF), [VM] * 2)(keep, got)
    branch = lax.all_to_all(branch, "x", 0, 0, tiled=True)
    return call(output_kernel, ((32, D), BF), [VM] * 3, flops=10**8)(branch, fac, latent)


def solution(mesh):
    split = Mesh(mesh.devices.reshape(4, 4, 4, 4, 2), ALL)
    return jax.shard_map(
        per_device,
        mesh=split,
        in_specs=(
            P(ALL, None),
            P(),
            P(SP, None),
            P(),
            P(None, SP, TP),
            P(None, TP),
            P(None, TP),
            P(None, TP),
            P(),
            P(),
            P(),
            P(),
            P(),
            P(SP, None),
            P(),
            P(TP, None),
        ),
        out_specs=P(ALL, None),
        check_vma=False,
    )
```
